32 devices in a mesh: sp: 8 (over z, core), tp: 4 (over y, x).
Axes of the slice: x: 2, y: 2, z: 4, core: 2. Of those that a mesh axis runs over, the one named last changes fastest.
Arguments:
- residual: bfloat16 [1024, 2048], P('sp'), may hold values from -45 to 45
- query_a: bfloat16 [1024, 16, 128], P('sp', 'tp'), may hold values from -125 to 125
- keys_a: bfloat16 [1024, 16, 128], P('sp', 'tp'), may hold values from -8 to 8
- values_a: bfloat16 [1024, 16, 128], P('sp', 'tp'), may hold values from -6 to 6
- query_b: bfloat16 [1024, 16, 256], P('sp', 'tp'), may hold values from -125 to 125
- keys_b: bfloat16 [1024, 16, 256], P('sp', 'tp'), may hold values from -8 to 8
- values_b: bfloat16 [1024, 16, 256], P('sp', 'tp'), may hold values from -6 to 6
- lambda_a: float32 [16], P('tp'), may hold values from 0.3 to 0.8
- lambda_b: float32 [16], P('tp'), may hold values from 0.3 to 0.8
- gain_a: float32 [128], replicated, may hold values from 0.1 to 1.9
- gain_b: float32 [256], replicated, may hold values from 0.1 to 1.9
- proj_a: bfloat16 [2048, 2048], P('tp'), may hold values from -0.078125 to 0.078125
- proj_b: bfloat16 [4096, 2048], P('tp'), may hold values from -0.078125 to 0.078125
- norm_gain: float32 [2048], replicated, may hold values from 0.1 to 1.9
- routes: int32 [1024, 2], P('sp'), may hold values from 0 to 7, all different within a row; in each aligned block of 128 rows (0 to 127, 128 to 255, ...) at most 64 rows name the same one
- route_weight: float32 [1024, 2], P('sp'), may hold values from 0.2 to 2
- expert_gate: bfloat16 [8, 2048, 2048], P('sp', None, 'tp'), may hold values from -0.125 to 0.125
- expert_up: bfloat16 [8, 2048, 2048], P('sp', None, 'tp'), may hold values from -0.125 to 0.125
- expert_down: bfloat16 [8, 2048, 2048], P('sp', 'tp'), may hold values from -0.125 to 0.125
Outputs:
- layer_out: bfloat16 [1024, 2048], P('sp', 'tp')
The draws below stay inside these ranges and needn't reach their ends.
Inputs may be any that keep to these rules, and one draw needn't show every extreme that they name: `routes`: each row names 2 different experts; in each aligned block of 128 rows no expert is named more than 64 times, a bound that some block reaches.
All inputs are finite; a program needn't handle non-finite values.
Results may differ from the reference program's by a relative error of at most 0.013.
Values may be sent and summed in bfloat16 or wider, within the bound.
A program may use at most 64 MiB of HBM per device.

```python
import math
import jax
import jax.numpy as jnp
import numpy as np
from jax import lax

D = 2048
HEADS = 16
DK_A = 64
DV_A = 128
DK_B = 128
DV_B = 256
DFF = 2048
SEG = 64
TOP = 2
TOK_DEV = 128
SEQ = 1024
EXPERTS = 8
CAP = 64
N_SP = 8
N_TP = 4


def query_key_pair(key, key_size, marker):
    base = jax.random.fold_in(key, marker)
    key_query, key_keys = jax.random.split(base, 2)
    shape = (SEQ, HEADS, 2, key_size)
    queries = jnp.clip(jax.random.normal(key_query, shape, jnp.float32), -6.0, 6.0) * 1.3
    keys_drawn = jnp.clip(jax.random.normal(key_keys, shape, jnp.float32), -6.0, 6.0) * 1.3
    return (queries.reshape(SEQ, HEADS, 2 * key_size), keys_drawn.reshape(SEQ, HEADS, 2 * key_size))


def draw_query_a(key, part):
    return query_key_pair(key, DK_A, 11)[0].astype(jnp.bfloat16)


def draw_keys_a(key, part):
    return query_key_pair(key, DK_A, 11)[1].astype(jnp.bfloat16)


def draw_query_b(key, part):
    return query_key_pair(key, DK_B, 23)[0].astype(jnp.bfloat16)


def draw_keys_b(key, part):
    return query_key_pair(key, DK_B, 23)[1].astype(jnp.bfloat16)


def draw_residual(key, part):
    base = jax.random.fold_in(key, 37)
    key_values = jax.random.fold_in(base, 0)
    column = jnp.exp(math.log(0.35) + math.log(9.0) * jnp.arange(D, dtype=jnp.float32) / (D - 1))
    values = jnp.clip(jax.random.normal(key_values, (SEQ, D), jnp.float32), -6.0, 6.0) * column[None, :]
    return values.astype(jnp.bfloat16)


def block_scale(key, shape, shards, smallest, top_value):
    loudness, own = 1.0, jax.random.fold_in(key, 6)
    for axis_at, parts in shards:
        steps = jnp.exp(jax.random.uniform(jax.random.fold_in(own, axis_at), (parts,), jnp.float32, smallest / len(shards), top_value / len(shards)))
        loudness = loudness * jnp.repeat(steps, shape[axis_at] // parts).reshape([-1 if axis == axis_at else 1 for axis in range(len(shape))])
    return loudness


def shared_out(own_key, own, number, rows, number_of, top, reach, lean):
    sequence = jax.random.permutation(own_key, number_of)
    packed, usual = shares(number_of, rows * top, reach, lean, True), shares(number_of, rows * top, reach, lean, False)
    places = jnp.arange(number_of)

    def named(sizes, offset_by):
        used = int((sizes > 0).sum())
        fixed = max(1, used // 4)
        passed = fixed + (places - fixed + offset_by * (used - fixed)) % max(1, number_of - fixed)
        return jnp.zeros((number_of,), jnp.int32).at[sequence[jnp.where(places < fixed, places, passed)]].set(jnp.asarray(sizes, jnp.int32))

    sizes = jnp.where(number % 4 == 0, named(packed, number // 4), named(usual, number - number // 4 - 1))
    mixed = jax.random.permutation(jax.random.fold_in(own, 3), number_of)
    source_of, receiver = mixed[0:number_of // 2 * 2:2], mixed[1:number_of // 2 * 2:2]
    slack = jnp.minimum(sizes[source_of] - 1, reach - sizes[receiver]) // 2
    slack = jnp.where((source_of == sequence[0]) | (receiver == sequence[0]) | (sizes[receiver] == 0), 0, jnp.maximum(slack, 0))
    passed = jax.random.randint(jax.random.fold_in(own, 4), (number_of // 2,), 0, 1 << 20) % (slack + 1)
    sizes = sizes.at[source_of].add(-passed).at[receiver].add(passed)
    labels = jnp.searchsorted(jnp.cumsum(sizes), jnp.arange(rows * top), side="right").astype(jnp.int32)
    table = labels.reshape(top, rows).T
    table = table[jax.random.permutation(jax.random.fold_in(own, 1), rows)]
    offset_by = jax.random.randint(jax.random.fold_in(own, 2), (rows, 1), 0, top)
    return jnp.take_along_axis(table, (jnp.arange(top)[None, :] + offset_by) % top, axis=1)


def shares(number_of, total, limit, skew, full):
    portions = [(1 << 20) // math.isqrt(standing ** skew) + 1 for standing in range(1, number_of + 1)]
    largest = limit if full else min(limit, max(-(-total // number_of), total * portions[0] // sum(portions)))
    least = 1 if total - largest >= number_of - 1 else 0
    given, spare = [largest] + [least] * (number_of - 1), total - largest - least * (number_of - 1)
    while spare > 0:
        free = [i for i in range(1, number_of) if given[i] < largest] or [i for i in range(1, number_of) if given[i] < limit]
        pool, left = sum([portions[i] for i in free]), spare
        for i in free:
            addition = min(limit - given[i], max(1, left * portions[i] // pool), spare)
            given[i] = given[i] + addition
            spare = spare - addition
    return np.array(given)


def normal_values(stream_key, extent, scale, reach, cuts=(), kind=jnp.bfloat16):
    values = scale * jax.random.normal(stream_key, extent, jnp.float32)
    if cuts:
        values = values * block_scale(stream_key, extent, cuts, -0.22, 0.18)
    return jnp.clip(values, -reach, reach).astype(kind)


def setup_inputs(seed: int = 0) -> dict:
    keys = jax.random.split(jax.random.key(seed), 20)
    residual = draw_residual(jax.random.fold_in(keys[19], 71), 0)
    query_a = draw_query_a(jax.random.fold_in(keys[19], 71), 0)
    keys_a = draw_keys_a(jax.random.fold_in(keys[19], 71), 0)
    values_a = normal_values(keys[3], (SEQ, HEADS, DV_A), 1.0, 6.0, ((0, 8), (1, 4)))
    query_b = draw_query_b(jax.random.fold_in(keys[19], 71), 0)
    keys_b = draw_keys_b(jax.random.fold_in(keys[19], 71), 0)
    values_b = normal_values(keys[6], (SEQ, HEADS, DV_B), 1.0, 6.0, ((0, 8), (1, 4)))
    lambda_a = jnp.clip(0.3 + 0.5 * jax.random.uniform(keys[7], (HEADS,), jnp.float32) ** block_scale(keys[7], (HEADS,), ((0, 4),), -0.2, 0.2), 0.3, 0.8)
    lambda_b = jnp.clip(0.3 + 0.5 * jax.random.uniform(keys[8], (HEADS,), jnp.float32) ** block_scale(keys[8], (HEADS,), ((0, 4),), -0.2, 0.2), 0.3, 0.8)
    gain_a = jnp.clip(1.0 + 0.18 * jax.random.normal(keys[9], (DV_A,), jnp.float32), 0.1, 1.9)
    gain_b = jnp.clip(1.0 + 0.18 * jax.random.normal(keys[10], (DV_B,), jnp.float32), 0.1, 1.9)
    proj_a = normal_values(keys[11], (HEADS * DV_A, D), (HEADS * (DV_A + DV_B)) ** -0.5, 0.078125, ((0, 4),))
    proj_b = normal_values(keys[12], (HEADS * DV_B, D), (HEADS * (DV_A + DV_B)) ** -0.5, 0.078125, ((0, 4),))
    norm_gain = jnp.clip(1.0 + 0.18 * jax.random.normal(keys[13], (D,), jnp.float32), 0.1, 1.9)
    routes_keys = jax.random.split(jax.random.fold_in(keys[14], 1), SEQ // TOK_DEV)
    routes_turns = jax.random.permutation(jax.random.fold_in(keys[14], 3), SEQ // TOK_DEV)
    routes = jax.vmap(lambda own, number: shared_out(jax.random.fold_in(keys[14], 2), own, number, TOK_DEV, EXPERTS, TOP, CAP, 1))(routes_keys, routes_turns).reshape((SEQ, TOP))
    route_weight = jnp.clip(jnp.exp(math.log(2.0) - 2.3025851 * jax.random.uniform(keys[15], (SEQ, TOP), jnp.float32) ** block_scale(keys[15], (SEQ, TOP), ((0, 8),), -0.2, 0.2)), 0.2, 2.0)
    expert_gate = normal_values(keys[16], (EXPERTS, D, DFF), D ** -0.5, 0.125, ((0, 8), (2, 4)))
    expert_up = normal_values(keys[17], (EXPERTS, D, DFF), D ** -0.5, 0.125, ((0, 8), (2, 4)))
    expert_down = normal_values(keys[18], (EXPERTS, DFF, D), DFF ** -0.5, 0.125, ((0, 8), (1, 4)))
    return dict(residual=residual, query_a=query_a, keys_a=keys_a, values_a=values_a, query_b=query_b, keys_b=keys_b, values_b=values_b, lambda_a=lambda_a, lambda_b=lambda_b, gain_a=gain_a, gain_b=gain_b, proj_a=proj_a, proj_b=proj_b, norm_gain=norm_gain, routes=routes, route_weight=route_weight, expert_gate=expert_gate, expert_up=expert_up, expert_down=expert_down)


EPS = 1e-06

def attend_group(queries, keys_all, values_all, mixing, head_gain, key_size):
    seq_rows = queries.shape[0]
    query_block = 512 if seq_rows % 512 == 0 else seq_rows
    positions = jnp.arange(seq_rows, dtype=jnp.int32)
    segment = positions // SEG
    factor = key_size ** (-0.5)
    keys_wide = keys_all.astype(jnp.float32)
    values_wide = values_all.astype(jnp.float32)

    def one_block(first_row):
        block_queries = lax.dynamic_slice_in_dim(queries, first_row, query_block, 0).astype(jnp.float32)
        block_segment = lax.dynamic_slice_in_dim(segment, first_row, query_block, 0)
        visible = block_segment[:, None] >= segment[None, :]

        def softmax_map(map_queries, map_keys):
            raw_scores = jnp.einsum('qhd,khd->hqk', map_queries, map_keys) * factor
            raw_scores = jnp.where(visible[None], raw_scores, -jnp.inf)
            largest = lax.optimization_barrier(jnp.max(raw_scores, axis=-1, keepdims=True))
            expo = jnp.exp(raw_scores - largest)
            return expo / lax.optimization_barrier(jnp.sum(expo, axis=-1, keepdims=True))
        first_probs = softmax_map(block_queries[..., :key_size], keys_wide[..., :key_size])
        second_probs = softmax_map(block_queries[..., key_size:], keys_wide[..., key_size:])
        weights = (first_probs - mixing[:, None, None] * second_probs).astype(jnp.bfloat16)
        mixed = jnp.einsum('hqk,khe->qhe', weights.astype(jnp.float32), values_wide)
        mean_sq = lax.optimization_barrier(jnp.mean(mixed * mixed, axis=-1, keepdims=True))
        return (mixed * lax.rsqrt(mean_sq + EPS) * head_gain).astype(jnp.bfloat16)
    starts = jnp.arange(seq_rows // query_block, dtype=jnp.int32) * query_block
    blocks = lax.map(one_block, starts)
    return blocks.reshape(seq_rows, -1)

def reference(residual, query_a, keys_a, values_a, query_b, keys_b, values_b, lambda_a, lambda_b, gain_a, gain_b, proj_a, proj_b, norm_gain, routes, route_weight, expert_gate, expert_up, expert_down):
    heads_a = attend_group(query_a, keys_a, values_a, lambda_a, gain_a, DK_A)
    heads_b = attend_group(query_b, keys_b, values_b, lambda_b, gain_b, DK_B)
    branch = jnp.dot(heads_a, proj_a, preferred_element_type=jnp.float32) + jnp.dot(heads_b, proj_b, preferred_element_type=jnp.float32)
    stream = (residual.astype(jnp.float32) + branch).astype(jnp.bfloat16)
    stream_wide = stream.astype(jnp.float32)
    mean_sq = lax.optimization_barrier(jnp.mean(stream_wide * stream_wide, axis=-1, keepdims=True))
    normed = (stream_wide * lax.rsqrt(mean_sq + EPS) * norm_gain).astype(jnp.bfloat16)
    assign = routes.reshape(N_SP, TOK_DEV * TOP)
    onehot = (assign[..., None] == jnp.arange(EXPERTS, dtype=jnp.int32)).astype(jnp.int32)
    earlier = jnp.cumsum(onehot, axis=1) - onehot
    slot_index = lax.optimization_barrier(jnp.sum(earlier * onehot, axis=-1))
    block_ids = jnp.arange(N_SP, dtype=jnp.int32)[:, None]
    target = ((block_ids * EXPERTS + assign) * CAP + slot_index).reshape(-1).astype(jnp.int32)
    token_ids = (jnp.arange(SEQ * TOP, dtype=jnp.int32) // TOP).astype(jnp.int32)
    buffer = jnp.zeros((N_SP * EXPERTS * CAP, D), jnp.bfloat16).at[target].set(normed[token_ids])
    grouped = buffer.reshape(N_SP, EXPERTS, CAP, D).transpose(1, 0, 2, 3).reshape(EXPERTS, N_SP * CAP, D)

    def one_expert(operands):
        rows, weight_gate, weight_up, weight_down = operands
        gate_val = jnp.dot(rows, weight_gate, preferred_element_type=jnp.float32)
        up_val = jnp.dot(rows, weight_up, preferred_element_type=jnp.float32)
        hidden = (jax.nn.silu(gate_val) * up_val).astype(jnp.bfloat16)
        hidden_blocks = hidden.reshape(rows.shape[0], N_TP, DFF // N_TP).astype(jnp.float32)
        down_blocks = weight_down.reshape(N_TP, DFF // N_TP, D).astype(jnp.float32)
        pieces = jnp.einsum('rjf,jfd->jrd', hidden_blocks, down_blocks)
        rounded = lax.optimization_barrier(pieces.astype(jnp.bfloat16))
        return lax.optimization_barrier(jnp.sum(rounded.astype(jnp.float32), axis=0)).astype(jnp.bfloat16)
    outputs = lax.map(one_expert, (grouped, expert_gate, expert_up, expert_down))
    flat_out = outputs.reshape(EXPERTS, N_SP, CAP, D).transpose(1, 0, 2, 3).reshape(-1, D)
    picked = flat_out[target].astype(jnp.float32).reshape(SEQ, TOP, D)
    gates = route_weight / lax.optimization_barrier(jnp.sum(route_weight, axis=-1, keepdims=True))
    experts_sum = lax.optimization_barrier(jnp.sum(gates[..., None] * picked, axis=1))
    return (stream_wide + experts_sum).astype(jnp.bfloat16)
```

```python
import jax
import jax.numpy as jnp
from jax import lax
from jax.experimental import pallas as pl
from jax.experimental.pallas import tpu as pltpu
from jax.sharding import PartitionSpec as P

SEG = 64
TOP = 2


EPS = 1e-06


def block_at(ref, index, split):
    if split == "lead":
        return ref.at[index]
    if split == "cols":
        width = ref.shape[-1] // lax.axis_size("tp")
        return ref.at[:, pl.ds(pl.multiple_of(index * width, width), width)]
    return ref


def exchange(array, out_shape, axis, source_split, target_split, collective_id):
    peers = lax.axis_size(axis)

    def kernel(in_ref, out_ref, send_sem, recv_sem):
        me = lax.axis_index(axis)
        barrier = pltpu.get_barrier_semaphore()
        for step in range(1, peers):
            pl.semaphore_signal(
                barrier,
                inc=1,
                device_id={axis: lax.rem(me + step, peers)},
                device_id_type=pl.DeviceIdType.MESH,
            )
        pl.semaphore_wait(barrier, peers - 1)
        copies = []
        for step in range(1, peers):
            peer = lax.rem(me + step, peers)
            copy = pltpu.make_async_remote_copy(
                src_ref=block_at(in_ref, peer, source_split),
                dst_ref=block_at(out_ref, me, target_split),
                send_sem=send_sem.at[step - 1],
                recv_sem=recv_sem.at[step - 1],
                device_id={axis: peer},
                device_id_type=pl.DeviceIdType.MESH,
            )
            copy.start()
            copies.append(copy)
        block_at(out_ref, me, target_split)[...] = block_at(in_ref, me, source_split)[...]
        for copy in copies:
            copy.wait()

    return pl.pallas_call(
        kernel,
        out_shape=jax.ShapeDtypeStruct(out_shape, array.dtype),
        in_specs=[pl.BlockSpec(memory_space=pltpu.VMEM)],
        out_specs=pl.BlockSpec(memory_space=pltpu.VMEM),
        scratch_shapes=[
            pltpu.SemaphoreType.DMA((peers - 1,)),
            pltpu.SemaphoreType.DMA((peers - 1,)),
        ],
        compiler_params=pltpu.CompilerParams(
            collective_id=collective_id, has_side_effects=True, vmem_limit_bytes=16 * 2**20
        ),
        name=f"exchange_{collective_id}",
    )(array)


def greet_peers():
    barrier = pltpu.get_barrier_semaphore()
    total = 0
    for axis in ("sp", "tp"):
        peers = lax.axis_size(axis)
        me = lax.axis_index(axis)
        for step in range(1, peers):
            pl.semaphore_signal(
                barrier,
                inc=1,
                device_id={axis: lax.rem(me + step, peers)},
                device_id_type=pl.DeviceIdType.MESH,
            )
        total += peers - 1
    pl.semaphore_wait(barrier, total)


def send_to(source, target, send_sem, recv_sem, axis, peer):
    copy = pltpu.make_async_remote_copy(
        src_ref=source,
        dst_ref=target,
        send_sem=send_sem,
        recv_sem=recv_sem,
        device_id={axis: peer},
        device_id_type=pl.DeviceIdType.MESH,
    )
    copy.start()
    return copy


def two_axis_call(kernel, array, out_shape, scratch, collective_id):
    seq, heads = lax.axis_size("sp"), lax.axis_size("tp")
    return pl.pallas_call(
        kernel,
        out_shape=jax.ShapeDtypeStruct(out_shape, array.dtype),
        in_specs=[pl.BlockSpec(memory_space=pltpu.VMEM)],
        out_specs=pl.BlockSpec(memory_space=pltpu.VMEM),
        scratch_shapes=list(scratch)
        + [
            pltpu.SemaphoreType.DMA((seq - 1,)),
            pltpu.SemaphoreType.DMA((seq - 1,)),
            pltpu.SemaphoreType.DMA((seq, heads - 1)),
            pltpu.SemaphoreType.DMA((seq, heads - 1)),
        ],
        compiler_params=pltpu.CompilerParams(
            collective_id=collective_id, has_side_effects=True, vmem_limit_bytes=24 * 2**20
        ),
        name=f"two_axis_{collective_id}",
    )(array)


def dispatch(send_rows, collective_id):
    seq, heads = lax.axis_size("sp"), lax.axis_size("tp")
    _, count, width = send_rows.shape

    def kernel(in_ref, out_ref, landed, seq_send, seq_recv, head_send, head_recv):
        seq_me, head_me = lax.axis_index("sp"), lax.axis_index("tp")
        greet_peers()
        first = []
        for step in range(1, seq):
            peer = lax.rem(seq_me + step, seq)
            first.append(
                send_to(
                    in_ref.at[peer],
                    landed.at[seq_me],
                    seq_send.at[step - 1],
                    seq_recv.at[step - 1],
                    "sp",
                    peer,
                )
            )
        second = []
        for step in range(seq):
            source = lax.rem(seq_me + seq - step, seq)
            if step:
                first[step - 1].wait_recv()
            block = landed.at[source] if step else in_ref.at[source]
            place = out_ref.at[
                pl.ds(pl.multiple_of(source * count, count), count),
                pl.ds(pl.multiple_of(head_me * width, width), width),
            ]
            for hop in range(1, heads):
                second.append(
                    send_to(
                        block,
                        place,
                        head_send.at[step, hop - 1],
                        head_recv.at[step, hop - 1],
                        "tp",
                        lax.rem(head_me + hop, heads),
                    )
                )
            place[...] = block[...]
        for copy in first:
            copy.wait_send()
        for copy in second:
            copy.wait()

    return two_axis_call(
        kernel,
        send_rows,
        (seq * count, heads * width),
        [pltpu.VMEM(send_rows.shape, send_rows.dtype)],
        collective_id,
    )


def sum_and_return(down_part, collective_id):
    seq, heads = lax.axis_size("sp"), lax.axis_size("tp")
    count, width = down_part.shape[0] // seq, down_part.shape[1] // heads

    def kernel(in_ref, out_ref, parts, sums, seq_send, seq_recv, head_send, head_recv):
        seq_me, head_me = lax.axis_index("sp"), lax.axis_index("tp")
        greet_peers()

        def piece(owner, column):
            return in_ref.at[
                pl.ds(pl.multiple_of(owner * count, count), count),
                pl.ds(pl.multiple_of(column * width, width), width),
            ]

        steps = list(range(1, seq)) + [0]
        first = {}
        for step in steps:
            owner = lax.rem(seq_me + step, seq)
            for hop in range(1, heads):
                peer = lax.rem(head_me + hop, heads)
                first[step, hop] = send_to(
                    piece(owner, peer),
                    parts.at[owner, head_me],
                    head_send.at[step, hop - 1],
                    head_recv.at[step, hop - 1],
                    "tp",
                    peer,
                )
        second = []
        for step in steps:
            owner = lax.rem(seq_me + step, seq)
            total = piece(owner, head_me)[...].astype(jnp.float32)
            for hop in range(1, heads):
                first[step, hop].wait_recv()
                giver = lax.rem(head_me + heads - hop, heads)
                total = total + parts[owner, giver].astype(jnp.float32)
            rounded = total.astype(out_ref.dtype)
            if step == 0:
                out_ref[owner] = rounded
            else:
                sums[owner] = rounded
                second.append(
                    send_to(
                        sums.at[owner],
                        out_ref.at[seq_me],
                        seq_send.at[step - 1],
                        seq_recv.at[step - 1],
                        "sp",
                        owner,
                    )
                )
        for step in steps:
            for hop in range(1, heads):
                first[step, hop].wait_send()
        for copy in second:
            copy.wait()

    return two_axis_call(
        kernel,
        down_part,
        (seq, count, width),
        [
            pltpu.VMEM((seq, heads, count, width), down_part.dtype),
            pltpu.VMEM((seq, count, width), down_part.dtype),
        ],
        collective_id,
    )


LOG2E = 1.4426950408889634
MESH = pl.DeviceIdType.MESH
F32 = jnp.float32
BF16 = jnp.bfloat16


def dot_nt(left, right):
    return lax.dot_general(left, right, (((1,), (1,)), ((), ())), preferred_element_type=F32)


def remote(source, target, send_sem, recv_sem, axis, peer):
    return pltpu.make_async_remote_copy(
        src_ref=source,
        dst_ref=target,
        send_sem=send_sem,
        recv_sem=recv_sem,
        device_id={axis: peer},
        device_id_type=MESH,
    )


def greet(axes):
    barrier = pltpu.get_barrier_semaphore()
    total = 0
    for axis in axes:
        peers = lax.axis_size(axis)
        me = lax.axis_index(axis)
        for step in range(1, peers):
            pl.semaphore_signal(
                barrier, inc=1, device_id={axis: lax.rem(me + step, peers)}, device_id_type=MESH
            )
        total += peers - 1
    pl.semaphore_wait(barrier, total)


def columns_of(stats):
    repeat = stats.shape[1] // stats.shape[0]
    return jnp.concatenate([stats] * repeat, axis=0).T


def rows_of(columns):
    rows = columns[0].shape[0]
    lane = lax.broadcasted_iota(jnp.int32, (rows, rows), 1)
    tile = jnp.zeros((rows, rows), F32)
    for at, column in enumerate(columns):
        tile = jnp.where(lane == at, column, tile)
    return tile.T[: len(columns)]


def attention(query_a, keys_a, values_a, query_b, keys_b, values_b, lambdas, gain_a, gain_b):
    seq = lax.axis_size("sp")
    rows, heads, width_a = query_a.shape
    width_b = query_b.shape[2]
    value_a, value_b = values_a.shape[2], values_b.shape[2]
    key_a, key_b = width_a // 2, width_b // 2
    chips = seq // 2
    half = chips // 2
    blocks = 2 * half
    wide_q = width_a + width_b
    wide_kv = width_a + value_a + width_b + value_b
    wide_o = value_a + value_b
    spans = ((0, width_a), (width_a + value_a, width_a + value_a + width_b))
    factors = (key_a ** (-0.5) * LOG2E, key_b ** (-0.5) * LOG2E)

    def kernel(
        lam, qa, ka, va, qb, kb, vb, gain_a, gain_b, out_a, out_b,
        kv, query, far_query, far_stats, own_stats, keep, part, far_part, total, far_total,
        chain_s, chain_r, part_s, part_r, query_s, query_r, stats_s, stats_r,
        back_s, back_r, total_s, total_r,
    ):
        me = lax.axis_index("sp")
        chip, core = me // 2, lax.rem(me, 2)
        upper = chip >= half
        place = lax.rem(chip, half)
        base = chip - place
        middle = 2 * (half - 1) + core
        is_middle = chip == half - 1
        partner = 2 * chip + 1 - core
        above = jnp.minimum(me + 2, seq - 1 - (1 - core))
        slot = 2 * place + core

        def chain(y, head):
            ref = kv.at[2 * y + core, head]
            return remote(ref, ref, chain_s.at[y, head], chain_r.at[y, head], "sp", above)

        def across(y, head):
            ref = kv.at[2 * y + core, head]
            return remote(ref, ref, part_s.at[y, head], part_r.at[y, head], "sp", partner)

        def ask(head):
            return remote(
                query.at[head], far_query.at[place, head], query_s.at[head],
                query_r.at[place, head], "sp", middle,
            )

        def tell(head):
            return remote(
                own_stats.at[head], far_stats.at[place, head], stats_s.at[head],
                stats_r.at[place, head], "sp", middle,
            )

        def answer(i, head):
            return remote(
                part.at[i, head], far_part.at[head], back_s.at[i, head], back_r.at[head],
                "sp", 2 * (half + i) + core,
            )

        def answer_total(i, head):
            return remote(
                total.at[i, head], far_total.at[head], total_s.at[i, head], total_r.at[head],
                "sp", 2 * (half + i) + core,
            )

        def asked(i, head):
            return remote(
                query.at[head], far_query.at[i, head], query_s.at[head],
                query_r.at[i, head], "sp", middle,
            )

        def told(i, head):
            return remote(
                own_stats.at[head], far_stats.at[i, head], stats_s.at[head],
                stats_r.at[i, head], "sp", middle,
            )

        greet(("sp",))

        def pack(head):
            query[head, :, :width_a] = qa[:, head, :]
            query[head, :, width_a:] = qb[:, head, :]
            kv[slot, head, :, :width_a] = ka[:, head, :]
            kv[slot, head, :, spans[0][1] : spans[1][0]] = va[:, head, :]
            kv[slot, head, :, spans[1][0] : spans[1][1]] = kb[:, head, :]
            kv[slot, head, :, spans[1][1] :] = vb[:, head, :]

        for head in range(heads):
            pack(head)

            @pl.when(upper)
            def _():
                ask(head).start()

            @pl.when(place < half - 1)
            def _():
                chain(place, head).start()

            across(place, head).start()

        def gather(here, head):
            for y in range(here):
                chain(y, head).wait_recv()
                across(y, head).start()
                if here < half - 1:
                    chain(y, head).start()
            for y in range(here + 1):
                across(y, head).wait_recv()

        def score_maps(ref, head, count):
            maps = []
            for group, (width, span) in enumerate(((width_a, spans[0][0]), (width_b, spans[1][0]))):
                begin = 0 if group == 0 else width_a
                wide = ref[:, begin : begin + width]
                block_keys = kv[:count, head, :, span : span + width].reshape(count * rows, width)
                size = width // 2
                if size % 128:
                    lane = lax.broadcasted_iota(jnp.int32, wide.shape, 1)
                    nothing = jnp.zeros_like(wide)
                    first = dot_nt(jnp.where(lane < size, wide, nothing), block_keys)
                    second = dot_nt(jnp.where(lane < size, nothing, wide), block_keys)
                else:
                    first = dot_nt(wide[:, :size], block_keys[:, :size])
                    second = dot_nt(wide[:, size:], block_keys[:, size:])
                maps += [first * factors[group], second * factors[group]]
            return maps

        def visible(count):
            query_seg = (
                slot * rows + lax.broadcasted_iota(jnp.int32, (rows, 1), 0)
            ) // SEG
            key_seg = lax.broadcasted_iota(jnp.int32, (1, count * rows), 1) // SEG
            return query_seg >= key_seg

        def combine(first, second, head, count, group):
            weights = (first - second).astype(BF16)
            begin = spans[group][1]
            size = value_a if group == 0 else value_b
            block_values = kv[:count, head, :, begin : begin + size].reshape(count * rows, size)
            return jnp.dot(weights, block_values, preferred_element_type=F32)

        def finish(mixed, gain, out, head, size):
            mean_sq = jnp.mean(mixed * mixed, axis=1, keepdims=True)
            value = (mixed * lax.rsqrt(mean_sq + EPS) * gain[...]).astype(BF16)
            out[:, pl.ds(pl.multiple_of(head * size, size), size)] = value

        def finish_both(mixed, head):
            finish(mixed[0], gain_a, out_a, head, value_a)
            finish(mixed[1], gain_b, out_b, head, value_b)

        def own_lower(head, count):
            seen = visible(count)
            maps = [jnp.where(seen, one, -jnp.inf) for one in score_maps(query.at[head], head, count)]
            mixed = []
            for group in range(2):
                parts = []
                for at in range(2):
                    scores = maps[2 * group + at]
                    expo = jnp.exp2(scores - jnp.max(scores, axis=1, keepdims=True))
                    scale = 1.0 / jnp.sum(expo, axis=1, keepdims=True)
                    if at:
                        scale = scale * lam[group, head]
                    parts.append(expo * scale)
                mixed.append(combine(parts[0], parts[1], head, count, group))
            finish_both(mixed, head)

        def for_upper(i, head):
            asked(i, head).wait_recv()
            maps = score_maps(far_query.at[i, head], head, blocks)
            told(i, head).wait_recv()
            far = columns_of(far_stats[i, head])
            stats = []
            for group in range(2):
                parts = []
                for at in range(2):
                    k = 2 * group + at
                    scores = maps[k]
                    far_max, far_sum = far[:, k : k + 1], far[:, 4 + k : 5 + k]
                    top = jnp.maximum(jnp.max(scores, axis=1, keepdims=True), far_max)
                    expo = jnp.exp2(scores - top)
                    summed = jnp.sum(expo, axis=1, keepdims=True) + far_sum * jnp.exp2(far_max - top)
                    stats.append((top, summed))
                    scale = 1.0 / summed
                    if at:
                        scale = scale * lam[group, head]
                    parts.append(expo * scale)
                mixed = combine(parts[0], parts[1], head, blocks, group)
                begin = 0 if group == 0 else value_a
                part[i, head, :, begin : begin + mixed.shape[1]] = mixed.astype(BF16)
            answer(i, head).start()
            total[i, head] = rows_of([one[0] for one in stats] + [one[1] for one in stats])
            answer_total(i, head).start()

        def upper_first(head, count):
            seen = visible(count)
            maps = [jnp.where(seen, one, -jnp.inf) for one in score_maps(query.at[head], head, count)]
            tops, sums = [], []
            for k in range(4):
                top = jnp.max(maps[k], axis=1, keepdims=True)
                expo = jnp.exp2(maps[k] - top)
                keep[head, k, :, : count * rows] = expo
                tops.append(top)
                sums.append(jnp.sum(expo, axis=1, keepdims=True))
            own_stats[head] = rows_of(tops + sums)
            tell(head).start()

        def upper_second(head, count):
            answer_total(0, head).wait_recv()
            own = columns_of(own_stats[head])
            whole = columns_of(far_total[head])
            scales = []
            for k in range(4):
                scale = jnp.exp2(own[:, k : k + 1] - whole[:, k : k + 1]) / whole[:, 4 + k : 5 + k]
                if k % 2:
                    scale = scale * lam[k // 2, head]
                scales.append(scale)
            mixed = []
            for group in range(2):
                first = keep[head, 2 * group, :, : count * rows] * scales[2 * group]
                second = keep[head, 2 * group + 1, :, : count * rows] * scales[2 * group + 1]
                mixed.append(combine(first, second, head, count, group))
            answer(0, head).wait_recv()
            far = far_part[head].astype(F32)
            finish_both([mixed[0] + far[:, :value_a], mixed[1] + far[:, value_a:]], head)

        for here in range(half):

            @pl.when((place == here) & jnp.logical_not(upper))
            def _():
                def step(head, carry):
                    gather(here, head)
                    own_lower(head, 2 * here + 2)
                    if here == half - 1:

                        def each(i, inner):
                            for_upper(i, head)
                            return inner

                        lax.fori_loop(0, half, each, 0)
                    return carry

                lax.fori_loop(0, heads, step, 0)

            @pl.when((place == here) & upper)
            def _():
                def step(head, carry):
                    gather(here, head)
                    upper_first(head, 2 * here + 2)
                    return carry

                lax.fori_loop(0, heads, step, 0)

                def second(head, carry):
                    upper_second(head, 2 * here + 2)
                    return carry

                lax.fori_loop(0, heads, second, 0)

            @pl.when(place == here)
            def _():
                def drain(head, carry):
                    for y in range(here + 1):
                        across(y, head).wait_send()
                        if here < half - 1:
                            chain(y, head).wait_send()
                    return carry

                lax.fori_loop(0, heads, drain, 0)

        @pl.when(upper)
        def _():
            def drain(head, carry):
                ask(head).wait_send()
                tell(head).wait_send()
                return carry

            lax.fori_loop(0, heads, drain, 0)

        @pl.when(is_middle)
        def _():
            def drain(head, carry):
                for i in range(half):
                    answer(i, head).wait_send()
                    answer_total(i, head).wait_send()
                return carry

            lax.fori_loop(0, heads, drain, 0)

    vmem = pl.BlockSpec(memory_space=pltpu.VMEM)
    dma = pltpu.SemaphoreType.DMA
    return pl.pallas_call(
        kernel,
        out_shape=(
            jax.ShapeDtypeStruct((rows, heads * value_a), BF16),
            jax.ShapeDtypeStruct((rows, heads * value_b), BF16),
        ),
        in_specs=[pl.BlockSpec(memory_space=pltpu.SMEM)] + [vmem] * 8,
        out_specs=(vmem, vmem),
        scratch_shapes=[
            pltpu.VMEM((blocks, heads, rows, wide_kv), BF16),
            pltpu.VMEM((heads, rows, wide_q), BF16),
            pltpu.VMEM((half, heads, rows, wide_q), BF16),
            pltpu.VMEM((half, heads, 8, rows), F32),
            pltpu.VMEM((heads, 8, rows), F32),
            pltpu.VMEM((heads, 4, rows, blocks * rows), F32),
            pltpu.VMEM((half, heads, rows, wide_o), BF16),
            pltpu.VMEM((heads, rows, wide_o), BF16),
            pltpu.VMEM((half, heads, 8, rows), F32),
            pltpu.VMEM((heads, 8, rows), F32),
            dma((half, heads)), dma((half, heads)), dma((half, heads)), dma((half, heads)),
            dma((heads,)), dma((half, heads)), dma((heads,)), dma((half, heads)),
            dma((half, heads)), dma((heads,)), dma((half, heads)), dma((heads,)),
        ],
        compiler_params=pltpu.CompilerParams(
            collective_id=4, has_side_effects=True, vmem_limit_bytes=40 * 2**20
        ),
        name="attention",
    )(
        lambdas, query_a, keys_a, values_a, query_b, keys_b, values_b,
        gain_a.reshape(1, -1), gain_b.reshape(1, -1),
    )


def local(
    residual,
    query_a,
    keys_a,
    values_a,
    query_b,
    keys_b,
    values_b,
    lambda_a,
    lambda_b,
    gain_a,
    gain_b,
    proj_a,
    proj_b,
    norm_gain,
    routes,
    route_weight,
    expert_gate,
    expert_up,
    expert_down,
):
    tok_rows = residual.shape[0]
    model_width = residual.shape[1]
    seq_devices = lax.axis_size("sp")
    head_devices = lax.axis_size("tp")
    head_index = lax.axis_index("tp")
    heads_a, heads_b = attention(
        query_a,
        keys_a,
        values_a,
        query_b,
        keys_b,
        values_b,
        jnp.stack([lambda_a, lambda_b]),
        gain_a,
        gain_b,
    )
    partial_branch = jnp.dot(
        heads_a, proj_a, preferred_element_type=jnp.float32
    )
    partial_branch = partial_branch + jnp.dot(
        heads_b, proj_b, preferred_element_type=jnp.float32
    )
    columns = model_width // head_devices
    col_start = head_index * columns
    branch_parts = exchange(
        partial_branch.astype(jnp.bfloat16),
        (head_devices, tok_rows, columns),
        "tp",
        "cols",
        "lead",
        0,
    )
    summed_cols = jnp.sum(branch_parts.astype(jnp.float32), axis=0)
    residual_cols = lax.dynamic_slice_in_dim(residual, col_start, columns, 1)
    stream_cols = (
        (residual_cols.astype(jnp.float32) + summed_cols).astype(jnp.bfloat16).astype(jnp.float32)
    )
    own_squares = jnp.broadcast_to(jnp.sum(stream_cols * stream_cols, axis=1)[None], (8, tok_rows))
    squares = jnp.sum(
        exchange(own_squares, (head_devices, 8, tok_rows), "tp", "all", "lead", 1)[:, 0], axis=0
    )
    row_scale = lax.rsqrt(squares / model_width + EPS)
    gain_cols = lax.dynamic_slice_in_dim(norm_gain, col_start, columns, 0)
    normed_cols = (stream_cols * row_scale[:, None] * gain_cols).astype(jnp.bfloat16)
    slot_count = 2 * tok_rows * TOP // seq_devices
    assign = routes.reshape(-1)
    onehot = (assign[:, None] == jnp.arange(seq_devices, dtype=jnp.int32)[None, :]).astype(
        jnp.int32
    )
    earlier = jnp.cumsum(onehot, axis=0) - onehot
    slot_index = jnp.sum(earlier * onehot, axis=1)
    target = assign * slot_count + slot_index
    placed = (
        target[:, None] == jnp.arange(seq_devices * slot_count, dtype=jnp.int32)[None, :]
    ).reshape(tok_rows, TOP, -1)
    select = jnp.sum(placed.astype(jnp.bfloat16), axis=1)
    gates = route_weight / jnp.sum(route_weight, axis=1, keepdims=True)
    combine = jnp.sum(placed.astype(jnp.float32) * gates[:, :, None], axis=1)
    send_rows = jnp.einsum(
        "ts,td->sd", select, normed_cols, preferred_element_type=jnp.float32
    ).astype(jnp.bfloat16)
    send_rows = send_rows.reshape(seq_devices, slot_count, columns)
    flat_rows = dispatch(send_rows, 2)
    gate_val = jnp.dot(flat_rows, expert_gate[0], preferred_element_type=jnp.float32)
    up_val = jnp.dot(flat_rows, expert_up[0], preferred_element_type=jnp.float32)
    hidden = (jax.nn.silu(gate_val) * up_val).astype(jnp.bfloat16)
    down_part = jnp.dot(hidden, expert_down[0], preferred_element_type=jnp.float32)
    returned = sum_and_return(down_part.astype(jnp.bfloat16), 3)
    returned_flat = returned.reshape(seq_devices * slot_count, columns).astype(jnp.float32)
    experts_sum = jnp.dot(combine, returned_flat, precision=lax.Precision.HIGHEST)
    return (stream_cols + experts_sum).astype(jnp.bfloat16)


def solution(mesh):
    placed = (
        P("sp", None),
        P("sp", "tp", None),
        P("sp", "tp", None),
        P("sp", "tp", None),
        P("sp", "tp", None),
        P("sp", "tp", None),
        P("sp", "tp", None),
        P("tp"),
        P("tp"),
        P(),
        P(),
        P("tp", None),
        P("tp", None),
        P(),
        P("sp", None),
        P("sp", None),
        P("sp", None, "tp"),
        P("sp", None, "tp"),
        P("sp", "tp", None),
    )
    return jax.shard_map(
        local, mesh=mesh, in_specs=placed, out_specs=P("sp", "tp"), check_vma=False
    )
```

```python
import math

import jax
import jax.numpy as jnp
from jax import lax
from jax.experimental import pallas as pl
from jax.experimental.pallas import tpu as pltpu
from jax.sharding import PartitionSpec as P

SEG = 64
TOP = 2
EPS = 1e-06

LOG2E = 1.4426950408889634
MESH = pl.DeviceIdType.MESH
F32 = jnp.float32
BF16 = jnp.bfloat16


def dot_nt(left, right):
    return lax.dot_general(left, right, (((1,), (1,)), ((), ())), preferred_element_type=F32)


def remote(source, target, send_sem, recv_sem, axis, peer):
    return pltpu.make_async_remote_copy(
        src_ref=source,
        dst_ref=target,
        send_sem=send_sem,
        recv_sem=recv_sem,
        device_id={axis: peer},
        device_id_type=MESH,
    )


def greet(axes):
    barrier = pltpu.get_barrier_semaphore()
    total = 0
    for axis in axes:
        peers = lax.axis_size(axis)
        me = lax.axis_index(axis)
        for step in range(1, peers):
            pl.semaphore_signal(
                barrier, inc=1, device_id={axis: lax.rem(me + step, peers)}, device_id_type=MESH
            )
        total += peers - 1
    pl.semaphore_wait(barrier, total)


def columns_of(stats):
    repeat = stats.shape[1] // stats.shape[0]
    return jnp.concatenate([stats] * repeat, axis=0).T


def rows_of(columns):
    rows = columns[0].shape[0]
    lane = lax.broadcasted_iota(jnp.int32, (rows, rows), 1)
    tile = jnp.zeros((rows, rows), F32)
    for at, column in enumerate(columns):
        tile = jnp.where(lane == at, column, tile)
    return tile.T[: len(columns)]


class Refs:
    def __init__(self, names, refs):
        for name, ref in zip(names, refs):
            setattr(self, name, ref)


def attend(r, arrived):
    seq = lax.axis_size("sp")
    rows, heads, width_a = r.qa.shape
    width_b = r.qb.shape[2]
    value_a, value_b = r.va.shape[2], r.vb.shape[2]
    key_a, key_b = width_a // 2, width_b // 2
    chips = seq // 2
    half = chips // 2
    blocks = 2 * half
    spans = ((0, width_a), (width_a + value_a, width_a + value_a + width_b))
    factors = (key_a ** (-0.5) * LOG2E, key_b ** (-0.5) * LOG2E)
    lam, qa, ka, va, qb, kb, vb = r.lam, r.qa, r.ka, r.va, r.qb, r.kb, r.vb
    gain_a, gain_b, out_a, out_b = r.gain_a, r.gain_b, r.heads_a, r.heads_b
    kv, query, far_query, far_stats, own_stats = r.kv, r.query, r.far_query, r.far_stats, r.own_stats
    keep, part, far_part, total, far_total = r.keep, r.part, r.far_part, r.total, r.far_total
    chain_s, chain_r, part_s, part_r = r.chain_s, r.chain_r, r.part_s, r.part_r
    query_s, query_r, stats_s, stats_r = r.query_s, r.query_r, r.stats_s, r.stats_r
    back_s, back_r, total_s, total_r = r.back_s, r.back_r, r.total_s, r.total_r
    me = lax.axis_index("sp")
    chip, core = me // 2, lax.rem(me, 2)
    upper = chip >= half
    place = lax.rem(chip, half)
    base = chip - place
    middle = 2 * (half - 1) + core
    is_middle = chip == half - 1
    partner = 2 * chip + 1 - core
    above = jnp.minimum(me + 2, seq - 1 - (1 - core))
    slot = 2 * place + core

    def chain(y, head):
        ref = kv.at[2 * y + core, head]
        return remote(ref, ref, chain_s.at[y, head], chain_r.at[y, head], "sp", above)

    def across(y, head):
        ref = kv.at[2 * y + core, head]
        return remote(ref, ref, part_s.at[y, head], part_r.at[y, head], "sp", partner)

    def ask(head):
        return remote(
            query.at[head], far_query.at[place, head], query_s.at[head],
            query_r.at[place, head], "sp", middle,
        )

    def tell(head):
        return remote(
            own_stats.at[head], far_stats.at[place, head], stats_s.at[head],
            stats_r.at[place, head], "sp", middle,
        )

    def answer(i, head):
        return remote(
            part.at[i, head], far_part.at[head], back_s.at[i, head], back_r.at[head],
            "sp", 2 * (half + i) + core,
        )

    def answer_total(i, head):
        return remote(
            total.at[i, head], far_total.at[head], total_s.at[i, head], total_r.at[head],
            "sp", 2 * (half + i) + core,
        )

    def asked(i, head):
        return remote(
            query.at[head], far_query.at[i, head], query_s.at[head],
            query_r.at[i, head], "sp", middle,
        )

    def told(i, head):
        return remote(
            own_stats.at[head], far_stats.at[i, head], stats_s.at[head],
            stats_r.at[i, head], "sp", middle,
        )

    def pack(head):
        query[head, :, :width_a] = qa[:, head, :]
        query[head, :, width_a:] = qb[:, head, :]
        kv[slot, head, :, :width_a] = ka[:, head, :]
        kv[slot, head, :, spans[0][1] : spans[1][0]] = va[:, head, :]
        kv[slot, head, :, spans[1][0] : spans[1][1]] = kb[:, head, :]
        kv[slot, head, :, spans[1][1] :] = vb[:, head, :]

    arrived()
    for head in range(heads):
        pack(head)

        @pl.when(upper)
        def _():
            ask(head).start()

        @pl.when(place < half - 1)
        def _():
            chain(place, head).start()

        across(place, head).start()

    def gather(here, head):
        for y in range(here):
            chain(y, head).wait_recv()
            across(y, head).start()
            if here < half - 1:
                chain(y, head).start()
        for y in range(here + 1):
            across(y, head).wait_recv()

    def score_maps(ref, head, count):
        maps = []
        for group, (width, span) in enumerate(((width_a, spans[0][0]), (width_b, spans[1][0]))):
            begin = 0 if group == 0 else width_a
            wide = ref[:, begin : begin + width]
            block_keys = kv[:count, head, :, span : span + width].reshape(count * rows, width)
            size = width // 2
            if size % 128:
                lane = lax.broadcasted_iota(jnp.int32, wide.shape, 1)
                nothing = jnp.zeros_like(wide)
                first = dot_nt(jnp.where(lane < size, wide, nothing), block_keys)
                second = dot_nt(jnp.where(lane < size, nothing, wide), block_keys)
            else:
                first = dot_nt(wide[:, :size], block_keys[:, :size])
                second = dot_nt(wide[:, size:], block_keys[:, size:])
            maps += [first * factors[group], second * factors[group]]
        return maps

    def visible(count):
        query_seg = (
            slot * rows + lax.broadcasted_iota(jnp.int32, (rows, 1), 0)
        ) // SEG
        key_seg = lax.broadcasted_iota(jnp.int32, (1, count * rows), 1) // SEG
        return query_seg >= key_seg

    def combine(first, second, head, count, group):
        weights = (first - second).astype(BF16)
        begin = spans[group][1]
        size = value_a if group == 0 else value_b
        block_values = kv[:count, head, :, begin : begin + size].reshape(count * rows, size)
        return jnp.dot(weights, block_values, preferred_element_type=F32)

    def finish(mixed, gain, out, head, size):
        mean_sq = jnp.mean(mixed * mixed, axis=1, keepdims=True)
        value = (mixed * lax.rsqrt(mean_sq + EPS) * gain[...]).astype(BF16)
        out[:, pl.ds(pl.multiple_of(head * size, size), size)] = value

    def finish_both(mixed, head):
        finish(mixed[0], gain_a, out_a, head, value_a)
        finish(mixed[1], gain_b, out_b, head, value_b)

    def own_lower(head, count):
        seen = visible(count)
        maps = [jnp.where(seen, one, -jnp.inf) for one in score_maps(query.at[head], head, count)]
        mixed = []
        for group in range(2):
            parts = []
            for at in range(2):
                scores = maps[2 * group + at]
                expo = jnp.exp2(scores - jnp.max(scores, axis=1, keepdims=True))
                scale = 1.0 / jnp.sum(expo, axis=1, keepdims=True)
                if at:
                    scale = scale * lam[group, head]
                parts.append(expo * scale)
            mixed.append(combine(parts[0], parts[1], head, count, group))
        finish_both(mixed, head)

    def for_upper(i, head):
        asked(i, head).wait_recv()
        maps = score_maps(far_query.at[i, head], head, blocks)
        told(i, head).wait_recv()
        far = columns_of(far_stats[i, head])
        stats = []
        for group in range(2):
            parts = []
            for at in range(2):
                k = 2 * group + at
                scores = maps[k]
                far_max, far_sum = far[:, k : k + 1], far[:, 4 + k : 5 + k]
                top = jnp.maximum(jnp.max(scores, axis=1, keepdims=True), far_max)
                expo = jnp.exp2(scores - top)
                summed = jnp.sum(expo, axis=1, keepdims=True) + far_sum * jnp.exp2(far_max - top)
                stats.append((top, summed))
                scale = 1.0 / summed
                if at:
                    scale = scale * lam[group, head]
                parts.append(expo * scale)
            mixed = combine(parts[0], parts[1], head, blocks, group)
            begin = 0 if group == 0 else value_a
            part[i, head, :, begin : begin + mixed.shape[1]] = mixed.astype(BF16)
        answer(i, head).start()
        total[i, head] = rows_of([one[0] for one in stats] + [one[1] for one in stats])
        answer_total(i, head).start()

    def upper_first(head, count):
        seen = visible(count)
        maps = [jnp.where(seen, one, -jnp.inf) for one in score_maps(query.at[head], head, count)]
        tops, sums = [], []
        for k in range(4):
            top = jnp.max(maps[k], axis=1, keepdims=True)
            expo = jnp.exp2(maps[k] - top)
            keep[head, k, :, : count * rows] = expo
            tops.append(top)
            sums.append(jnp.sum(expo, axis=1, keepdims=True))
        own_stats[head] = rows_of(tops + sums)
        tell(head).start()

    def upper_second(head, count):
        answer_total(0, head).wait_recv()
        own = columns_of(own_stats[head])
        whole = columns_of(far_total[head])
        scales = []
        for k in range(4):
            scale = jnp.exp2(own[:, k : k + 1] - whole[:, k : k + 1]) / whole[:, 4 + k : 5 + k]
            if k % 2:
                scale = scale * lam[k // 2, head]
            scales.append(scale)
        mixed = []
        for group in range(2):
            first = keep[head, 2 * group, :, : count * rows] * scales[2 * group]
            second = keep[head, 2 * group + 1, :, : count * rows] * scales[2 * group + 1]
            mixed.append(combine(first, second, head, count, group))
        answer(0, head).wait_recv()
        far = far_part[head].astype(F32)
        finish_both([mixed[0] + far[:, :value_a], mixed[1] + far[:, value_a:]], head)

    for here in range(half):

        @pl.when((place == here) & jnp.logical_not(upper))
        def _():
            def step(head, carry):
                gather(here, head)
                own_lower(head, 2 * here + 2)
                if here == half - 1:

                    def each(i, inner):
                        for_upper(i, head)
                        return inner

                    lax.fori_loop(0, half, each, 0)
                return carry

            lax.fori_loop(0, heads, step, 0)

        @pl.when((place == here) & upper)
        def _():
            def step(head, carry):
                gather(here, head)
                upper_first(head, 2 * here + 2)
                return carry

            lax.fori_loop(0, heads, step, 0)

            def second(head, carry):
                upper_second(head, 2 * here + 2)
                return carry

            lax.fori_loop(0, heads, second, 0)

        @pl.when(place == here)
        def _():
            def drain(head, carry):
                for y in range(here + 1):
                    across(y, head).wait_send()
                    if here < half - 1:
                        chain(y, head).wait_send()
                return carry

            lax.fori_loop(0, heads, drain, 0)

    @pl.when(upper)
    def _():
        def drain(head, carry):
            ask(head).wait_send()
            tell(head).wait_send()
            return carry

        lax.fori_loop(0, heads, drain, 0)

    @pl.when(is_middle)
    def _():
        def drain(head, carry):
            for i in range(half):
                answer(i, head).wait_send()
                answer_total(i, head).wait_send()
            return carry

        lax.fori_loop(0, heads, drain, 0)


def grid_of(count):
    side = math.isqrt(count)
    return (side, side) if side * side == count else (1, count)


def peer_at(dy, dx):
    ny, nx = grid_of(lax.axis_size("tp"))
    me = lax.axis_index("tp")
    return lax.rem(me // nx + dy, ny) * nx + lax.rem(lax.rem(me, nx) + dx, nx)


def peer_offsets():
    ny, nx = grid_of(lax.axis_size("tp"))
    offsets = [(dy, dx) for dy in range(ny) for dx in range(nx) if dy or dx]
    far = lambda one: min(one[0], ny - one[0]) + min(one[1], nx - one[1])
    return sorted(offsets, key=far, reverse=True), ny, nx


def block_of(index, width):
    return pl.ds(pl.multiple_of(index * width, width), width)


def route(r):
    experts, slots, rows = r.select.shape
    square = (rows, rows)
    lane = lax.broadcasted_iota(jnp.int32, square, 1)
    line = lax.broadcasted_iota(jnp.int32, square, 0)
    named = r.routes[...]
    weight = r.route_weight[...]
    share = weight / jnp.sum(weight, axis=1, keepdims=True)
    chosen = jnp.zeros(square, F32)
    gate = jnp.zeros(square, F32)
    for k in range(TOP):
        match = named[:, k : k + 1] == lane
        chosen = chosen + jnp.where(match, 1.0, 0.0)
        gate = gate + jnp.where(match, share[:, k : k + 1], 0.0)
    chosen, gate = chosen.T, gate.T
    earlier = jnp.dot(
        chosen.astype(BF16),
        jnp.where(line < lane, 1.0, 0.0).astype(BF16),
        preferred_element_type=F32,
    )
    slot = lax.broadcasted_iota(jnp.int32, (slots, rows), 0).astype(F32)
    for expert in range(experts):
        pick = (chosen[expert : expert + 1] > 0.5) & (earlier[expert : expert + 1] == slot)
        r.select[expert] = jnp.where(pick, 1.0, 0.0).astype(BF16)
        r.weigh[expert * slots : (expert + 1) * slots, :] = jnp.where(
            pick, gate[expert : expert + 1], 0.0
        )
    weigh = r.weigh[...].T
    high = weigh.astype(BF16)
    r.high[...] = high
    r.low[...] = (weigh - high.astype(F32)).astype(BF16)


def project(r, loaded):
    offsets, _, _ = peer_offsets()
    me = lax.axis_index("tp")
    width = r.stream.shape[1]

    def piece(owner):
        columns = block_of(owner, width)
        return jnp.dot(
            r.heads_a[...], r.proj_a[:, columns], preferred_element_type=F32
        ) + jnp.dot(r.heads_b[...], r.proj_b[:, columns], preferred_element_type=F32)

    loaded()
    copies = []
    for at, offset in enumerate(offsets):
        peer = peer_at(*offset)
        r.branch_out[at] = piece(peer).astype(BF16)
        copy = remote(
            r.branch_out.at[at], r.branch_in.at[at], r.branch_s.at[at], r.branch_r.at[at], "tp", peer
        )
        copy.start()
        copies.append(copy)
    summed = piece(me)
    for at, copy in reversed(list(enumerate(copies))):
        copy.wait_recv()
        summed = summed + r.branch_in[at].astype(F32)
    r.stream[...] = (r.residual[...].astype(F32) + summed).astype(BF16)
    return copies


def experts_part(r, loaded):
    offsets, ny, nx = peer_offsets()
    seq, heads = lax.axis_size("sp"), lax.axis_size("tp")
    me, mine = lax.axis_index("sp"), lax.axis_index("tp")
    chips = seq // 2
    chip, core = me // 2, lax.rem(me, 2)
    experts, slots, rows = r.select.shape
    width = r.stream.shape[1]
    square = ny == 2 and nx == 2
    across_x, across_y, across_both = peer_at(0, 1), peer_at(1, 0), peer_at(1, 1)
    top, bottom = pl.ds(0, slots), pl.ds(slots, slots)

    def source(step):
        return lax.rem(chip + chips - step, chips)

    def outgoing(step, side):
        target_core = core if side == 0 else 1 - core
        expert = 2 * lax.rem(chip + step, chips) + target_core
        return expert, remote(
            r.send.at[expert],
            r.rows.at[chip, block_of(core, slots), block_of(mine, width)],
            r.out_s.at[step, side],
            r.out_r.at[step, side],
            "sp",
            expert,
        )

    for step in range(chips):
        for side in range(2):
            expert, copy = outgoing(step, side)
            picked = jnp.dot(r.select[expert], r.stream[...], preferred_element_type=F32)
            if step == 0 and side == 0:
                r.rows[chip, block_of(core, slots), block_of(mine, width)] = picked.astype(BF16)
            else:
                r.send[expert] = picked.astype(BF16)
                copy.start()

    def incoming(step, side):
        origin_core = core if side == 0 else 1 - core
        origin = source(step)
        return remote(
            r.send.at[me],
            r.rows.at[origin, block_of(origin_core, slots), block_of(mine, width)],
            r.out_s.at[step, side],
            r.out_r.at[step, side],
            "sp",
            2 * origin + origin_core,
        )

    def land(step):
        @pl.when(step > 0)
        def _():
            incoming(step, 0).wait_recv()

        incoming(step, 1).wait_recv()

    def spread(step, at, peer, owner):
        ref = r.rows.at[source(step), :, block_of(owner, width)]
        return remote(ref, ref, r.spread_s.at[step, at], r.spread_r.at[step, at], "tp", peer)

    def relay(step, at, peer, owner):
        ref = r.rows.at[source(step), top if at == 0 else bottom, block_of(owner, width)]
        return remote(ref, ref, r.relay_s.at[step, at], r.relay_r.at[step, at], "tp", peer)

    near = ((0, 1), (1, 0)) if square else offsets

    def start_spread(step):
        land(step)
        for at, offset in enumerate(near):
            spread(step, at, peer_at(*offset), mine).start()

    def start_relay(step):
        for at, offset in enumerate(near):
            giver = peer_at(ny - offset[0], nx - offset[1])
            spread(step, at, giver, giver).wait_recv()
        if square:
            relay(step, 0, across_y, across_x).start()
            relay(step, 1, across_x, across_y).start()

    def compute(step):
        if square:
            relay(step, 0, across_y, across_both).wait_recv()
            relay(step, 1, across_x, across_both).wait_recv()
        origin = source(step)
        wide = r.rows[origin].astype(F32)
        mean_sq = jnp.mean(wide * wide, axis=1, keepdims=True)
        normed = (wide * lax.rsqrt(mean_sq + EPS) * r.norm_gain[...]).astype(BF16)
        gate = jnp.dot(normed, r.gate[...], preferred_element_type=F32)
        up = jnp.dot(normed, r.up[...], preferred_element_type=F32)
        hidden = (gate / (1.0 + jnp.exp(-gate)) * up).astype(BF16)
        r.down_out[step] = jnp.dot(hidden, r.down[...], preferred_element_type=F32).astype(BF16)

    def first_copies(step):
        if not square:
            return [
                remote(
                    r.down_out.at[step, :, block_of(peer_at(*offset), width)],
                    r.first.at[step, at],
                    r.first_s.at[step, at],
                    r.first_r.at[step, at],
                    "tp",
                    peer_at(*offset),
                )
                for at, offset in enumerate(offsets)
            ]
        plan = (
            (top, across_x, across_both, 1),
            (bottom, across_y, across_both, 3),
            (top, across_x, across_x, 0),
            (bottom, across_y, across_y, 2),
        )
        return [
            remote(
                r.down_out.at[step, part, block_of(owner, width)],
                r.first.at[step, slot],
                r.first_s.at[step, slot],
                r.first_r.at[step, slot],
                "tp",
                peer,
            )
            for part, peer, owner, slot in plan
        ]

    def second_copies(step):
        return [
            remote(
                r.second_out.at[step, at],
                r.second.at[step, at],
                r.second_s.at[step, at],
                r.second_r.at[step, at],
                "tp",
                peer,
            )
            for at, peer in enumerate((across_y, across_x))
        ]

    def start_first(step):
        for copy in first_copies(step):
            copy.start()

    def start_second(step):
        if not square:
            return
        firsts, seconds = first_copies(step), second_copies(step)
        for at, part, owner, slot in ((0, top, across_y, 1), (1, bottom, across_x, 3)):
            firsts[at].wait_recv()
            summed = r.down_out[step, part, block_of(owner, width)].astype(F32)
            summed = summed + r.first[step, slot].astype(F32)
            r.second_out[step, at] = summed.astype(BF16)
            seconds[at].start()

    def home(step, side):
        origin_core = core if side == 0 else 1 - core
        return remote(
            r.summed.at[step, side],
            r.back.at[me],
            r.home_s.at[step, side],
            r.home_r.at[step, side],
            "sp",
            2 * source(step) + origin_core,
        )

    def returned(step, side):
        expert_core = core if side == 0 else 1 - core
        expert = 2 * lax.rem(chip + step, chips) + expert_core
        return remote(
            r.summed.at[step, side],
            r.back.at[expert],
            r.home_s.at[step, side],
            r.home_r.at[step, side],
            "sp",
            expert,
        )

    def start_home(step):
        own = block_of(mine, width)
        firsts = first_copies(step)
        if square:
            seconds = second_copies(step)
            firsts[2].wait_recv()
            firsts[3].wait_recv()
            halves = []
            for at, part, slot in ((0, top, 0), (1, bottom, 2)):
                seconds[at].wait_recv()
                halves.append(
                    r.down_out[step, part, own].astype(F32)
                    + r.first[step, slot].astype(F32)
                    + r.second[step, at].astype(F32)
                )
            r.sums[0] = halves[0].astype(BF16)
            r.sums[1] = halves[1].astype(BF16)
        else:
            summed = r.down_out[step, :, own].astype(F32)
            for at, copy in enumerate(firsts):
                copy.wait_recv()
                summed = summed + r.first[step, at].astype(F32)
            r.sums[0] = summed[:slots].astype(BF16)
            r.sums[1] = summed[slots:].astype(BF16)
        r.summed[step, 0] = r.sums[core]
        r.summed[step, 1] = r.sums[1 - core]

        @pl.when(step == 0)
        def _():
            r.back[me] = r.summed[0, 0]

        @pl.when(step > 0)
        def _():
            home(step, 0).start()

        home(step, 1).start()

    loaded()
    start_spread(0)
    if chips > 1:
        start_spread(1)
    start_relay(0)

    def body(step, carry):
        @pl.when(step + 2 < chips)
        def _():
            start_spread(step + 2)

        @pl.when(step + 1 < chips)
        def _():
            start_relay(step + 1)

        @pl.when(step < chips)
        def _():
            compute(step)
            start_first(step)

        @pl.when((step >= 1) & (step < chips + 1))
        def _():
            start_second(step - 1)

        @pl.when(step >= 2)
        def _():
            start_home(step - 2)

        return carry

    lax.fori_loop(0, chips + 2, body, 0)

    def arrive(step, carry):
        @pl.when(step > 0)
        def _():
            returned(step, 0).wait_recv()

        returned(step, 1).wait_recv()
        return carry

    lax.fori_loop(0, chips, arrive, 0)
    back = r.back[...].reshape(experts * slots, width)
    mixed = jnp.dot(r.high[...], back, preferred_element_type=F32)
    mixed = mixed + jnp.dot(r.low[...], back, preferred_element_type=F32)
    r.out[...] = (r.stream[...].astype(F32) + mixed).astype(BF16)

    def drain(step, carry):
        @pl.when(step > 0)
        def _():
            outgoing(step, 0)[1].wait_send()
            home(step, 0).wait_send()

        outgoing(step, 1)[1].wait_send()
        home(step, 1).wait_send()
        for at, offset in enumerate(near):
            spread(step, at, peer_at(*offset), mine).wait_send()
        if square:
            relay(step, 0, across_y, across_x).wait_send()
            relay(step, 1, across_x, across_y).wait_send()
            for copy in second_copies(step):
                copy.wait_send()
        for copy in first_copies(step):
            copy.wait_send()
        return carry

    lax.fori_loop(0, chips, drain, 0)


def layer(args):
    seq, heads_dev = lax.axis_size("sp"), lax.axis_size("tp")
    rows, heads, width_a = args["qa"].shape
    width_b = args["qb"].shape[2]
    value_a, value_b = args["va"].shape[2], args["vb"].shape[2]
    model = args["residual"].shape[1]
    width = model // heads_dev
    chips = seq // 2
    half = chips // 2
    blocks = 2 * half
    slots = 2 * rows * TOP // seq
    _, ny, nx = peer_offsets()
    square = ny == 2 and nx == 2
    spreads = 2 if square else heads_dev - 1
    first_shape = (4, slots, width) if square else (heads_dev - 1, 2 * slots, width)
    dma = pltpu.SemaphoreType.DMA
    big = ("qa", "ka", "va", "qb", "kb", "vb", "residual", "proj_a", "proj_b", "gate", "up", "down")
    small = ("lam", "gain_a", "gain_b", "norm_gain", "routes", "route_weight")

    def landing(name):
        shape = args[name].shape
        if name == "residual":
            shape = (rows, width)
        if len(shape) == 3 and name in ("gate", "up", "down"):
            shape = shape[1:]
        return pltpu.VMEM(shape, args[name].dtype)

    scratch = {name: landing(name) for name in big}
    scratch.update(
        load_s=dma((len(big),)),
        heads_a=pltpu.VMEM((rows, heads * value_a), BF16),
        heads_b=pltpu.VMEM((rows, heads * value_b), BF16),
        kv=pltpu.VMEM((blocks, heads, rows, width_a + value_a + width_b + value_b), BF16),
        query=pltpu.VMEM((heads, rows, width_a + width_b), BF16),
        far_query=pltpu.VMEM((half, heads, rows, width_a + width_b), BF16),
        far_stats=pltpu.VMEM((half, heads, 8, rows), F32),
        own_stats=pltpu.VMEM((heads, 8, rows), F32),
        keep=pltpu.VMEM((heads, 4, rows, blocks * rows), F32),
        part=pltpu.VMEM((half, heads, rows, value_a + value_b), BF16),
        far_part=pltpu.VMEM((heads, rows, value_a + value_b), BF16),
        total=pltpu.VMEM((half, heads, 8, rows), F32),
        far_total=pltpu.VMEM((heads, 8, rows), F32),
        chain_s=dma((half, heads)), chain_r=dma((half, heads)),
        part_s=dma((half, heads)), part_r=dma((half, heads)),
        query_s=dma((heads,)), query_r=dma((half, heads)),
        stats_s=dma((heads,)), stats_r=dma((half, heads)),
        back_s=dma((half, heads)), back_r=dma((heads,)),
        total_s=dma((half, heads)), total_r=dma((heads,)),
        branch_out=pltpu.VMEM((heads_dev - 1, rows, width), BF16),
        branch_in=pltpu.VMEM((heads_dev - 1, rows, width), BF16),
        branch_s=dma((heads_dev - 1,)), branch_r=dma((heads_dev - 1,)),
        stream=pltpu.VMEM((rows, width), BF16),
        select=pltpu.VMEM((seq, slots, rows), BF16),
        weigh=pltpu.VMEM((seq * slots, rows), F32),
        high=pltpu.VMEM((rows, seq * slots), BF16),
        low=pltpu.VMEM((rows, seq * slots), BF16),
        send=pltpu.VMEM((seq, slots, width), BF16),
        rows=pltpu.VMEM((chips, 2 * slots, model), BF16),
        out_s=dma((chips, 2)), out_r=dma((chips, 2)),
        spread_s=dma((chips, spreads)), spread_r=dma((chips, spreads)),
        relay_s=dma((chips, 2)), relay_r=dma((chips, 2)),
        down_out=pltpu.VMEM((chips, 2 * slots, model), BF16),
        first=pltpu.VMEM((chips,) + first_shape, BF16),
        first_s=dma((chips, first_shape[0])), first_r=dma((chips, first_shape[0])),
        second_out=pltpu.VMEM((chips, 2, slots, width), BF16),
        second=pltpu.VMEM((chips, 2, slots, width), BF16),
        second_s=dma((chips, 2)), second_r=dma((chips, 2)),
        sums=pltpu.VMEM((2, slots, width), BF16),
        summed=pltpu.VMEM((chips, 2, slots, width), BF16),
        back=pltpu.VMEM((seq, slots, width), BF16),
        home_s=dma((chips, 2)), home_r=dma((chips, 2)),
    )

    def kernel(*refs):
        small_refs = refs[: len(small)]
        hbm = Refs(big, refs[len(small) : len(small) + len(big)])
        at = len(small) + len(big)
        r = Refs(
            small + ("out",) + tuple(scratch), tuple(small_refs) + (refs[at],) + tuple(refs[at + 1 :])
        )

        def load(name):
            source = getattr(hbm, name)
            if name == "residual":
                source = source.at[:, block_of(lax.axis_index("tp"), width)]
            if name in ("gate", "up", "down"):
                source = source.at[0]
            return pltpu.make_async_copy(source, getattr(r, name), r.load_s.at[big.index(name)])

        def wait(*names):
            for name in names:
                load(name).wait()

        for name in big:
            load(name).start()
        greet(("sp", "tp"))
        attend(r, lambda: wait("qa", "ka", "va", "qb", "kb", "vb"))
        route(r)
        copies = project(r, lambda: wait("residual", "proj_a", "proj_b"))
        experts_part(r, lambda: wait("gate", "up", "down"))
        for copy in copies:
            copy.wait_send()

    vmem = pl.BlockSpec(memory_space=pltpu.VMEM)
    specs = [pl.BlockSpec(memory_space=pltpu.SMEM)] + [vmem] * (len(small) - 1)
    specs += [pl.BlockSpec(memory_space=pl.ANY)] * len(big)
    return pl.pallas_call(
        kernel,
        out_shape=jax.ShapeDtypeStruct((rows, width), BF16),
        in_specs=specs,
        out_specs=vmem,
        scratch_shapes=list(scratch.values()),
        compiler_params=pltpu.CompilerParams(
            collective_id=0, has_side_effects=True, vmem_limit_bytes=56 * 2**20
        ),
        name="layer",
    )(*[args[name] for name in small + big])


def local(
    residual,
    query_a,
    keys_a,
    values_a,
    query_b,
    keys_b,
    values_b,
    lambda_a,
    lambda_b,
    gain_a,
    gain_b,
    proj_a,
    proj_b,
    norm_gain,
    routes,
    route_weight,
    expert_gate,
    expert_up,
    expert_down,
):
    args = dict(
        residual=residual,
        qa=query_a,
        ka=keys_a,
        va=values_a,
        qb=query_b,
        kb=keys_b,
        vb=values_b,
        lam=jnp.stack([lambda_a, lambda_b]),
        gain_a=gain_a.reshape(1, -1),
        gain_b=gain_b.reshape(1, -1),
        proj_a=proj_a,
        proj_b=proj_b,
        norm_gain=norm_gain.reshape(1, -1),
        routes=routes,
        route_weight=route_weight,
        gate=expert_gate,
        up=expert_up,
        down=expert_down,
    )
    return layer(args)


def solution(mesh):
    placed = (
        P("sp", None),
        P("sp", "tp", None),
        P("sp", "tp", None),
        P("sp", "tp", None),
        P("sp", "tp", None),
        P("sp", "tp", None),
        P("sp", "tp", None),
        P("tp"),
        P("tp"),
        P(),
        P(),
        P("tp", None),
        P("tp", None),
        P(),
        P("sp", None),
        P("sp", None),
        P("sp", None, "tp"),
        P("sp", None, "tp"),
        P("sp", "tp", None),
    )
    return jax.shard_map(
        local, mesh=mesh, in_specs=placed, out_specs=P("sp", "tp"), check_vma=False
    )
```

```python
import math

import jax
import jax.numpy as jnp
from jax import lax
from jax.experimental import pallas as pl
from jax.experimental.pallas import tpu as pltpu
from jax.sharding import PartitionSpec as P

SEG = 64
TOP = 2
EPS = 1e-06

LOG2E = 1.4426950408889634
MESH = pl.DeviceIdType.MESH
F32 = jnp.float32
BF16 = jnp.bfloat16


def dot_nt(left, right):
    return lax.dot_general(left, right, (((1,), (1,)), ((), ())), preferred_element_type=F32)


def remote(source, target, send_sem, recv_sem, axis, peer):
    return pltpu.make_async_remote_copy(
        src_ref=source,
        dst_ref=target,
        send_sem=send_sem,
        recv_sem=recv_sem,
        device_id={axis: peer},
        device_id_type=MESH,
    )


def greet(axes):
    barrier = pltpu.get_barrier_semaphore()
    total = 0
    for axis in axes:
        peers = lax.axis_size(axis)
        me = lax.axis_index(axis)
        for step in range(1, peers):
            pl.semaphore_signal(
                barrier, inc=1, device_id={axis: lax.rem(me + step, peers)}, device_id_type=MESH
            )
        total += peers - 1
    return lambda: pl.semaphore_wait(barrier, total)


def columns_of(stats):
    repeat = stats.shape[1] // stats.shape[0]
    return jnp.concatenate([stats] * repeat, axis=0).T


def rows_of(columns):
    rows = columns[0].shape[0]
    lane = lax.broadcasted_iota(jnp.int32, (rows, rows), 1)
    tile = jnp.zeros((rows, rows), F32)
    for at, column in enumerate(columns):
        tile = jnp.where(lane == at, column, tile)
    return tile.T[: len(columns)]


class Refs:
    def __init__(self, names, refs):
        for name, ref in zip(names, refs):
            setattr(self, name, ref)


def attend(r, arrived, greeted, meanwhile):
    seq = lax.axis_size("sp")
    rows, heads, width_a = r.qa.shape
    width_b = r.qb.shape[2]
    value_a, value_b = r.va.shape[2], r.vb.shape[2]
    key_a, key_b = width_a // 2, width_b // 2
    chips = seq // 2
    half = chips // 2
    blocks = 2 * half
    pair = 2 - half % 2
    wide_q = width_a + width_b
    key_spans = ((0, width_a), (width_a, width_b))
    value_spans = ((wide_q, value_a), (wide_q + value_a, value_b))
    parts_of = (pl.ds(0, wide_q), pl.ds(wide_q, value_a + value_b))
    factors = (key_a ** (-0.5) * LOG2E, key_b ** (-0.5) * LOG2E)
    lams = (r.lam_a, r.lam_b)
    kv, query = r.kv, r.query

    me = lax.axis_index("sp")
    chip, core = me // 2, lax.rem(me, 2)
    upper = chip >= half
    lower = chip < half
    place = lax.rem(chip, half)
    middle = 2 * (half - 1) + core
    partner = 2 * chip + 1 - core
    above = jnp.minimum(me + 2, seq - 2 + core)
    slot = 2 * place + core

    def chain(y, head, part):
        ref = kv.at[2 * y + core, head, :, parts_of[part]]
        return remote(
            ref, ref, r.chain_s.at[y, head, part], r.chain_r.at[y, head, part], "sp", above
        )

    def across(y, head, part):
        ref = kv.at[2 * y + core, head, :, parts_of[part]]
        return remote(
            ref, ref, r.part_s.at[y, head, part], r.part_r.at[y, head, part], "sp", partner
        )

    def ask(i, head):
        return remote(
            query.at[head], r.far_query.at[i, head], r.query_s.at[head], r.query_r.at[i, head],
            "sp", middle,
        )

    def tell(i, head):
        return remote(
            r.own_stats.at[head], r.far_stats.at[i, head], r.stats_s.at[head],
            r.stats_r.at[i, head], "sp", middle,
        )

    def answer(i, head):
        return remote(
            r.part.at[i, head], r.far_part.at[head], r.back_s.at[i, head], r.back_r.at[head],
            "sp", 2 * (half + i) + core,
        )

    def answer_total(i, head):
        return remote(
            r.total.at[i, head], r.far_total.at[head], r.total_s.at[i, head], r.total_r.at[head],
            "sp", 2 * (half + i) + core,
        )

    def pack(head):
        query[head, :, :width_a] = r.qa[:, head, :]
        query[head, :, width_a:] = r.qb[:, head, :]
        for span, ref in zip(key_spans + value_spans, (r.ka, r.kb, r.va, r.vb)):
            kv[slot, head, :, span[0] : span[0] + span[1]] = ref[:, head, :]

    arrived()
    for head in range(heads):
        pack(head)
    greeted()

    def give(head, part):
        @pl.when(place < half - 1)
        def _():
            chain(place, head, part).start()

        across(place, head, part).start()

    @pl.when(upper)
    def _():
        for head in range(heads):
            if head == 0:
                ask(place, head).start()
            give(head, 0)
        for head in range(heads):
            give(head, 1)

    @pl.when(lower)
    def _():
        for head in range(heads):
            give(head, 0)
            give(head, 1)

    def pass_on(here, head, part):
        for y in range(here):
            chain(y, head, part).wait_recv()
            across(y, head, part).start()
            if here < half - 1:
                chain(y, head, part).start()

    def landed(here, head, part):
        for y in range(here + 1):
            across(y, head, part).wait_recv()

    def gather(here, head, part):
        pass_on(here, head, part)
        landed(here, head, part)

    def score_maps(queries, head, count):
        maps = []
        for group, (begin, width) in enumerate(key_spans):
            wide = queries[:, begin : begin + width]
            block_keys = kv[:count, head, :, begin : begin + width].reshape(count * rows, width)
            size = width // 2
            if size % 128:
                lane = lax.broadcasted_iota(jnp.int32, wide.shape, 1)
                nothing = jnp.zeros_like(wide)
                first = dot_nt(jnp.where(lane < size, wide, nothing), block_keys)
                second = dot_nt(jnp.where(lane < size, nothing, wide), block_keys)
            else:
                first = dot_nt(wide[:, :size], block_keys[:, :size])
                second = dot_nt(wide[:, size:], block_keys[:, size:])
            maps += [first * factors[group], second * factors[group]]
        return maps

    def visible(count):
        query_seg = (slot * rows + lax.broadcasted_iota(jnp.int32, (rows, 1), 0)) // SEG
        key_seg = lax.broadcasted_iota(jnp.int32, (1, count * rows), 1) // SEG
        return query_seg >= key_seg

    def combine(first, second, head, count, group):
        weights = (first - second).astype(BF16)
        begin, size = value_spans[group]
        block_values = kv[:count, head, :, begin : begin + size].reshape(count * rows, size)
        return jnp.dot(weights, block_values, preferred_element_type=F32)

    def finish(mixed, gain, out, head, size):
        mean_sq = jnp.mean(mixed * mixed, axis=1, keepdims=True)
        value = (mixed * lax.rsqrt(mean_sq + EPS) * gain[...]).astype(BF16)
        out[:, pl.ds(pl.multiple_of(head * size, size), size)] = value

    def finish_both(mixed, head):
        finish(mixed[0], r.gain_a, r.heads_a, head, value_a)
        finish(mixed[1], r.gain_b, r.heads_b, head, value_b)

    def own_lower(head, count):
        seen = visible(count)
        maps = [jnp.where(seen, one, -jnp.inf) for one in score_maps(query.at[head], head, count)]
        mixed = []
        for group in range(2):
            parts = []
            for at in range(2):
                scores = maps[2 * group + at]
                expo = jnp.exp2(scores - jnp.max(scores, axis=1, keepdims=True))
                scale = 1.0 / jnp.sum(expo, axis=1, keepdims=True)
                if at:
                    scale = scale * lams[group][head]
                parts.append(expo * scale)
            mixed.append(combine(parts[0], parts[1], head, count, group))
        finish_both(mixed, head)

    def wait_far(i, head):
        for at in range(pair):
            ask(i + at, head).wait_recv()
        for at in range(pair):
            tell(i + at, head).wait_recv()

    def for_upper(i, head):
        queries = r.far_query[pl.ds(i, pair), head].reshape(pair * rows, wide_q)
        maps = score_maps(queries, head, blocks)
        far = jnp.concatenate(
            [columns_of(r.far_stats[i + at, head]) for at in range(pair)], axis=0
        )
        stats, expos, scales = [], [], []
        for k in range(4):
            far_max, far_sum = far[:, k : k + 1], far[:, 4 + k : 5 + k]
            own_max = jnp.max(maps[k], axis=1, keepdims=True)
            expo = jnp.exp2(maps[k] - own_max)
            top = jnp.maximum(own_max, far_max)
            down = jnp.exp2(own_max - top)
            summed = jnp.sum(expo, axis=1, keepdims=True) * down + far_sum * jnp.exp2(far_max - top)
            stats.append((top, summed))
            expos.append(expo)
            scales.append(down / summed)
        for group in range(2):
            first = expos[2 * group] * scales[2 * group]
            second = expos[2 * group + 1] * (lams[group][head] * scales[2 * group + 1])
            mixed = combine(first, second, head, blocks, group)
            begin, size = (0, value_a) if group == 0 else (value_a, value_b)
            r.part[pl.ds(i, pair), head, :, begin : begin + size] = mixed.astype(BF16).reshape(
                pair, rows, size
            )
        for at in range(pair):
            part = slice(at * rows, (at + 1) * rows)
            r.total[i + at, head] = rows_of(
                [one[0][part] for one in stats] + [one[1][part] for one in stats]
            )
        for at in reversed(range(pair)):
            answer_total(i + at, head).start()
            answer(i + at, head).start()

    def upper_first(head, count):
        seen = visible(count)
        maps = [jnp.where(seen, one, -jnp.inf) for one in score_maps(query.at[head], head, count)]
        tops, sums = [], []
        for k in range(4):
            top = jnp.max(maps[k], axis=1, keepdims=True)
            expo = jnp.exp2(maps[k] - top)
            r.keep[head, k, :, : count * rows] = expo
            tops.append(top)
            sums.append(jnp.sum(expo, axis=1, keepdims=True))
        r.own_stats[head] = rows_of(tops + sums)
        tell(place, head).start()

    def upper_second(head, count):
        answer_total(0, head).wait_recv()
        own = columns_of(r.own_stats[head])
        whole = columns_of(r.far_total[head])
        scales = []
        for k in range(4):
            scale = jnp.exp2(own[:, k : k + 1] - whole[:, k : k + 1]) / whole[:, 4 + k : 5 + k]
            if k % 2:
                scale = scale * lams[k // 2][head]
            scales.append(scale)
        mixed = []
        for group in range(2):
            first = r.keep[head, 2 * group, :, : count * rows] * scales[2 * group]
            second = r.keep[head, 2 * group + 1, :, : count * rows] * scales[2 * group + 1]
            mixed.append(combine(first, second, head, count, group))
        answer(0, head).wait_recv()
        far = r.far_part[head].astype(F32)
        finish_both([mixed[0] + far[:, :value_a], mixed[1] + far[:, value_a:]], head)

    for here in range(half):

        @pl.when((place == here) & lower)
        def _():
            meanwhile()

            pass_on(here, 0, 0)
            pass_on(here, 0, 1)

            def step(head, carry):
                landed(here, head, 0)
                landed(here, head, 1)
                if here == half - 1:

                    def each(i, inner):
                        wait_far(i * pair, head)
                        for_upper(i * pair, head)
                        return inner

                    lax.fori_loop(1, half // pair, each, 0)
                    wait_far(0, head)
                    own_lower(head, 2 * here + 2)
                    for_upper(0, head)
                else:
                    own_lower(head, 2 * here + 2)
                if here:

                    @pl.when((head == 0) & (heads > 1))
                    def _():
                        pass_on(here, min(1, heads - 1), 0)
                        pass_on(here, min(1, heads - 1), 1)

                    @pl.when(head + 2 < heads)
                    def _():
                        pass_on(here, head + 2, 0)
                        pass_on(here, head + 2, 1)

                return carry

            lax.fori_loop(0, heads, step, 0)

        @pl.when((place == here) & upper)
        def _():
            def step(head, carry):
                gather(here, head, 0)
                upper_first(head, 2 * here + 2)

                @pl.when(head + 1 < heads)
                def _():
                    ask(place, head + 1).start()

                return carry

            lax.fori_loop(0, heads, step, 0)
            meanwhile()

            def rest(head, carry):
                gather(here, head, 1)
                return carry

            lax.fori_loop(0, heads, rest, 0)

            def second(head, carry):
                upper_second(head, 2 * here + 2)
                return carry

            lax.fori_loop(0, heads, second, 0)

    def drain():
        for here in range(half):

            @pl.when(place == here)
            def _():
                def each(head, carry):
                    for y in range(here + 1):
                        for part in range(2):
                            across(y, head, part).wait_send()
                            if here < half - 1:
                                chain(y, head, part).wait_send()
                    return carry

                lax.fori_loop(0, heads, each, 0)

        @pl.when(upper)
        def _():
            def each(head, carry):
                ask(place, head).wait_send()
                tell(place, head).wait_send()
                return carry

            lax.fori_loop(0, heads, each, 0)

    def answered():
        def each(head, carry):
            for i in range(half):
                answer(i, head).wait_send()
                answer_total(i, head).wait_send()
            return carry

        lax.fori_loop(0, heads, each, 0)

    return drain, answered


def grid_of(count):
    side = math.isqrt(count)
    return (side, side) if side * side == count else (1, count)


def peer_at(dy, dx):
    ny, nx = grid_of(lax.axis_size("tp"))
    me = lax.axis_index("tp")
    return lax.rem(me // nx + dy, ny) * nx + lax.rem(lax.rem(me, nx) + dx, nx)


def peer_offsets():
    ny, nx = grid_of(lax.axis_size("tp"))
    offsets = [(dy, dx) for dy in range(ny) for dx in range(nx) if dy or dx]
    far = lambda one: min(one[0], ny - one[0]) + min(one[1], nx - one[1])
    return sorted(offsets, key=far, reverse=True), ny, nx


def block_of(index, width):
    return pl.ds(pl.multiple_of(index * width, width), width)


def route(r):
    experts, slots, rows = r.select.shape
    square = (rows, rows)
    lane = lax.broadcasted_iota(jnp.int32, square, 1)
    line = lax.broadcasted_iota(jnp.int32, square, 0)
    named = r.routes[...]
    weight = r.route_weight[...]
    share = weight / jnp.sum(weight, axis=0, keepdims=True)
    chosen = jnp.zeros(square, F32)
    gate = jnp.zeros(square, F32)
    for k in range(TOP):
        match = named[k : k + 1] == line
        chosen = chosen + jnp.where(match, 1.0, 0.0)
        gate = gate + jnp.where(match, share[k : k + 1], 0.0)
    earlier = jnp.dot(
        chosen.astype(BF16),
        jnp.where(line < lane, 1.0, 0.0).astype(BF16),
        preferred_element_type=F32,
    )
    slot = lax.broadcasted_iota(jnp.int32, (slots, rows), 0).astype(F32)
    for expert in range(experts):
        pick = (chosen[expert : expert + 1] > 0.5) & (earlier[expert : expert + 1] == slot)
        r.select[expert] = jnp.where(pick, 1.0, 0.0).astype(BF16)
        r.weigh[expert * slots : (expert + 1) * slots, :] = jnp.where(
            pick, gate[expert : expert + 1], 0.0
        )
    weigh = r.weigh[...].T
    high = weigh.astype(BF16)
    r.high[...] = high
    r.low[...] = (weigh - high.astype(F32)).astype(BF16)


def project(r, loaded):
    offsets, _, _ = peer_offsets()
    me = lax.axis_index("tp")
    width = r.stream.shape[1]

    def piece(owner):
        columns = block_of(owner, width)
        return jnp.dot(
            r.heads_a[...], r.proj_a[:, columns], preferred_element_type=F32
        ) + jnp.dot(r.heads_b[...], r.proj_b[:, columns], preferred_element_type=F32)

    loaded()
    copies = []
    for at, offset in enumerate(offsets):
        peer = peer_at(*offset)
        r.branch_out[at] = piece(peer).astype(BF16)
        copy = remote(
            r.branch_out.at[at], r.branch_in.at[at], r.branch_s.at[at], r.branch_r.at[at], "tp", peer
        )
        copy.start()
        copies.append(copy)
    r.branch_own[...] = r.residual[...].astype(F32) + piece(me)

    def settle():
        summed = r.branch_own[...]
        for at, copy in reversed(list(enumerate(copies))):
            copy.wait_recv()
            summed = summed + r.branch_in[at].astype(F32)
        r.stream[...] = summed.astype(BF16)

    def drain():
        for copy in copies:
            copy.wait_send()

    return settle, drain


def experts_part(r):
    offsets, ny, nx = peer_offsets()
    seq, heads = lax.axis_size("sp"), lax.axis_size("tp")
    me, mine = lax.axis_index("sp"), lax.axis_index("tp")
    chips = seq // 2
    chip, core = me // 2, lax.rem(me, 2)
    experts, slots, rows = r.select.shape
    width = r.stream.shape[1]
    square = ny == 2 and nx == 2
    across_x, across_y, across_both = peer_at(0, 1), peer_at(1, 0), peer_at(1, 1)
    top, bottom = pl.ds(0, slots), pl.ds(slots, slots)

    half = chips // 2

    def source(k):
        late = half + lax.rem(lax.rem(chip, half) + 1 + k, half)
        return jnp.where(k < half, k, late)

    def distance(k):
        return lax.rem(chip + chips - source(k), chips)

    def outgoing(step, side):
        target_core = core if side == 0 else 1 - core
        expert = 2 * lax.rem(chip + step, chips) + target_core
        return expert, remote(
            r.send.at[expert],
            r.rows.at[chip, block_of(core, slots), block_of(mine, width)],
            r.out_s.at[step, side],
            r.out_r.at[step, side],
            "sp",
            expert,
        )

    def send_out(steps):
        for step in sorted(steps, key=lambda step: (step == 0, step % 2 == 0, -step)):
            for side in range(2):
                expert, copy = outgoing(step, side)
                picked = jnp.dot(r.select[expert], r.stream[...], preferred_element_type=F32)
                if step == 0 and side == 0:
                    place = (chip, block_of(core, slots), block_of(mine, width))
                    r.rows[place] = picked.astype(BF16)
                else:
                    r.send[expert] = picked.astype(BF16)
                    copy.start()

    def incoming(k, side):
        origin_core = core if side == 0 else 1 - core
        origin = source(k)
        return remote(
            r.send.at[me],
            r.rows.at[origin, block_of(origin_core, slots), block_of(mine, width)],
            r.out_s.at[distance(k), side],
            r.out_r.at[distance(k), side],
            "sp",
            2 * origin + origin_core,
        )

    def land(k):
        @pl.when(distance(k) > 0)
        def _():
            incoming(k, 0).wait_recv()

        incoming(k, 1).wait_recv()

    def spread(step, at, peer, owner):
        ref = r.rows.at[source(step), :, block_of(owner, width)]
        return remote(ref, ref, r.spread_s.at[step, at], r.spread_r.at[step, at], "tp", peer)

    def relay(step, at, peer, owner):
        ref = r.rows.at[source(step), top if at == 0 else bottom, block_of(owner, width)]
        return remote(ref, ref, r.relay_s.at[step, at], r.relay_r.at[step, at], "tp", peer)

    near = ((0, 1), (1, 0)) if square else offsets

    def start_spread(step):
        land(step)
        for at, offset in enumerate(near):
            spread(step, at, peer_at(*offset), mine).start()

    def start_relay(step):
        for at, offset in enumerate(near):
            giver = peer_at(ny - offset[0], nx - offset[1])
            spread(step, at, giver, giver).wait_recv()
        if square:
            relay(step, 0, across_y, across_x).start()
            relay(step, 1, across_x, across_y).start()

    def compute(step):
        if square:
            relay(step, 0, across_y, across_both).wait_recv()
            relay(step, 1, across_x, across_both).wait_recv()
        origin = source(step)
        wide = r.rows[origin].astype(F32)
        mean_sq = jnp.mean(wide * wide, axis=1, keepdims=True)
        normed = (wide * lax.rsqrt(mean_sq + EPS) * r.norm_gain[...]).astype(BF16)
        gate = jnp.dot(normed, r.gate[...], preferred_element_type=F32)
        up = jnp.dot(normed, r.up[...], preferred_element_type=F32)
        hidden = (gate / (1.0 + jnp.exp(-gate)) * up).astype(BF16)
        r.down_out[step] = jnp.dot(hidden, r.down[...], preferred_element_type=F32).astype(BF16)

    def first_copies(step):
        if not square:
            return [
                remote(
                    r.down_out.at[step, :, block_of(peer_at(*offset), width)],
                    r.first.at[step, at],
                    r.first_s.at[step, at],
                    r.first_r.at[step, at],
                    "tp",
                    peer_at(*offset),
                )
                for at, offset in enumerate(offsets)
            ]
        plan = (
            (top, across_x, across_both, 1),
            (bottom, across_y, across_both, 3),
            (top, across_x, across_x, 0),
            (bottom, across_y, across_y, 2),
        )
        return [
            remote(
                r.down_out.at[step, part, block_of(owner, width)],
                r.first.at[step, slot],
                r.first_s.at[step, slot],
                r.first_r.at[step, slot],
                "tp",
                peer,
            )
            for part, peer, owner, slot in plan
        ]

    def second_copies(step):
        return [
            remote(
                r.second_out.at[step, at],
                r.second.at[step, at],
                r.second_s.at[step, at],
                r.second_r.at[step, at],
                "tp",
                peer,
            )
            for at, peer in enumerate((across_y, across_x))
        ]

    def start_first(step):
        for copy in first_copies(step):
            copy.start()

    def start_second(step):
        if not square:
            return
        firsts, seconds = first_copies(step), second_copies(step)
        for at, part, owner, slot in ((0, top, across_y, 1), (1, bottom, across_x, 3)):
            firsts[at].wait_recv()
            summed = r.down_out[step, part, block_of(owner, width)].astype(F32)
            summed = summed + r.first[step, slot].astype(F32)
            r.second_out[step, at] = summed.astype(BF16)
            seconds[at].start()

    def home(step, side):
        origin_core = core if side == 0 else 1 - core
        return remote(
            r.summed.at[step, side],
            r.back.at[me],
            r.home_s.at[distance(step), side],
            r.home_r.at[distance(step), side],
            "sp",
            2 * source(step) + origin_core,
        )

    def returned(step, side):
        expert_core = core if side == 0 else 1 - core
        expert = 2 * lax.rem(chip + step, chips) + expert_core
        return remote(
            r.summed.at[step, side],
            r.back.at[expert],
            r.home_s.at[step, side],
            r.home_r.at[step, side],
            "sp",
            expert,
        )

    def start_home(step):
        own = block_of(mine, width)
        firsts = first_copies(step)
        if square:
            seconds = second_copies(step)
            firsts[2].wait_recv()
            firsts[3].wait_recv()
            halves = []
            for at, part, slot in ((0, top, 0), (1, bottom, 2)):
                seconds[at].wait_recv()
                halves.append(
                    r.down_out[step, part, own].astype(F32)
                    + r.first[step, slot].astype(F32)
                    + r.second[step, at].astype(F32)
                )
            r.sums[0] = halves[0].astype(BF16)
            r.sums[1] = halves[1].astype(BF16)
        else:
            summed = r.down_out[step, :, own].astype(F32)
            for at, copy in enumerate(firsts):
                copy.wait_recv()
                summed = summed + r.first[step, at].astype(F32)
            r.sums[0] = summed[:slots].astype(BF16)
            r.sums[1] = summed[slots:].astype(BF16)
        r.summed[step, 0] = r.sums[core]
        r.summed[step, 1] = r.sums[1 - core]

        @pl.when(distance(step) == 0)
        def _():
            r.back[me] = r.summed[step, 0]

        @pl.when(distance(step) > 0)
        def _():
            home(step, 0).start()

        home(step, 1).start()

    def start():
        start_spread(0)

    def first_relay():
        start_relay(0)

    def others():
        def body(k, carry):
            @pl.when(k < chips)
            def _():
                start_relay(k)

            @pl.when(k + 1 < chips)
            def _():
                start_spread(k + 1)

            @pl.when(k < chips)
            def _():
                compute(k)
                start_first(k)

            @pl.when(k < chips + 1)
            def _():
                start_second(k - 1)

            @pl.when(k >= 2)
            def _():
                start_home(k - 2)

            return carry

        lax.fori_loop(1, chips + 2, body, 0)
        finish()

    def finish():
        def arrive(step, carry):
            @pl.when(step > 0)
            def _():
                returned(step, 0).wait_recv()

            returned(step, 1).wait_recv()
            return carry

        lax.fori_loop(0, chips, arrive, 0)
        back = r.back[...].reshape(experts * slots, width)
        mixed = jnp.dot(r.high[...], back, preferred_element_type=F32)
        mixed = mixed + jnp.dot(r.low[...], back, preferred_element_type=F32)
        r.out[...] = (r.stream[...].astype(F32) + mixed).astype(BF16)

    def drain():
        def each(k, carry):
            @pl.when(k > 0)
            def _():
                outgoing(k, 0)[1].wait_send()

            outgoing(k, 1)[1].wait_send()

            @pl.when(distance(k) > 0)
            def _():
                home(k, 0).wait_send()

            home(k, 1).wait_send()
            for at, offset in enumerate(near):
                spread(k, at, peer_at(*offset), mine).wait_send()
            if square:
                relay(k, 0, across_y, across_x).wait_send()
                relay(k, 1, across_x, across_y).wait_send()
                for copy in second_copies(k):
                    copy.wait_send()
            for copy in first_copies(k):
                copy.wait_send()
            return carry

        lax.fori_loop(0, chips, each, 0)

    return send_out, start, first_relay, compute, start_first, start_spread, others, drain


def layer(args):
    seq, heads_dev = lax.axis_size("sp"), lax.axis_size("tp")
    rows, heads, width_a = args["qa"].shape
    width_b = args["qb"].shape[2]
    value_a, value_b = args["va"].shape[2], args["vb"].shape[2]
    model = args["residual"].shape[1]
    width = model // heads_dev
    chips = seq // 2
    half = chips // 2
    blocks = 2 * half
    slots = 2 * rows * TOP // seq
    _, ny, nx = peer_offsets()
    square = ny == 2 and nx == 2
    spreads = 2 if square else heads_dev - 1
    first_shape = (4, slots, width) if square else (heads_dev - 1, 2 * slots, width)
    dma = pltpu.SemaphoreType.DMA
    big = ("qa", "ka", "va", "qb", "kb", "vb", "residual", "proj_a", "proj_b", "gate", "up", "down")
    small = ("lam_a", "lam_b", "gain_a", "gain_b", "norm_gain", "routes", "route_weight")

    def landing(name):
        shape = args[name].shape
        if name == "residual":
            shape = (rows, width)
        if len(shape) == 3 and name in ("gate", "up", "down"):
            shape = shape[1:]
        return pltpu.VMEM(shape, args[name].dtype)

    scratch = {name: landing(name) for name in big}
    scratch.update(
        load_s=dma((len(big),)),
        go=pltpu.SemaphoreType.REGULAR,
        heads_a=pltpu.VMEM((rows, heads * value_a), BF16),
        heads_b=pltpu.VMEM((rows, heads * value_b), BF16),
        kv=pltpu.VMEM((blocks, heads, rows, width_a + value_a + width_b + value_b), BF16),
        query=pltpu.VMEM((heads, rows, width_a + width_b), BF16),
        far_query=pltpu.VMEM((half, heads, rows, width_a + width_b), BF16),
        far_stats=pltpu.VMEM((half, heads, 8, rows), F32),
        own_stats=pltpu.VMEM((heads, 8, rows), F32),
        keep=pltpu.VMEM((heads, 4, rows, blocks * rows), F32),
        part=pltpu.VMEM((half, heads, rows, value_a + value_b), BF16),
        far_part=pltpu.VMEM((heads, rows, value_a + value_b), BF16),
        total=pltpu.VMEM((half, heads, 8, rows), F32),
        far_total=pltpu.VMEM((heads, 8, rows), F32),
        chain_s=dma((half, heads, 2)), chain_r=dma((half, heads, 2)),
        part_s=dma((half, heads, 2)), part_r=dma((half, heads, 2)),
        query_s=dma((heads,)), query_r=dma((half, heads)),
        stats_s=dma((heads,)), stats_r=dma((half, heads)),
        back_s=dma((half, heads)), back_r=dma((heads,)),
        total_s=dma((half, heads)), total_r=dma((heads,)),
        branch_out=pltpu.VMEM((heads_dev - 1, rows, width), BF16),
        branch_own=pltpu.VMEM((rows, width), F32),
        branch_in=pltpu.VMEM((heads_dev - 1, rows, width), BF16),
        branch_s=dma((heads_dev - 1,)), branch_r=dma((heads_dev - 1,)),
        stream=pltpu.VMEM((rows, width), BF16),
        select=pltpu.VMEM((seq, slots, rows), BF16),
        weigh=pltpu.VMEM((seq * slots, rows), F32),
        high=pltpu.VMEM((rows, seq * slots), BF16),
        low=pltpu.VMEM((rows, seq * slots), BF16),
        send=pltpu.VMEM((seq, slots, width), BF16),
        rows=pltpu.VMEM((chips, 2 * slots, model), BF16),
        out_s=dma((chips, 2)), out_r=dma((chips, 2)),
        spread_s=dma((chips, spreads)), spread_r=dma((chips, spreads)),
        relay_s=dma((chips, 2)), relay_r=dma((chips, 2)),
        down_out=pltpu.VMEM((chips, 2 * slots, model), BF16),
        first=pltpu.VMEM((chips,) + first_shape, BF16),
        first_s=dma((chips, first_shape[0])), first_r=dma((chips, first_shape[0])),
        second_out=pltpu.VMEM((chips, 2, slots, width), BF16),
        second=pltpu.VMEM((chips, 2, slots, width), BF16),
        second_s=dma((chips, 2)), second_r=dma((chips, 2)),
        sums=pltpu.VMEM((2, slots, width), BF16),
        summed=pltpu.VMEM((chips, 2, slots, width), BF16),
        back=pltpu.VMEM((seq, slots, width), BF16),
        home_s=dma((chips, 2)), home_r=dma((chips, 2)),
    )

    def kernel(*refs):
        small_refs = refs[: len(small)]
        hbm = Refs(big, refs[len(small) : len(small) + len(big)])
        at = len(small) + len(big)
        r = Refs(
            small + ("out",) + tuple(scratch), tuple(small_refs) + (refs[at],) + tuple(refs[at + 1 :])
        )

        def load(name):
            source = getattr(hbm, name)
            if name == "residual":
                source = source.at[:, block_of(lax.axis_index("tp"), width)]
            if name in ("gate", "up", "down"):
                source = source.at[0]
            return pltpu.make_async_copy(source, getattr(r, name), r.load_s.at[big.index(name)])

        def wait(*names):
            for name in names:
                load(name).wait()

        for name in big:
            load(name).start()
        greeted = greet(("sp", "tp"))
        (
            send_out, start, first_relay, compute, start_first, start_spread, others, drain_experts,
        ) = experts_part(r)
        chip = lax.axis_index("sp") // 2
        drain_heads, answered = attend(
            r, lambda: wait("qa", "ka", "va", "qb", "kb", "vb"), greeted, lambda: route(r)
        )

        settle, drain_branch = project(r, lambda: wait("residual", "proj_a", "proj_b"))
        wait("gate", "up", "down")

        @pl.when(chip == half - 1)
        def _():
            answered()
            if half > 1:
                pl.semaphore_signal(
                    r.go, inc=1, device_id={"sp": lax.rem(lax.axis_index("sp"), 2)}, device_id_type=MESH
                )

        @pl.when(chip == 0)
        def _():
            settle()
            send_out(range(half))
            start()
            first_relay()
            compute(0)
            start_first(0)
            if half > 1:
                pl.semaphore_wait(r.go, 1)
            send_out(range(half, chips))
            start_spread(1)

        @pl.when(chip > 0)
        def _():
            start()
            settle()
            send_out(range(chips))
            first_relay()
            start_spread(1)
            compute(0)
            start_first(0)

        others()
        drain_heads()
        drain_branch()
        drain_experts()

    vmem = pl.BlockSpec(memory_space=pltpu.VMEM)
    specs = [pl.BlockSpec(memory_space=pltpu.SMEM)] * 2 + [vmem] * (len(small) - 2)
    specs += [pl.BlockSpec(memory_space=pl.ANY)] * len(big)
    return pl.pallas_call(
        kernel,
        out_shape=jax.ShapeDtypeStruct((rows, width), BF16),
        in_specs=specs,
        out_specs=vmem,
        scratch_shapes=list(scratch.values()),
        compiler_params=pltpu.CompilerParams(
            collective_id=0, has_side_effects=True, vmem_limit_bytes=56 * 2**20
        ),
        name="layer",
    )(*[args[name] for name in small + big])


def local(
    residual,
    query_a,
    keys_a,
    values_a,
    query_b,
    keys_b,
    values_b,
    lambda_a,
    lambda_b,
    gain_a,
    gain_b,
    proj_a,
    proj_b,
    norm_gain,
    routes,
    route_weight,
    expert_gate,
    expert_up,
    expert_down,
):
    args = dict(
        residual=residual,
        qa=query_a,
        ka=keys_a,
        va=values_a,
        qb=query_b,
        kb=keys_b,
        vb=values_b,
        lam_a=lambda_a,
        lam_b=lambda_b,
        gain_a=gain_a.reshape(1, -1),
        gain_b=gain_b.reshape(1, -1),
        proj_a=proj_a,
        proj_b=proj_b,
        norm_gain=norm_gain.reshape(1, -1),
        routes=routes.T,
        route_weight=route_weight.T,
        gate=expert_gate,
        up=expert_up,
        down=expert_down,
    )
    return layer(args)


def solution(mesh):
    placed = (
        P("sp", None),
        P("sp", "tp", None),
        P("sp", "tp", None),
        P("sp", "tp", None),
        P("sp", "tp", None),
        P("sp", "tp", None),
        P("sp", "tp", None),
        P("tp"),
        P("tp"),
        P(),
        P(),
        P("tp", None),
        P("tp", None),
        P(),
        P("sp", None),
        P("sp", None),
        P("sp", None, "tp"),
        P("sp", None, "tp"),
        P("sp", "tp", None),
    )
    return jax.shard_map(
        local, mesh=mesh, in_specs=placed, out_specs=P("sp", "tp"), check_vma=False
    )
```

```python
import math

import jax
import jax.numpy as jnp
from jax import lax
from jax.experimental import pallas as pl
from jax.experimental.pallas import tpu as pltpu
from jax.sharding import PartitionSpec as P

SEG = 64
TOP = 2
EPS = 1e-06

LOG2E = 1.4426950408889634
MESH = pl.DeviceIdType.MESH
F32 = jnp.float32
BF16 = jnp.bfloat16


def dot_nt(left, right):
    return lax.dot_general(left, right, (((1,), (1,)), ((), ())), preferred_element_type=F32)


def remote(source, target, send_sem, recv_sem, axis, peer):
    return pltpu.make_async_remote_copy(
        src_ref=source,
        dst_ref=target,
        send_sem=send_sem,
        recv_sem=recv_sem,
        device_id={axis: peer},
        device_id_type=MESH,
    )


def greet(axes):
    barrier = pltpu.get_barrier_semaphore()
    total = 0
    for axis in axes:
        peers = lax.axis_size(axis)
        me = lax.axis_index(axis)
        for step in range(1, peers):
            pl.semaphore_signal(
                barrier, inc=1, device_id={axis: lax.rem(me + step, peers)}, device_id_type=MESH
            )
        total += peers - 1
    return lambda: pl.semaphore_wait(barrier, total)


def columns_of(stats):
    repeat = stats.shape[1] // stats.shape[0]
    return jnp.concatenate([stats] * repeat, axis=0).T


def rows_of(columns):
    rows = columns[0].shape[0]
    lane = lax.broadcasted_iota(jnp.int32, (rows, rows), 1)
    tile = jnp.zeros((rows, rows), F32)
    for at, column in enumerate(columns):
        tile = jnp.where(lane == at, column, tile)
    return tile.T[: len(columns)]


class Refs:
    def __init__(self, names, refs):
        for name, ref in zip(names, refs):
            setattr(self, name, ref)


def attend(r, arrived, greeted, meanwhile):
    seq = lax.axis_size("sp")
    rows, heads, width_a = r.qa.shape
    width_b = r.qb.shape[2]
    value_a, value_b = r.va.shape[2], r.vb.shape[2]
    key_a, key_b = width_a // 2, width_b // 2
    chips = seq // 2
    half = chips // 2
    blocks = 2 * half
    pair = 2 - half % 2
    wide_q = width_a + width_b
    key_spans = ((0, width_a), (width_a, width_b))
    value_spans = ((wide_q, value_a), (wide_q + value_a, value_b))
    parts_of = (pl.ds(0, wide_q), pl.ds(wide_q, value_a + value_b))
    factors = (key_a ** (-0.5) * LOG2E, key_b ** (-0.5) * LOG2E)
    lams = (r.lam_a, r.lam_b)
    kv, query = r.kv, r.query

    me = lax.axis_index("sp")
    chip, core = me // 2, lax.rem(me, 2)
    upper = chip >= half
    lower = chip < half
    place = lax.rem(chip, half)
    middle = 2 * (half - 1) + core
    partner = 2 * chip + 1 - core
    above = jnp.minimum(me + 2, seq - 2 + core)
    slot = 2 * place + core

    def chain(y, head, part):
        ref = kv.at[2 * y + core, head, :, parts_of[part]]
        return remote(
            ref, ref, r.chain_s.at[y, head, part], r.chain_r.at[y, head, part], "sp", above
        )

    def across(y, head, part):
        ref = kv.at[2 * y + core, head, :, parts_of[part]]
        return remote(
            ref, ref, r.part_s.at[y, head, part], r.part_r.at[y, head, part], "sp", partner
        )

    def ask(i, head):
        return remote(
            query.at[head], r.far_query.at[i, head], r.query_s.at[head], r.query_r.at[i, head],
            "sp", middle,
        )

    def tell(i, head):
        return remote(
            r.own_stats.at[head], r.far_stats.at[i, head], r.stats_s.at[head],
            r.stats_r.at[i, head], "sp", middle,
        )

    def answer(i, head):
        return remote(
            r.part.at[i, head], r.far_part.at[head], r.back_s.at[i, head], r.back_r.at[head],
            "sp", 2 * (half + i) + core,
        )

    def answer_total(i, head):
        return remote(
            r.total.at[i, head], r.far_total.at[head], r.total_s.at[i, head], r.total_r.at[head],
            "sp", 2 * (half + i) + core,
        )

    def pack_keys(head):
        query[head, :, :width_a] = r.qa[:, head, :]
        query[head, :, width_a:] = r.qb[:, head, :]
        for span, ref in zip(key_spans, (r.ka, r.kb)):
            kv[slot, head, :, span[0] : span[0] + span[1]] = ref[:, head, :]

    def pack_values(head):
        for span, ref in zip(value_spans, (r.va, r.vb)):
            kv[slot, head, :, span[0] : span[0] + span[1]] = ref[:, head, :]

    arrived()
    pack_keys(0)
    greeted()

    def give(head, part):
        @pl.when(place < half - 1)
        def _():
            chain(place, head, part).start()

        across(place, head, part).start()

    @pl.when(upper)
    def _():
        ask(place, 0).start()
        for head in range(heads):
            if head:
                pack_keys(head)
            give(head, 0)
        for head in range(heads):
            pack_values(head)
            give(head, 1)

    @pl.when(lower)
    def _():
        for head in range(heads):
            if head:
                pack_keys(head)
            give(head, 0)
            pack_values(head)
            give(head, 1)

    def pass_on(here, head, part):
        for y in range(here):
            chain(y, head, part).wait_recv()
            across(y, head, part).start()
            if here < half - 1:
                chain(y, head, part).start()

    def landed(here, head, part):
        for y in range(here + 1):
            across(y, head, part).wait_recv()

    def gather(here, head, part):
        pass_on(here, head, part)
        landed(here, head, part)

    def score_maps(queries, head, count):
        maps = []
        for group, (begin, width) in enumerate(key_spans):
            wide = queries[:, begin : begin + width]
            block_keys = kv[:count, head, :, begin : begin + width].reshape(count * rows, width)
            size = width // 2
            if size % 128:
                lane = lax.broadcasted_iota(jnp.int32, wide.shape, 1)
                nothing = jnp.zeros_like(wide)
                first = dot_nt(jnp.where(lane < size, wide, nothing), block_keys)
                second = dot_nt(jnp.where(lane < size, nothing, wide), block_keys)
            else:
                first = dot_nt(wide[:, :size], block_keys[:, :size])
                second = dot_nt(wide[:, size:], block_keys[:, size:])
            maps += [first * factors[group], second * factors[group]]
        return maps

    def visible(count):
        query_seg = (slot * rows + lax.broadcasted_iota(jnp.int32, (rows, 1), 0)) // SEG
        key_seg = lax.broadcasted_iota(jnp.int32, (1, count * rows), 1) // SEG
        return query_seg >= key_seg

    def combine(first, second, head, count, group):
        weights = (first - second).astype(BF16)
        begin, size = value_spans[group]
        block_values = kv[:count, head, :, begin : begin + size].reshape(count * rows, size)
        return jnp.dot(weights, block_values, preferred_element_type=F32)

    def finish(mixed, gain, out, head, size):
        mean_sq = jnp.mean(mixed * mixed, axis=1, keepdims=True)
        value = (mixed * lax.rsqrt(mean_sq + EPS) * gain[...]).astype(BF16)
        out[:, pl.ds(pl.multiple_of(head * size, size), size)] = value

    def finish_both(mixed, head):
        finish(mixed[0], r.gain_a, r.heads_a, head, value_a)
        finish(mixed[1], r.gain_b, r.heads_b, head, value_b)

    def own_lower(head, count):
        seen = visible(count)
        maps = [jnp.where(seen, one, -jnp.inf) for one in score_maps(query.at[head], head, count)]
        mixed = []
        for group in range(2):
            parts = []
            for at in range(2):
                scores = maps[2 * group + at]
                expo = jnp.exp2(scores - jnp.max(scores, axis=1, keepdims=True))
                scale = 1.0 / jnp.sum(expo, axis=1, keepdims=True)
                if at:
                    scale = scale * lams[group][head]
                parts.append(expo * scale)
            mixed.append(combine(parts[0], parts[1], head, count, group))
        finish_both(mixed, head)

    def wait_far(i, head):
        for at in range(pair):
            ask(i + at, head).wait_recv()
        for at in range(pair):
            tell(i + at, head).wait_recv()

    def for_upper(i, head, values_here):
        queries = r.far_query[pl.ds(i, pair), head].reshape(pair * rows, wide_q)
        maps = score_maps(queries, head, blocks)
        far = jnp.concatenate(
            [columns_of(r.far_stats[i + at, head]) for at in range(pair)], axis=0
        )
        stats, expos, scales = [], [], []
        for k in range(4):
            far_max, far_sum = far[:, k : k + 1], far[:, 4 + k : 5 + k]
            own_max = jnp.max(maps[k], axis=1, keepdims=True)
            expo = jnp.exp2(maps[k] - own_max)
            top = jnp.maximum(own_max, far_max)
            down = jnp.exp2(own_max - top)
            summed = jnp.sum(expo, axis=1, keepdims=True) * down + far_sum * jnp.exp2(far_max - top)
            stats.append((top, summed))
            expos.append(expo)
            scales.append(down / summed)
        values_here()
        for group in range(2):
            first = expos[2 * group] * scales[2 * group]
            second = expos[2 * group + 1] * (lams[group][head] * scales[2 * group + 1])
            mixed = combine(first, second, head, blocks, group)
            begin, size = (0, value_a) if group == 0 else (value_a, value_b)
            r.part[pl.ds(i, pair), head, :, begin : begin + size] = mixed.astype(BF16).reshape(
                pair, rows, size
            )
        for at in range(pair):
            part = slice(at * rows, (at + 1) * rows)
            r.total[i + at, head] = rows_of(
                [one[0][part] for one in stats] + [one[1][part] for one in stats]
            )
        for at in reversed(range(pair)):
            answer_total(i + at, head).start()
            answer(i + at, head).start()

    def upper_first(head, count):
        seen = visible(count)
        maps = [jnp.where(seen, one, -jnp.inf) for one in score_maps(query.at[head], head, count)]
        tops, sums = [], []
        for k in range(4):
            top = jnp.max(maps[k], axis=1, keepdims=True)
            expo = jnp.exp2(maps[k] - top)
            r.keep[head, k, :, : count * rows] = expo
            tops.append(top)
            sums.append(jnp.sum(expo, axis=1, keepdims=True))
        r.own_stats[head] = rows_of(tops + sums)
        tell(place, head).start()

    def upper_second(head, count):
        answer_total(0, head).wait_recv()
        own = columns_of(r.own_stats[head])
        whole = columns_of(r.far_total[head])
        scales = []
        for k in range(4):
            scale = jnp.exp2(own[:, k : k + 1] - whole[:, k : k + 1]) / whole[:, 4 + k : 5 + k]
            if k % 2:
                scale = scale * lams[k // 2][head]
            scales.append(scale)
        mixed = []
        for group in range(2):
            first = r.keep[head, 2 * group, :, : count * rows] * scales[2 * group]
            second = r.keep[head, 2 * group + 1, :, : count * rows] * scales[2 * group + 1]
            mixed.append(combine(first, second, head, count, group))
        answer(0, head).wait_recv()
        far = r.far_part[head].astype(F32)
        finish_both([mixed[0] + far[:, :value_a], mixed[1] + far[:, value_a:]], head)

    for here in range(half):

        @pl.when((place == here) & lower)
        def _():
            meanwhile()

            pass_on(here, 0, 0)

            def values_here(head):
                landed(here, head, 1)

            def step(head, carry):
                landed(here, head, 0)
                pl.when(head == 0)(lambda: pass_on(here, 0, 1))
                if here < half - 1:
                    values_here(head)
                if here == half - 1:

                    def each(i, inner):
                        wait_far(i * pair, head)
                        for_upper(i * pair, head, lambda: None)
                        return inner

                    wait_far(0, head)
                    for_upper(0, head, lambda: values_here(head))
                    lax.fori_loop(1, half // pair, each, 0)
                own_lower(head, 2 * here + 2)
                if here:

                    @pl.when((head == 0) & (heads > 1))
                    def _():
                        pass_on(here, min(1, heads - 1), 0)
                        pass_on(here, min(1, heads - 1), 1)

                    @pl.when(head + 2 < heads)
                    def _():
                        pass_on(here, head + 2, 0)
                        pass_on(here, head + 2, 1)

                return carry

            lax.fori_loop(0, heads, step, 0)

        @pl.when((place == here) & upper)
        def _():
            def step(head, carry):
                gather(here, head, 0)
                upper_first(head, 2 * here + 2)
                if here < half - 1:
                    chain(here, head, 0).wait_send()

                @pl.when(head + 1 < heads)
                def _():
                    ask(place, head + 1).start()

                return carry

            lax.fori_loop(0, heads, step, 0)
            meanwhile()

            def rest(head, carry):
                gather(here, head, 1)
                return carry

            lax.fori_loop(0, heads, rest, 0)

            def second(head, carry):
                upper_second(head, 2 * here + 2)
                return carry

            lax.fori_loop(0, heads, second, 0)

    def drain():
        for here in range(half):

            @pl.when(place == here)
            def _():
                def each(head, carry):
                    for y in range(here + 1):
                        for part in range(2):
                            across(y, head, part).wait_send()
                            if here < half - 1:
                                if y == here and part == 0:
                                    pl.when(lower)(chain(y, head, part).wait_send)
                                else:
                                    chain(y, head, part).wait_send()
                    return carry

                lax.fori_loop(0, heads, each, 0)

        @pl.when(upper)
        def _():
            def each(head, carry):
                ask(place, head).wait_send()
                tell(place, head).wait_send()
                return carry

            lax.fori_loop(0, heads, each, 0)

    def answered():
        def each(head, carry):
            for i in range(half):
                answer(i, head).wait_send()
                answer_total(i, head).wait_send()
            return carry

        lax.fori_loop(0, heads, each, 0)

    return drain, answered


def grid_of(count):
    side = math.isqrt(count)
    return (side, side) if side * side == count else (1, count)


def peer_at(dy, dx):
    ny, nx = grid_of(lax.axis_size("tp"))
    me = lax.axis_index("tp")
    return lax.rem(me // nx + dy, ny) * nx + lax.rem(lax.rem(me, nx) + dx, nx)


def peer_offsets():
    ny, nx = grid_of(lax.axis_size("tp"))
    offsets = [(dy, dx) for dy in range(ny) for dx in range(nx) if dy or dx]
    far = lambda one: min(one[0], ny - one[0]) + min(one[1], nx - one[1])
    return sorted(offsets, key=far, reverse=True), ny, nx


def block_of(index, width):
    return pl.ds(pl.multiple_of(index * width, width), width)


def route(r):
    experts, slots, rows = r.select.shape
    square = (rows, rows)
    lane = lax.broadcasted_iota(jnp.int32, square, 1)
    line = lax.broadcasted_iota(jnp.int32, square, 0)
    named = r.routes[...]
    weight = r.route_weight[...]
    share = weight / jnp.sum(weight, axis=0, keepdims=True)
    chosen = jnp.zeros(square, F32)
    gate = jnp.zeros(square, F32)
    for k in range(TOP):
        match = named[k : k + 1] == line
        chosen = chosen + jnp.where(match, 1.0, 0.0)
        gate = gate + jnp.where(match, share[k : k + 1], 0.0)
    earlier = jnp.dot(
        chosen.astype(BF16),
        jnp.where(line < lane, 1.0, 0.0).astype(BF16),
        preferred_element_type=F32,
    )
    slot = lax.broadcasted_iota(jnp.int32, (slots, rows), 0).astype(F32)
    for expert in range(experts):
        pick = (chosen[expert : expert + 1] > 0.5) & (earlier[expert : expert + 1] == slot)
        r.select[expert] = jnp.where(pick, 1.0, 0.0).astype(BF16)
        r.weigh[expert * slots : (expert + 1) * slots, :] = jnp.where(
            pick, gate[expert : expert + 1], 0.0
        )
    weigh = r.weigh[...].T
    high = weigh.astype(BF16)
    r.high[...] = high
    r.low[...] = (weigh - high.astype(F32)).astype(BF16)


def project(r, loaded):
    offsets, _, _ = peer_offsets()
    me = lax.axis_index("tp")
    width = r.stream.shape[1]

    def piece(owner):
        columns = block_of(owner, width)
        return jnp.dot(
            r.heads_a[...], r.proj_a[:, columns], preferred_element_type=F32
        ) + jnp.dot(r.heads_b[...], r.proj_b[:, columns], preferred_element_type=F32)

    loaded()
    copies = []
    for at, offset in enumerate(offsets):
        peer = peer_at(*offset)
        r.branch_out[at] = piece(peer).astype(BF16)
        copy = remote(
            r.branch_out.at[at], r.branch_in.at[at], r.branch_s.at[at], r.branch_r.at[at], "tp", peer
        )
        copy.start()
        copies.append(copy)
    r.branch_own[...] = r.residual[...].astype(F32) + piece(me)

    def settle():
        summed = r.branch_own[...]
        for at, copy in reversed(list(enumerate(copies))):
            copy.wait_recv()
            summed = summed + r.branch_in[at].astype(F32)
        r.stream[...] = summed.astype(BF16)

    def drain():
        for copy in copies:
            copy.wait_send()

    return settle, drain


def experts_part(r):
    offsets, ny, nx = peer_offsets()
    seq, heads = lax.axis_size("sp"), lax.axis_size("tp")
    me, mine = lax.axis_index("sp"), lax.axis_index("tp")
    chips = seq // 2
    chip, core = me // 2, lax.rem(me, 2)
    experts, slots, rows = r.select.shape
    width = r.stream.shape[1]
    square = ny == 2 and nx == 2
    across_x, across_y, across_both = peer_at(0, 1), peer_at(1, 0), peer_at(1, 1)
    top, bottom = pl.ds(0, slots), pl.ds(slots, slots)

    half = chips // 2

    def source(k):
        late = half + lax.rem(lax.rem(chip, half) + 1 + k, half)
        return jnp.where(k < half, k, late)

    def distance(k):
        return lax.rem(chip + chips - source(k), chips)

    def outgoing(step, side):
        target_core = core if side == 0 else 1 - core
        expert = 2 * lax.rem(chip + step, chips) + target_core
        return expert, remote(
            r.send.at[expert],
            r.rows.at[chip, block_of(core, slots), block_of(mine, width)],
            r.out_s.at[step, side],
            r.out_r.at[step, side],
            "sp",
            expert,
        )

    def send_out(steps):
        for step in sorted(steps, key=lambda step: (step == 0, step % 2 == 0, -step)):
            for side in range(2):
                expert, copy = outgoing(step, side)
                picked = jnp.dot(r.select[expert], r.stream[...], preferred_element_type=F32)
                if step == 0 and side == 0:
                    place = (chip, block_of(core, slots), block_of(mine, width))
                    r.rows[place] = picked.astype(BF16)
                else:
                    r.send[expert] = picked.astype(BF16)
                    copy.start()

    def incoming(k, side):
        origin_core = core if side == 0 else 1 - core
        origin = source(k)
        return remote(
            r.send.at[me],
            r.rows.at[origin, block_of(origin_core, slots), block_of(mine, width)],
            r.out_s.at[distance(k), side],
            r.out_r.at[distance(k), side],
            "sp",
            2 * origin + origin_core,
        )

    def land(k):
        @pl.when(distance(k) > 0)
        def _():
            incoming(k, 0).wait_recv()

        incoming(k, 1).wait_recv()

    def spread(step, at, peer, owner):
        ref = r.rows.at[source(step), :, block_of(owner, width)]
        return remote(ref, ref, r.spread_s.at[step, at], r.spread_r.at[step, at], "tp", peer)

    def relay(step, at, peer, owner):
        ref = r.rows.at[source(step), top if at == 0 else bottom, block_of(owner, width)]
        return remote(ref, ref, r.relay_s.at[step, at], r.relay_r.at[step, at], "tp", peer)

    near = ((0, 1), (1, 0)) if square else offsets

    def start_spread(step):
        land(step)
        for at, offset in enumerate(near):
            spread(step, at, peer_at(*offset), mine).start()

    def start_relay(step):
        for at, offset in enumerate(near):
            giver = peer_at(ny - offset[0], nx - offset[1])
            spread(step, at, giver, giver).wait_recv()
        if square:
            relay(step, 0, across_y, across_x).start()
            relay(step, 1, across_x, across_y).start()

    def ready(step):
        if square:
            relay(step, 0, across_y, across_both).wait_recv()
            relay(step, 1, across_x, across_both).wait_recv()

    def compute(step):
        origin = source(step)
        wide = r.rows[origin].astype(F32)
        mean_sq = jnp.mean(wide * wide, axis=1, keepdims=True)
        normed = (wide * lax.rsqrt(mean_sq + EPS) * r.norm_gain[...]).astype(BF16)
        gate = jnp.dot(normed, r.gate[...], preferred_element_type=F32)
        up = jnp.dot(normed, r.up[...], preferred_element_type=F32)
        hidden = (gate / (1.0 + jnp.exp(-gate)) * up).astype(BF16)
        r.down_out[step] = jnp.dot(hidden, r.down[...], preferred_element_type=F32).astype(BF16)

    def first_copies(step):
        if not square:
            return [
                remote(
                    r.down_out.at[step, :, block_of(peer_at(*offset), width)],
                    r.first.at[step, at],
                    r.first_s.at[step, at],
                    r.first_r.at[step, at],
                    "tp",
                    peer_at(*offset),
                )
                for at, offset in enumerate(offsets)
            ]
        plan = (
            (top, across_x, across_both, 1),
            (bottom, across_y, across_both, 3),
            (top, across_x, across_x, 0),
            (bottom, across_y, across_y, 2),
        )
        return [
            remote(
                r.down_out.at[step, part, block_of(owner, width)],
                r.first.at[step, slot],
                r.first_s.at[step, slot],
                r.first_r.at[step, slot],
                "tp",
                peer,
            )
            for part, peer, owner, slot in plan
        ]

    def second_copies(step):
        return [
            remote(
                r.second_out.at[step, at],
                r.second.at[step, at],
                r.second_s.at[step, at],
                r.second_r.at[step, at],
                "tp",
                peer,
            )
            for at, peer in enumerate((across_y, across_x))
        ]

    def start_first(step):
        for copy in first_copies(step):
            copy.start()

    def start_second(step):
        if not square:
            return
        firsts, seconds = first_copies(step), second_copies(step)
        for at, part, owner, slot in ((0, top, across_y, 1), (1, bottom, across_x, 3)):
            firsts[at].wait_recv()
            summed = r.down_out[step, part, block_of(owner, width)].astype(F32)
            summed = summed + r.first[step, slot].astype(F32)
            r.second_out[step, at] = summed.astype(BF16)
            seconds[at].start()

    def home(step, side):
        origin_core = core if side == 0 else 1 - core
        return remote(
            r.summed.at[step, side],
            r.back.at[me],
            r.home_s.at[distance(step), side],
            r.home_r.at[distance(step), side],
            "sp",
            2 * source(step) + origin_core,
        )

    def returned(step, side):
        expert_core = core if side == 0 else 1 - core
        expert = 2 * lax.rem(chip + step, chips) + expert_core
        return remote(
            r.summed.at[step, side],
            r.back.at[expert],
            r.home_s.at[step, side],
            r.home_r.at[step, side],
            "sp",
            expert,
        )

    def start_home(step):
        own = block_of(mine, width)
        firsts = first_copies(step)
        if square:
            seconds = second_copies(step)
            firsts[2].wait_recv()
            firsts[3].wait_recv()
            halves = []
            for at, part, slot in ((0, top, 0), (1, bottom, 2)):
                seconds[at].wait_recv()
                halves.append(
                    r.down_out[step, part, own].astype(F32)
                    + r.first[step, slot].astype(F32)
                    + r.second[step, at].astype(F32)
                )
            r.sums[0] = halves[0].astype(BF16)
            r.sums[1] = halves[1].astype(BF16)
        else:
            summed = r.down_out[step, :, own].astype(F32)
            for at, copy in enumerate(firsts):
                copy.wait_recv()
                summed = summed + r.first[step, at].astype(F32)
            r.sums[0] = summed[:slots].astype(BF16)
            r.sums[1] = summed[slots:].astype(BF16)
        r.summed[step, 0] = r.sums[core]
        r.summed[step, 1] = r.sums[1 - core]

        @pl.when(distance(step) == 0)
        def _():
            r.back[me] = r.summed[step, 0]

        @pl.when(distance(step) > 0)
        def _():
            home(step, 0).start()

        home(step, 1).start()

    def start():
        start_spread(0)

    def first_relay():
        start_relay(0)

    def others():
        def body(k, carry):
            start_relay(k)

            @pl.when(k + 1 < chips)
            def _():
                start_spread(k + 1)

            ready(k)
            start_second(k - 1)

            @pl.when(k >= 2)
            def _():
                start_home(k - 2)

            compute(k)
            start_first(k)
            return carry

        lax.fori_loop(1, chips, body, 0)
        start_home(chips - 2)
        start_second(chips - 1)
        start_home(chips - 1)
        finish()

    def finish():
        def arrive(step, carry):
            @pl.when(step > 0)
            def _():
                returned(step, 0).wait_recv()

            returned(step, 1).wait_recv()
            return carry

        lax.fori_loop(0, chips, arrive, 0)
        back = r.back[...].reshape(experts * slots, width)
        mixed = jnp.dot(r.high[...], back, preferred_element_type=F32)
        mixed = mixed + jnp.dot(r.low[...], back, preferred_element_type=F32)
        r.out[...] = (r.stream[...].astype(F32) + mixed).astype(BF16)

    def drain():
        def each(k, carry):
            @pl.when(k > 0)
            def _():
                outgoing(k, 0)[1].wait_send()

            outgoing(k, 1)[1].wait_send()

            @pl.when(distance(k) > 0)
            def _():
                home(k, 0).wait_send()

            home(k, 1).wait_send()
            for at, offset in enumerate(near):
                spread(k, at, peer_at(*offset), mine).wait_send()
            if square:
                relay(k, 0, across_y, across_x).wait_send()
                relay(k, 1, across_x, across_y).wait_send()
                for copy in second_copies(k):
                    copy.wait_send()
            for copy in first_copies(k):
                copy.wait_send()
            return carry

        lax.fori_loop(0, chips, each, 0)

    return send_out, start, first_relay, ready, compute, start_first, start_spread, others, drain


def layer(args):
    seq, heads_dev = lax.axis_size("sp"), lax.axis_size("tp")
    rows, heads, width_a = args["qa"].shape
    width_b = args["qb"].shape[2]
    value_a, value_b = args["va"].shape[2], args["vb"].shape[2]
    model = args["residual"].shape[1]
    width = model // heads_dev
    chips = seq // 2
    half = chips // 2
    blocks = 2 * half
    slots = 2 * rows * TOP // seq
    _, ny, nx = peer_offsets()
    square = ny == 2 and nx == 2
    spreads = 2 if square else heads_dev - 1
    first_shape = (4, slots, width) if square else (heads_dev - 1, 2 * slots, width)
    dma = pltpu.SemaphoreType.DMA
    big = ("qa", "ka", "va", "qb", "kb", "vb", "residual", "proj_a", "proj_b", "gate", "up", "down")
    small = ("lam_a", "lam_b", "gain_a", "gain_b", "norm_gain", "routes", "route_weight")

    def landing(name):
        shape = args[name].shape
        if name == "residual":
            shape = (rows, width)
        if len(shape) == 3 and name in ("gate", "up", "down"):
            shape = shape[1:]
        return pltpu.VMEM(shape, args[name].dtype)

    scratch = {name: landing(name) for name in big}
    scratch.update(
        load_s=dma((len(big),)),
        go=pltpu.SemaphoreType.REGULAR,
        heads_a=pltpu.VMEM((rows, heads * value_a), BF16),
        heads_b=pltpu.VMEM((rows, heads * value_b), BF16),
        kv=pltpu.VMEM((blocks, heads, rows, width_a + value_a + width_b + value_b), BF16),
        query=pltpu.VMEM((heads, rows, width_a + width_b), BF16),
        far_query=pltpu.VMEM((half, heads, rows, width_a + width_b), BF16),
        far_stats=pltpu.VMEM((half, heads, 8, rows), F32),
        own_stats=pltpu.VMEM((heads, 8, rows), F32),
        keep=pltpu.VMEM((heads, 4, rows, blocks * rows), F32),
        part=pltpu.VMEM((half, heads, rows, value_a + value_b), BF16),
        far_part=pltpu.VMEM((heads, rows, value_a + value_b), BF16),
        total=pltpu.VMEM((half, heads, 8, rows), F32),
        far_total=pltpu.VMEM((heads, 8, rows), F32),
        chain_s=dma((half, heads, 2)), chain_r=dma((half, heads, 2)),
        part_s=dma((half, heads, 2)), part_r=dma((half, heads, 2)),
        query_s=dma((heads,)), query_r=dma((half, heads)),
        stats_s=dma((heads,)), stats_r=dma((half, heads)),
        back_s=dma((half, heads)), back_r=dma((heads,)),
        total_s=dma((half, heads)), total_r=dma((heads,)),
        branch_out=pltpu.VMEM((heads_dev - 1, rows, width), BF16),
        branch_own=pltpu.VMEM((rows, width), F32),
        branch_in=pltpu.VMEM((heads_dev - 1, rows, width), BF16),
        branch_s=dma((heads_dev - 1,)), branch_r=dma((heads_dev - 1,)),
        stream=pltpu.VMEM((rows, width), BF16),
        select=pltpu.VMEM((seq, slots, rows), BF16),
        weigh=pltpu.VMEM((seq * slots, rows), F32),
        high=pltpu.VMEM((rows, seq * slots), BF16),
        low=pltpu.VMEM((rows, seq * slots), BF16),
        send=pltpu.VMEM((seq, slots, width), BF16),
        rows=pltpu.VMEM((chips, 2 * slots, model), BF16),
        out_s=dma((chips, 2)), out_r=dma((chips, 2)),
        spread_s=dma((chips, spreads)), spread_r=dma((chips, spreads)),
        relay_s=dma((chips, 2)), relay_r=dma((chips, 2)),
        down_out=pltpu.VMEM((chips, 2 * slots, model), BF16),
        first=pltpu.VMEM((chips,) + first_shape, BF16),
        first_s=dma((chips, first_shape[0])), first_r=dma((chips, first_shape[0])),
        second_out=pltpu.VMEM((chips, 2, slots, width), BF16),
        second=pltpu.VMEM((chips, 2, slots, width), BF16),
        second_s=dma((chips, 2)), second_r=dma((chips, 2)),
        sums=pltpu.VMEM((2, slots, width), BF16),
        summed=pltpu.VMEM((chips, 2, slots, width), BF16),
        back=pltpu.VMEM((seq, slots, width), BF16),
        home_s=dma((chips, 2)), home_r=dma((chips, 2)),
    )

    def kernel(*refs):
        small_refs = refs[: len(small)]
        hbm = Refs(big, refs[len(small) : len(small) + len(big)])
        at = len(small) + len(big)
        r = Refs(
            small + ("out",) + tuple(scratch), tuple(small_refs) + (refs[at],) + tuple(refs[at + 1 :])
        )

        def load(name):
            source = getattr(hbm, name)
            if name == "residual":
                source = source.at[:, block_of(lax.axis_index("tp"), width)]
            if name in ("gate", "up", "down"):
                source = source.at[0]
            return pltpu.make_async_copy(source, getattr(r, name), r.load_s.at[big.index(name)])

        def wait(*names):
            for name in names:
                load(name).wait()

        for name in big:
            load(name).start()
        greeted = greet(("sp", "tp"))
        (
            send_out, start, first_relay, ready, compute, start_first, start_spread, others,
            drain_experts,
        ) = experts_part(r)
        chip = lax.axis_index("sp") // 2
        drain_heads, answered = attend(
            r, lambda: wait("qa", "ka", "va", "qb", "kb", "vb"), greeted, lambda: route(r)
        )

        settle, drain_branch = project(r, lambda: wait("residual", "proj_a", "proj_b"))
        wait("gate", "up", "down")

        @pl.when(chip == half - 1)
        def _():
            answered()
            if half > 1:
                pl.semaphore_signal(
                    r.go, inc=1, device_id={"sp": lax.rem(lax.axis_index("sp"), 2)}, device_id_type=MESH
                )

        @pl.when(chip == 0)
        def _():
            settle()
            send_out(range(half))
            start()
            first_relay()
            ready(0)
            compute(0)
            start_first(0)
            if half > 1:
                pl.semaphore_wait(r.go, 1)
            send_out(range(half, chips))
            start_spread(1)

        @pl.when(chip > 0)
        def _():
            start()
            settle()
            send_out(range(chips))
            first_relay()
            start_spread(1)
            ready(0)
            compute(0)
            start_first(0)

        others()
        drain_heads()
        drain_branch()
        drain_experts()

    vmem = pl.BlockSpec(memory_space=pltpu.VMEM)
    specs = [pl.BlockSpec(memory_space=pltpu.SMEM)] * 2 + [vmem] * (len(small) - 2)
    specs += [pl.BlockSpec(memory_space=pl.ANY)] * len(big)
    return pl.pallas_call(
        kernel,
        out_shape=jax.ShapeDtypeStruct((rows, width), BF16),
        in_specs=specs,
        out_specs=vmem,
        scratch_shapes=list(scratch.values()),
        compiler_params=pltpu.CompilerParams(
            collective_id=0, has_side_effects=True, vmem_limit_bytes=56 * 2**20
        ),
        name="layer",
    )(*[args[name] for name in small + big])


def local(
    residual,
    query_a,
    keys_a,
    values_a,
    query_b,
    keys_b,
    values_b,
    lambda_a,
    lambda_b,
    gain_a,
    gain_b,
    proj_a,
    proj_b,
    norm_gain,
    routes,
    route_weight,
    expert_gate,
    expert_up,
    expert_down,
):
    args = dict(
        residual=residual,
        qa=query_a,
        ka=keys_a,
        va=values_a,
        qb=query_b,
        kb=keys_b,
        vb=values_b,
        lam_a=lambda_a,
        lam_b=lambda_b,
        gain_a=gain_a.reshape(1, -1),
        gain_b=gain_b.reshape(1, -1),
        proj_a=proj_a,
        proj_b=proj_b,
        norm_gain=norm_gain.reshape(1, -1),
        routes=routes.T,
        route_weight=route_weight.T,
        gate=expert_gate,
        up=expert_up,
        down=expert_down,
    )
    return layer(args)


def solution(mesh):
    placed = (
        P("sp", None),
        P("sp", "tp", None),
        P("sp", "tp", None),
        P("sp", "tp", None),
        P("sp", "tp", None),
        P("sp", "tp", None),
        P("sp", "tp", None),
        P("tp"),
        P("tp"),
        P(),
        P(),
        P("tp", None),
        P("tp", None),
        P(),
        P("sp", None),
        P("sp", None),
        P("sp", None, "tp"),
        P("sp", None, "tp"),
        P("sp", "tp", None),
    )
    return jax.shard_map(
        local, mesh=mesh, in_specs=placed, out_specs=P("sp", "tp"), check_vma=False
    )
```

```python
import math

import jax
import jax.numpy as jnp
from jax import lax
from jax.experimental import pallas as pl
from jax.experimental.pallas import tpu as pltpu
from jax.sharding import PartitionSpec as P

SEG = 64
TOP = 2
EPS = 1e-06

LOG2E = 1.4426950408889634
MESH = pl.DeviceIdType.MESH
F32 = jnp.float32
BF16 = jnp.bfloat16


def dot_nt(left, right):
    return lax.dot_general(left, right, (((1,), (1,)), ((), ())), preferred_element_type=F32)


def remote(source, target, send_sem, recv_sem, axis, peer):
    return pltpu.make_async_remote_copy(
        src_ref=source,
        dst_ref=target,
        send_sem=send_sem,
        recv_sem=recv_sem,
        device_id={axis: peer},
        device_id_type=MESH,
    )


def wait_bytes(ref, semaphore):
    pltpu.make_async_copy(ref, ref, semaphore).wait()


def greet(axes):
    barrier = pltpu.get_barrier_semaphore()
    total = 0
    for axis in axes:
        peers = lax.axis_size(axis)
        me = lax.axis_index(axis)
        for step in range(1, peers):
            pl.semaphore_signal(
                barrier, inc=1, device_id={axis: lax.rem(me + step, peers)}, device_id_type=MESH
            )
        total += peers - 1
    return lambda: pl.semaphore_wait(barrier, total)


def columns_of(stats):
    repeat = stats.shape[1] // stats.shape[0]
    return jnp.concatenate([stats] * repeat, axis=0).T


def rows_of(columns):
    rows = columns[0].shape[0]
    lane = lax.broadcasted_iota(jnp.int32, (rows, rows), 1)
    tile = jnp.zeros((rows, rows), F32)
    for at, column in enumerate(columns):
        tile = jnp.where(lane == at, column, tile)
    return tile.T[: len(columns)]


class Refs:
    def __init__(self, names, refs):
        for name, ref in zip(names, refs):
            setattr(self, name, ref)


def attend(r, arrived, greeted, meanwhile):
    seq = lax.axis_size("sp")
    rows, heads, width_a = r.qa.shape
    width_b = r.qb.shape[2]
    value_a, value_b = r.va.shape[2], r.vb.shape[2]
    key_a, key_b = width_a // 2, width_b // 2
    chips = seq // 2
    half = chips // 2
    blocks = 2 * half
    pair = 2 - half % 2
    wide_q = width_a + width_b
    key_spans = ((0, width_a), (width_a, width_b))
    value_spans = ((wide_q, value_a), (wide_q + value_a, value_b))
    parts_of = (pl.ds(0, wide_q), pl.ds(wide_q, value_a + value_b))
    factors = (key_a ** (-0.5) * LOG2E, key_b ** (-0.5) * LOG2E)
    lams = (r.lam_a, r.lam_b)
    kv, query = r.kv, r.query

    me = lax.axis_index("sp")
    chip, core = me // 2, lax.rem(me, 2)
    upper = chip >= half
    lower = chip < half
    place = lax.rem(chip, half)
    middle = 2 * (half - 1) + core
    partner = 2 * chip + 1 - core
    above = jnp.minimum(me + 2, seq - 2 + core)
    slot = 2 * place + core

    def chain(y, head, part):
        ref = kv.at[2 * y + core, head, :, parts_of[part]]
        return remote(
            ref, ref, r.chain_s.at[y, head, part], r.chain_r.at[y, head, part], "sp", above
        )

    def across(y, head, part):
        ref = kv.at[2 * y + core, head, :, parts_of[part]]
        return remote(
            ref, ref, r.part_s.at[0], r.part_r.at[head, part], "sp", partner
        )

    def ask(i, head):
        return remote(
            query.at[head], r.far_query.at[i, head], r.query_s.at[0], r.query_r.at[i, head],
            "sp", middle,
        )

    def tell(i, head):
        return remote(
            r.own_stats.at[head], r.far_stats.at[i, head], r.stats_s.at[0],
            r.stats_r.at[i, head], "sp", middle,
        )

    def answer(i, head):
        return remote(
            r.part.at[i, head], r.far_part.at[head], r.back_s.at[0], r.back_r.at[head],
            "sp", 2 * (half + i) + core,
        )

    def answer_total(i, head):
        return remote(
            r.total.at[i, head], r.far_total.at[head], r.total_s.at[0], r.total_r.at[head],
            "sp", 2 * (half + i) + core,
        )

    def pack_keys(head):
        query[head, :, :width_a] = r.qa[:, head, :]
        query[head, :, width_a:] = r.qb[:, head, :]
        for span, ref in zip(key_spans, (r.ka, r.kb)):
            kv[slot, head, :, span[0] : span[0] + span[1]] = ref[:, head, :]

    def pack_values(head):
        for span, ref in zip(value_spans, (r.va, r.vb)):
            kv[slot, head, :, span[0] : span[0] + span[1]] = ref[:, head, :]

    arrived()
    pack_keys(0)
    greeted()

    def give(head, part):
        @pl.when(place < half - 1)
        def _():
            chain(place, head, part).start()

        across(place, head, part).start()

    @pl.when(upper)
    def _():
        ask(place, 0).start()
        for head in range(heads):
            if head:
                pack_keys(head)
            give(head, 0)
        for head in range(heads):
            pack_values(head)
            give(head, 1)

    @pl.when(lower)
    def _():
        for head in range(heads):
            if head:
                pack_keys(head)
            give(head, 0)
            pack_values(head)
            give(head, 1)

    def pass_on(here, head, part):
        for y in range(here):
            chain(y, head, part).wait_recv()
            across(y, head, part).start()
            if here < half - 1:
                chain(y, head, part).start()

    def landed(here, head, part):
        wait_bytes(kv.at[: here + 1, head, :, parts_of[part]], r.part_r.at[head, part])

    def gather(here, head, part):
        pass_on(here, head, part)
        landed(here, head, part)

    def score_maps(queries, head, count):
        maps = []
        for group, (begin, width) in enumerate(key_spans):
            wide = queries[:, begin : begin + width]
            block_keys = kv[:count, head, :, begin : begin + width].reshape(count * rows, width)
            size = width // 2
            if size % 128:
                lane = lax.broadcasted_iota(jnp.int32, wide.shape, 1)
                nothing = jnp.zeros_like(wide)
                first = dot_nt(jnp.where(lane < size, wide, nothing), block_keys)
                second = dot_nt(jnp.where(lane < size, nothing, wide), block_keys)
            else:
                first = dot_nt(wide[:, :size], block_keys[:, :size])
                second = dot_nt(wide[:, size:], block_keys[:, size:])
            maps += [first * factors[group], second * factors[group]]
        return maps

    def visible(count):
        query_seg = (slot * rows + lax.broadcasted_iota(jnp.int32, (rows, 1), 0)) // SEG
        key_seg = lax.broadcasted_iota(jnp.int32, (1, count * rows), 1) // SEG
        return query_seg >= key_seg

    def combine(first, second, head, count, group):
        weights = (first - second).astype(BF16)
        begin, size = value_spans[group]
        block_values = kv[:count, head, :, begin : begin + size].reshape(count * rows, size)
        return jnp.dot(weights, block_values, preferred_element_type=F32)

    def finish(mixed, gain, out, head, size):
        mean_sq = jnp.mean(mixed * mixed, axis=1, keepdims=True)
        value = (mixed * lax.rsqrt(mean_sq + EPS) * gain[...]).astype(BF16)
        out[:, pl.ds(pl.multiple_of(head * size, size), size)] = value

    def finish_both(mixed, head):
        finish(mixed[0], r.gain_a, r.heads_a, head, value_a)
        finish(mixed[1], r.gain_b, r.heads_b, head, value_b)

    def own_lower(head, count):
        seen = visible(count)
        maps = [jnp.where(seen, one, -jnp.inf) for one in score_maps(query.at[head], head, count)]
        mixed = []
        for group in range(2):
            parts = []
            for at in range(2):
                scores = maps[2 * group + at]
                expo = jnp.exp2(scores - jnp.max(scores, axis=1, keepdims=True))
                scale = 1.0 / jnp.sum(expo, axis=1, keepdims=True)
                if at:
                    scale = scale * lams[group][head]
                parts.append(expo * scale)
            mixed.append(combine(parts[0], parts[1], head, count, group))
        finish_both(mixed, head)

    def wait_far(i, head):
        for at in range(pair):
            ask(i + at, head).wait_recv()
        for at in range(pair):
            tell(i + at, head).wait_recv()

    def for_upper(i, head, values_here):
        queries = r.far_query[pl.ds(i, pair), head].reshape(pair * rows, wide_q)
        maps = score_maps(queries, head, blocks)
        far = jnp.concatenate(
            [columns_of(r.far_stats[i + at, head]) for at in range(pair)], axis=0
        )
        stats, expos, scales = [], [], []
        for k in range(4):
            far_max, far_sum = far[:, k : k + 1], far[:, 4 + k : 5 + k]
            own_max = jnp.max(maps[k], axis=1, keepdims=True)
            expo = jnp.exp2(maps[k] - own_max)
            top = jnp.maximum(own_max, far_max)
            down = jnp.exp2(own_max - top)
            summed = jnp.sum(expo, axis=1, keepdims=True) * down + far_sum * jnp.exp2(far_max - top)
            stats.append((top, summed))
            expos.append(expo)
            scales.append(down / summed)
        values_here()
        for group in range(2):
            first = expos[2 * group] * scales[2 * group]
            second = expos[2 * group + 1] * (lams[group][head] * scales[2 * group + 1])
            mixed = combine(first, second, head, blocks, group)
            begin, size = (0, value_a) if group == 0 else (value_a, value_b)
            r.part[pl.ds(i, pair), head, :, begin : begin + size] = mixed.astype(BF16).reshape(
                pair, rows, size
            )
        for at in range(pair):
            part = slice(at * rows, (at + 1) * rows)
            r.total[i + at, head] = rows_of(
                [one[0][part] for one in stats] + [one[1][part] for one in stats]
            )
        for at in reversed(range(pair)):
            answer_total(i + at, head).start()
            answer(i + at, head).start()

    def upper_first(head, count):
        seen = visible(count)
        maps = [jnp.where(seen, one, -jnp.inf) for one in score_maps(query.at[head], head, count)]
        tops, sums = [], []
        for k in range(4):
            top = jnp.max(maps[k], axis=1, keepdims=True)
            expo = jnp.exp2(maps[k] - top)
            r.keep[head, k, :, : count * rows] = expo
            tops.append(top)
            sums.append(jnp.sum(expo, axis=1, keepdims=True))
        r.own_stats[head] = rows_of(tops + sums)
        tell(place, head).start()

    def upper_second(head, count):
        answer_total(0, head).wait_recv()
        own = columns_of(r.own_stats[head])
        whole = columns_of(r.far_total[head])
        scales = []
        for k in range(4):
            scale = jnp.exp2(own[:, k : k + 1] - whole[:, k : k + 1]) / whole[:, 4 + k : 5 + k]
            if k % 2:
                scale = scale * lams[k // 2][head]
            scales.append(scale)
        mixed = []
        for group in range(2):
            first = r.keep[head, 2 * group, :, : count * rows] * scales[2 * group]
            second = r.keep[head, 2 * group + 1, :, : count * rows] * scales[2 * group + 1]
            mixed.append(combine(first, second, head, count, group))
        answer(0, head).wait_recv()
        far = r.far_part[head].astype(F32)
        finish_both([mixed[0] + far[:, :value_a], mixed[1] + far[:, value_a:]], head)

    for here in range(half):

        @pl.when((place == here) & lower)
        def _():
            meanwhile()

            pass_on(here, 0, 0)

            def values_here(head):
                landed(here, head, 1)

            def step(head, carry):
                landed(here, head, 0)
                pl.when(head == 0)(lambda: pass_on(here, 0, 1))
                if here < half - 1:
                    values_here(head)
                if here == half - 1:

                    def each(i, inner):
                        wait_far(i * pair, head)
                        for_upper(i * pair, head, lambda: None)
                        return inner

                    wait_far(0, head)
                    for_upper(0, head, lambda: values_here(head))
                    lax.fori_loop(1, half // pair, each, 0)
                own_lower(head, 2 * here + 2)
                if here:

                    @pl.when((head == 0) & (heads > 1))
                    def _():
                        pass_on(here, min(1, heads - 1), 0)
                        pass_on(here, min(1, heads - 1), 1)

                    @pl.when(head + 2 < heads)
                    def _():
                        pass_on(here, head + 2, 0)
                        pass_on(here, head + 2, 1)

                return carry

            lax.fori_loop(0, heads, step, 0)

        @pl.when((place == here) & upper)
        def _():
            def step(head, carry):
                gather(here, head, 0)
                upper_first(head, 2 * here + 2)
                if here < half - 1:
                    chain(here, head, 0).wait_send()

                @pl.when(head + 1 < heads)
                def _():
                    ask(place, head + 1).start()

                return carry

            lax.fori_loop(0, heads, step, 0)
            meanwhile()

            def rest(head, carry):
                gather(here, head, 1)
                return carry

            lax.fori_loop(0, heads, rest, 0)

            def second(head, carry):
                upper_second(head, 2 * here + 2)
                return carry

            lax.fori_loop(0, heads, second, 0)

    def drain():
        for here in range(half):

            @pl.when(place == here)
            def _():
                wait_bytes(kv.at[: here + 1], r.part_s.at[0])
                if here < half - 1:

                    def each(head, carry):
                        for y in range(here + 1):
                            if y < here:
                                chain(y, head, 0).wait_send()
                            else:
                                pl.when(lower)(chain(y, head, 0).wait_send)
                            chain(y, head, 1).wait_send()
                        return carry

                    lax.fori_loop(0, heads, each, 0)

        @pl.when(upper)
        def _():
            wait_bytes(query, r.query_s.at[0])
            wait_bytes(r.own_stats, r.stats_s.at[0])

    def answered():
        wait_bytes(r.part, r.back_s.at[0])
        wait_bytes(r.total, r.total_s.at[0])

    return drain, answered


def grid_of(count):
    side = math.isqrt(count)
    return (side, side) if side * side == count else (1, count)


def peer_at(dy, dx):
    ny, nx = grid_of(lax.axis_size("tp"))
    me = lax.axis_index("tp")
    return lax.rem(me // nx + dy, ny) * nx + lax.rem(lax.rem(me, nx) + dx, nx)


def peer_offsets():
    ny, nx = grid_of(lax.axis_size("tp"))
    offsets = [(dy, dx) for dy in range(ny) for dx in range(nx) if dy or dx]
    far = lambda one: min(one[0], ny - one[0]) + min(one[1], nx - one[1])
    return sorted(offsets, key=far, reverse=True), ny, nx


def block_of(index, width):
    return pl.ds(pl.multiple_of(index * width, width), width)


def route(r):
    experts, slots, rows = r.select.shape
    square = (rows, rows)
    lane = lax.broadcasted_iota(jnp.int32, square, 1)
    line = lax.broadcasted_iota(jnp.int32, square, 0)
    named = r.routes[...]
    weight = r.route_weight[...]
    share = weight / jnp.sum(weight, axis=0, keepdims=True)
    chosen = jnp.zeros(square, F32)
    gate = jnp.zeros(square, F32)
    for k in range(TOP):
        match = named[k : k + 1] == line
        chosen = chosen + jnp.where(match, 1.0, 0.0)
        gate = gate + jnp.where(match, share[k : k + 1], 0.0)
    earlier = jnp.dot(
        chosen.astype(BF16),
        jnp.where(line < lane, 1.0, 0.0).astype(BF16),
        preferred_element_type=F32,
    )
    slot = lax.broadcasted_iota(jnp.int32, (slots, rows), 0).astype(F32)
    for expert in range(experts):
        pick = (chosen[expert : expert + 1] > 0.5) & (earlier[expert : expert + 1] == slot)
        r.select[expert] = jnp.where(pick, 1.0, 0.0).astype(BF16)
        r.weigh[expert * slots : (expert + 1) * slots, :] = jnp.where(
            pick, gate[expert : expert + 1], 0.0
        )
    weigh = r.weigh[...].T
    high = weigh.astype(BF16)
    r.high[...] = high
    r.low[...] = (weigh - high.astype(F32)).astype(BF16)


def project(r, loaded):
    offsets, _, _ = peer_offsets()
    me = lax.axis_index("tp")
    width = r.stream.shape[1]

    def piece(owner):
        columns = block_of(owner, width)
        return jnp.dot(
            r.heads_a[...], r.proj_a[:, columns], preferred_element_type=F32
        ) + jnp.dot(r.heads_b[...], r.proj_b[:, columns], preferred_element_type=F32)

    loaded()
    copies = []
    for at, offset in enumerate(offsets):
        peer = peer_at(*offset)
        r.branch_out[at] = piece(peer).astype(BF16)
        copy = remote(
            r.branch_out.at[at], r.branch_in.at[at], r.branch_s.at[0], r.branch_r.at[at], "tp", peer
        )
        copy.start()
        copies.append(copy)
    r.branch_own[...] = r.residual[...].astype(F32) + piece(me)

    def settle():
        summed = r.branch_own[...]
        for at, copy in reversed(list(enumerate(copies))):
            copy.wait_recv()
            summed = summed + r.branch_in[at].astype(F32)
        r.stream[...] = summed.astype(BF16)

    def drain():
        wait_bytes(r.branch_out, r.branch_s.at[0])

    return settle, drain


def experts_part(r):
    offsets, ny, nx = peer_offsets()
    seq, heads = lax.axis_size("sp"), lax.axis_size("tp")
    me, mine = lax.axis_index("sp"), lax.axis_index("tp")
    chips = seq // 2
    chip, core = me // 2, lax.rem(me, 2)
    experts, slots, rows = r.select.shape
    width = r.stream.shape[1]
    square = ny == 2 and nx == 2
    across_x, across_y, across_both = peer_at(0, 1), peer_at(1, 0), peer_at(1, 1)
    top, bottom = pl.ds(0, slots), pl.ds(slots, slots)

    half = chips // 2

    def source(k):
        late = half + lax.rem(lax.rem(chip, half) + 1 + k, half)
        return jnp.where(k < half, k, late)

    def distance(k):
        return lax.rem(chip + chips - source(k), chips)

    def outgoing(step, side):
        target_core = core if side == 0 else 1 - core
        expert = 2 * lax.rem(chip + step, chips) + target_core
        return expert, remote(
            r.send.at[expert],
            r.rows.at[chip, block_of(core, slots), block_of(mine, width)],
            r.out_s.at[0],
            r.out_r.at[step],
            "sp",
            expert,
        )

    def send_out(steps):
        for step in sorted(steps, key=lambda step: (step == 0, step % 2 == 0, -step)):
            for side in range(2):
                expert, copy = outgoing(step, side)
                picked = jnp.dot(r.select[expert], r.stream[...], preferred_element_type=F32)
                if step == 0 and side == 0:
                    place = (chip, block_of(core, slots), block_of(mine, width))
                    r.rows[place] = picked.astype(BF16)
                else:
                    r.send[expert] = picked.astype(BF16)
                    copy.start()

    def land(k):
        @pl.when(distance(k) > 0)
        def _():
            wait_bytes(r.rows.at[source(k), :, block_of(mine, width)], r.out_r.at[distance(k)])

        @pl.when(distance(k) == 0)
        def _():
            wait_bytes(r.rows.at[source(k), bottom, block_of(mine, width)], r.out_r.at[0])

    def spread(step, at, peer, owner):
        ref = r.rows.at[source(step), :, block_of(owner, width)]
        return remote(ref, ref, r.spread_s.at[0], r.spread_r.at[step], "tp", peer)

    def relay(step, at, peer, owner):
        ref = r.rows.at[source(step), top if at == 0 else bottom, block_of(owner, width)]
        return remote(ref, ref, r.relay_s.at[0], r.relay_r.at[step], "tp", peer)

    near = ((0, 1), (1, 0)) if square else offsets

    def start_spread(step):
        land(step)
        for at, offset in enumerate(near):
            spread(step, at, peer_at(*offset), mine).start()

    def start_relay(step):
        wait_bytes(r.rows.at[source(step), :, : len(near) * width], r.spread_r.at[step])
        if square:
            relay(step, 0, across_y, across_x).start()
            relay(step, 1, across_x, across_y).start()

    def ready(step):
        if square:
            wait_bytes(r.rows.at[source(step), :, :width], r.relay_r.at[step])

    def compute(step):
        origin = source(step)
        wide = r.rows[origin].astype(F32)
        mean_sq = jnp.mean(wide * wide, axis=1, keepdims=True)
        normed = (wide * lax.rsqrt(mean_sq + EPS) * r.norm_gain[...]).astype(BF16)
        gate = jnp.dot(normed, r.gate[...], preferred_element_type=F32)
        up = jnp.dot(normed, r.up[...], preferred_element_type=F32)
        hidden = (gate / (1.0 + jnp.exp(-gate)) * up).astype(BF16)
        r.down_out[step] = jnp.dot(hidden, r.down[...], preferred_element_type=F32).astype(BF16)

    def first_copies(step):
        if not square:
            return [
                remote(
                    r.down_out.at[step, :, block_of(peer_at(*offset), width)],
                    r.first.at[step, at],
                    r.first_s.at[0],
                    r.first_r.at[step, 0],
                    "tp",
                    peer_at(*offset),
                )
                for at, offset in enumerate(offsets)
            ]
        plan = (
            (top, across_x, across_both, 1),
            (bottom, across_y, across_both, 3),
            (top, across_x, across_x, 0),
            (bottom, across_y, across_y, 2),
        )
        return [
            remote(
                r.down_out.at[step, part, block_of(owner, width)],
                r.first.at[step, slot],
                r.first_s.at[0],
                r.first_r.at[step, slot % 2],
                "tp",
                peer,
            )
            for part, peer, owner, slot in plan
        ]

    def second_copies(step):
        return [
            remote(
                r.second_out.at[step, at],
                r.second.at[step, at],
                r.second_s.at[0],
                r.second_r.at[step],
                "tp",
                peer,
            )
            for at, peer in enumerate((across_y, across_x))
        ]

    def start_first(step):
        for copy in first_copies(step):
            copy.start()

    def start_second(step):
        if not square:
            return
        seconds = second_copies(step)
        wait_bytes(r.first.at[step, :2], r.first_r.at[step, 1])
        for at, part, owner, slot in ((0, top, across_y, 1), (1, bottom, across_x, 3)):
            summed = r.down_out[step, part, block_of(owner, width)].astype(F32)
            summed = summed + r.first[step, slot].astype(F32)
            r.second_out[step, at] = summed.astype(BF16)
            seconds[at].start()

    def home(step, side):
        origin_core = core if side == 0 else 1 - core
        return remote(
            r.summed.at[step, side],
            r.back.at[me],
            r.home_s.at[0],
            r.home_r.at[0],
            "sp",
            2 * source(step) + origin_core,
        )

    def start_home(step):
        own = block_of(mine, width)
        if square:
            wait_bytes(r.first.at[step, :2], r.first_r.at[step, 0])
            wait_bytes(r.second.at[step], r.second_r.at[step])
            halves = []
            for at, part, slot in ((0, top, 0), (1, bottom, 2)):
                halves.append(
                    r.down_out[step, part, own].astype(F32)
                    + r.first[step, slot].astype(F32)
                    + r.second[step, at].astype(F32)
                )
            r.sums[0] = halves[0].astype(BF16)
            r.sums[1] = halves[1].astype(BF16)
        else:
            wait_bytes(r.first.at[step], r.first_r.at[step, 0])
            summed = r.down_out[step, :, own].astype(F32)
            for at in range(len(offsets)):
                summed = summed + r.first[step, at].astype(F32)
            r.sums[0] = summed[:slots].astype(BF16)
            r.sums[1] = summed[slots:].astype(BF16)
        r.summed[step, 0] = r.sums[core]
        r.summed[step, 1] = r.sums[1 - core]

        @pl.when(distance(step) == 0)
        def _():
            r.back[me] = r.summed[step, 0]

        @pl.when(distance(step) > 0)
        def _():
            home(step, 0).start()

        home(step, 1).start()

    def start():
        start_spread(0)

    def first_relay():
        start_relay(0)

    def others():
        def body(k, carry):
            start_relay(k)

            @pl.when(k + 1 < chips)
            def _():
                start_spread(k + 1)

            ready(k)
            start_second(k - 1)

            @pl.when(k >= 2)
            def _():
                start_home(k - 2)

            compute(k)
            start_first(k)
            return carry

        lax.fori_loop(1, chips, body, 0)
        start_home(chips - 2)
        start_second(chips - 1)
        start_home(chips - 1)
        finish()

    def finish():
        wait_bytes(r.back.at[: experts - 1], r.home_r.at[0])
        back = r.back[...].reshape(experts * slots, width)
        mixed = jnp.dot(r.high[...], back, preferred_element_type=F32)
        mixed = mixed + jnp.dot(r.low[...], back, preferred_element_type=F32)
        r.out[...] = (r.stream[...].astype(F32) + mixed).astype(BF16)

    def drain():
        wait_bytes(r.send.at[: experts - 1], r.out_s.at[0])
        wait_bytes(r.back.at[: experts - 1], r.home_s.at[0])
        wait_bytes(r.rows.at[:, :, : len(near) * width], r.spread_s.at[0])
        wait_bytes(r.first, r.first_s.at[0])
        if square:
            wait_bytes(r.rows.at[:, :, :width], r.relay_s.at[0])
            wait_bytes(r.second, r.second_s.at[0])

    return send_out, start, first_relay, ready, compute, start_first, start_spread, others, drain


def layer(args):
    seq, heads_dev = lax.axis_size("sp"), lax.axis_size("tp")
    rows, heads, width_a = args["qa"].shape
    width_b = args["qb"].shape[2]
    value_a, value_b = args["va"].shape[2], args["vb"].shape[2]
    model = args["residual"].shape[1]
    width = model // heads_dev
    chips = seq // 2
    half = chips // 2
    blocks = 2 * half
    slots = 2 * rows * TOP // seq
    _, ny, nx = peer_offsets()
    square = ny == 2 and nx == 2
    first_shape = (4, slots, width) if square else (heads_dev - 1, 2 * slots, width)
    dma = pltpu.SemaphoreType.DMA
    big = ("qa", "ka", "va", "qb", "kb", "vb", "residual", "proj_a", "proj_b", "gate", "up", "down")
    small = ("lam_a", "lam_b", "gain_a", "gain_b", "norm_gain", "routes", "route_weight")

    def landing(name):
        shape = args[name].shape
        if name == "residual":
            shape = (rows, width)
        if len(shape) == 3 and name in ("gate", "up", "down"):
            shape = shape[1:]
        return pltpu.VMEM(shape, args[name].dtype)

    scratch = {name: landing(name) for name in big}
    scratch.update(
        load_s=dma((len(big),)),
        go=pltpu.SemaphoreType.REGULAR,
        heads_a=pltpu.VMEM((rows, heads * value_a), BF16),
        heads_b=pltpu.VMEM((rows, heads * value_b), BF16),
        kv=pltpu.VMEM((blocks, heads, rows, width_a + value_a + width_b + value_b), BF16),
        query=pltpu.VMEM((heads, rows, width_a + width_b), BF16),
        far_query=pltpu.VMEM((half, heads, rows, width_a + width_b), BF16),
        far_stats=pltpu.VMEM((half, heads, 8, rows), F32),
        own_stats=pltpu.VMEM((heads, 8, rows), F32),
        keep=pltpu.VMEM((heads, 4, rows, blocks * rows), F32),
        part=pltpu.VMEM((half, heads, rows, value_a + value_b), BF16),
        far_part=pltpu.VMEM((heads, rows, value_a + value_b), BF16),
        total=pltpu.VMEM((half, heads, 8, rows), F32),
        far_total=pltpu.VMEM((heads, 8, rows), F32),
        chain_s=dma((max(half - 1, 1), heads, 2)), chain_r=dma((max(half - 1, 1), heads, 2)),
        part_s=dma((1,)), part_r=dma((heads, 2)),
        query_s=dma((1,)), query_r=dma((half, heads)),
        stats_s=dma((1,)), stats_r=dma((half, heads)),
        back_s=dma((1,)), back_r=dma((heads,)),
        total_s=dma((1,)), total_r=dma((heads,)),
        branch_out=pltpu.VMEM((heads_dev - 1, rows, width), BF16),
        branch_own=pltpu.VMEM((rows, width), F32),
        branch_in=pltpu.VMEM((heads_dev - 1, rows, width), BF16),
        branch_s=dma((1,)), branch_r=dma((heads_dev - 1,)),
        stream=pltpu.VMEM((rows, width), BF16),
        select=pltpu.VMEM((seq, slots, rows), BF16),
        weigh=pltpu.VMEM((seq * slots, rows), F32),
        high=pltpu.VMEM((rows, seq * slots), BF16),
        low=pltpu.VMEM((rows, seq * slots), BF16),
        send=pltpu.VMEM((seq, slots, width), BF16),
        rows=pltpu.VMEM((chips, 2 * slots, model), BF16),
        out_s=dma((1,)), out_r=dma((chips,)),
        spread_s=dma((1,)), spread_r=dma((chips,)),
        relay_s=dma((1,)), relay_r=dma((chips,)),
        down_out=pltpu.VMEM((chips, 2 * slots, model), BF16),
        first=pltpu.VMEM((chips,) + first_shape, BF16),
        first_s=dma((1,)), first_r=dma((chips, 2)),
        second_out=pltpu.VMEM((chips, 2, slots, width), BF16),
        second=pltpu.VMEM((chips, 2, slots, width), BF16),
        second_s=dma((1,)), second_r=dma((chips,)),
        sums=pltpu.VMEM((2, slots, width), BF16),
        summed=pltpu.VMEM((chips, 2, slots, width), BF16),
        back=pltpu.VMEM((seq, slots, width), BF16),
        home_s=dma((1,)), home_r=dma((1,)),
    )

    def kernel(*refs):
        small_refs = refs[: len(small)]
        hbm = Refs(big, refs[len(small) : len(small) + len(big)])
        at = len(small) + len(big)
        r = Refs(
            small + ("out",) + tuple(scratch), tuple(small_refs) + (refs[at],) + tuple(refs[at + 1 :])
        )

        def load(name):
            source = getattr(hbm, name)
            if name == "residual":
                source = source.at[:, block_of(lax.axis_index("tp"), width)]
            if name in ("gate", "up", "down"):
                source = source.at[0]
            return pltpu.make_async_copy(source, getattr(r, name), r.load_s.at[big.index(name)])

        def wait(*names):
            for name in names:
                load(name).wait()

        for name in big:
            load(name).start()
        greeted = greet(("sp", "tp"))
        (
            send_out, start, first_relay, ready, compute, start_first, start_spread, others,
            drain_experts,
        ) = experts_part(r)
        chip = lax.axis_index("sp") // 2
        drain_heads, answered = attend(
            r, lambda: wait("qa", "ka", "va", "qb", "kb", "vb"), greeted, lambda: route(r)
        )

        settle, drain_branch = project(r, lambda: wait("residual", "proj_a", "proj_b"))
        wait("gate", "up", "down")

        @pl.when(chip == half - 1)
        def _():
            answered()
            if half > 1:
                pl.semaphore_signal(
                    r.go, inc=1, device_id={"sp": lax.rem(lax.axis_index("sp"), 2)}, device_id_type=MESH
                )

        @pl.when(chip == 0)
        def _():
            settle()
            send_out(range(half))
            start()
            first_relay()
            ready(0)
            compute(0)
            start_first(0)
            if half > 1:
                pl.semaphore_wait(r.go, 1)
            send_out(range(half, chips))
            start_spread(1)

        @pl.when(chip > 0)
        def _():
            start()
            settle()
            send_out(range(chips))
            first_relay()
            start_spread(1)
            ready(0)
            compute(0)
            start_first(0)

        others()
        drain_heads()
        drain_branch()
        drain_experts()

    vmem = pl.BlockSpec(memory_space=pltpu.VMEM)
    specs = [pl.BlockSpec(memory_space=pltpu.SMEM)] * 2 + [vmem] * (len(small) - 2)
    specs += [pl.BlockSpec(memory_space=pl.ANY)] * len(big)
    return pl.pallas_call(
        kernel,
        out_shape=jax.ShapeDtypeStruct((rows, width), BF16),
        in_specs=specs,
        out_specs=vmem,
        scratch_shapes=list(scratch.values()),
        compiler_params=pltpu.CompilerParams(
            collective_id=0, has_side_effects=True, vmem_limit_bytes=56 * 2**20
        ),
        name="layer",
    )(*[args[name] for name in small + big])


def local(
    residual,
    query_a,
    keys_a,
    values_a,
    query_b,
    keys_b,
    values_b,
    lambda_a,
    lambda_b,
    gain_a,
    gain_b,
    proj_a,
    proj_b,
    norm_gain,
    routes,
    route_weight,
    expert_gate,
    expert_up,
    expert_down,
):
    args = dict(
        residual=residual,
        qa=query_a,
        ka=keys_a,
        va=values_a,
        qb=query_b,
        kb=keys_b,
        vb=values_b,
        lam_a=lambda_a,
        lam_b=lambda_b,
        gain_a=gain_a.reshape(1, -1),
        gain_b=gain_b.reshape(1, -1),
        proj_a=proj_a,
        proj_b=proj_b,
        norm_gain=norm_gain.reshape(1, -1),
        routes=routes.T,
        route_weight=route_weight.T,
        gate=expert_gate,
        up=expert_up,
        down=expert_down,
    )
    return layer(args)


def solution(mesh):
    placed = (
        P("sp", None),
        P("sp", "tp", None),
        P("sp", "tp", None),
        P("sp", "tp", None),
        P("sp", "tp", None),
        P("sp", "tp", None),
        P("sp", "tp", None),
        P("tp"),
        P("tp"),
        P(),
        P(),
        P("tp", None),
        P("tp", None),
        P(),
        P("sp", None),
        P("sp", None),
        P("sp", None, "tp"),
        P("sp", None, "tp"),
        P("sp", "tp", None),
    )
    return jax.shard_map(
        local, mesh=mesh, in_specs=placed, out_specs=P("sp", "tp"), check_vma=False
    )
```

```python
import math

import jax
import jax.numpy as jnp
from jax import lax
from jax.experimental import pallas as pl
from jax.experimental.pallas import tpu as pltpu
from jax.sharding import PartitionSpec as P

SEG = 64
TOP = 2
EPS = 1e-06

LOG2E = 1.4426950408889634
MESH = pl.DeviceIdType.MESH
F32 = jnp.float32
BF16 = jnp.bfloat16


def dot_nt(left, right):
    return lax.dot_general(left, right, (((1,), (1,)), ((), ())), preferred_element_type=F32)


def remote(source, target, send_sem, recv_sem, axis, peer):
    return pltpu.make_async_remote_copy(
        src_ref=source,
        dst_ref=target,
        send_sem=send_sem,
        recv_sem=recv_sem,
        device_id={axis: peer},
        device_id_type=MESH,
    )


def wait_bytes(ref, semaphore):
    pltpu.make_async_copy(ref, ref, semaphore).wait()


def greet(axes):
    barrier = pltpu.get_barrier_semaphore()
    total = 0
    for axis in axes:
        peers = lax.axis_size(axis)
        me = lax.axis_index(axis)
        for step in range(1, peers):
            pl.semaphore_signal(
                barrier, inc=1, device_id={axis: lax.rem(me + step, peers)}, device_id_type=MESH
            )
        total += peers - 1
    return lambda: pl.semaphore_wait(barrier, total)


def columns_of(stats):
    repeat = stats.shape[1] // stats.shape[0]
    return jnp.concatenate([stats] * repeat, axis=0).T


def rows_of(columns):
    rows = columns[0].shape[0]
    lane = lax.broadcasted_iota(jnp.int32, (rows, rows), 1)
    tile = jnp.zeros((rows, rows), F32)
    for at, column in enumerate(columns):
        tile = jnp.where(lane == at, column, tile)
    return tile.T[: len(columns)]


class Refs:
    def __init__(self, names, refs):
        for name, ref in zip(names, refs):
            setattr(self, name, ref)


def attend(r, arrived, greeted, meanwhile):
    seq = lax.axis_size("sp")
    rows, heads, width_a = r.qa.shape
    width_b = r.qb.shape[2]
    value_a, value_b = r.va.shape[2], r.vb.shape[2]
    key_a, key_b = width_a // 2, width_b // 2
    chips = seq // 2
    half = chips // 2
    blocks = 2 * half
    pair = 2 - half % 2
    wide_q = width_a + width_b
    key_spans = ((0, width_a), (width_a, width_b))
    value_spans = ((wide_q, value_a), (wide_q + value_a, value_b))
    parts_of = (pl.ds(0, wide_q), pl.ds(wide_q, value_a + value_b))
    factors = (key_a ** (-0.5) * LOG2E, key_b ** (-0.5) * LOG2E)
    lams = (r.lam_a, r.lam_b)
    kv, query = r.kv, r.query

    me = lax.axis_index("sp")
    chip, core = me // 2, lax.rem(me, 2)
    upper = chip >= half
    lower = chip < half
    place = lax.rem(chip, half)
    middle = 2 * (half - 1) + core
    partner = 2 * chip + 1 - core
    above = jnp.minimum(me + 2, seq - 2 + core)
    slot = 2 * place + core

    def chain(y, head, part):
        ref = kv.at[2 * y + core, head, :, parts_of[part]]
        return remote(
            ref, ref, r.chain_s.at[y, head, part], r.chain_r.at[y, head, part], "sp", above
        )

    def across(y, head, part):
        ref = kv.at[2 * y + core, head, :, parts_of[part]]
        return remote(
            ref, ref, r.part_s.at[0], r.part_r.at[head, part], "sp", partner
        )

    def ask(i, head):
        return remote(
            query.at[head], r.far_query.at[i, head], r.query_s.at[0], r.query_r.at[i, head],
            "sp", middle,
        )

    def tell(i, head):
        return remote(
            r.own_stats.at[head], r.far_stats.at[i, head], r.stats_s.at[0],
            r.stats_r.at[i, head], "sp", middle,
        )

    def answer(i, head):
        return remote(
            r.part.at[i, head], r.far_part.at[head], r.back_s.at[0], r.back_r.at[head],
            "sp", 2 * (half + i) + core,
        )

    def answer_total(i, head):
        return remote(
            r.total.at[i, head], r.far_total.at[head], r.total_s.at[0], r.total_r.at[head],
            "sp", 2 * (half + i) + core,
        )

    def pack_keys(head):
        query[head, :, :width_a] = r.qa[:, head, :]
        query[head, :, width_a:] = r.qb[:, head, :]
        for span, ref in zip(key_spans, (r.ka, r.kb)):
            kv[slot, head, :, span[0] : span[0] + span[1]] = ref[:, head, :]

    def pack_values(head):
        for span, ref in zip(value_spans, (r.va, r.vb)):
            kv[slot, head, :, span[0] : span[0] + span[1]] = ref[:, head, :]

    arrived()
    pack_keys(0)
    greeted()

    def give(head, part):
        @pl.when(place < half - 1)
        def _():
            chain(place, head, part).start()

        across(place, head, part).start()

    @pl.when(upper)
    def _():
        ask(place, 0).start()
        for head in range(heads):
            if head:
                pack_keys(head)
            give(head, 0)
        for head in range(heads):
            pack_values(head)
            give(head, 1)

    @pl.when(lower)
    def _():
        for head in range(heads):
            if head:
                pack_keys(head)
            give(head, 0)
            pack_values(head)
            give(head, 1)

    def pass_on(here, head, part):
        for y in range(here):
            chain(y, head, part).wait_recv()
            across(y, head, part).start()
            if here < half - 1:
                chain(y, head, part).start()

    def landed(here, head, part):
        wait_bytes(kv.at[: here + 1, head, :, parts_of[part]], r.part_r.at[head, part])

    def gather(here, head, part):
        pass_on(here, head, part)
        landed(here, head, part)

    def score_maps(queries, head, count):
        maps = []
        for group, (begin, width) in enumerate(key_spans):
            wide = queries[:, begin : begin + width]
            block_keys = kv[:count, head, :, begin : begin + width].reshape(count * rows, width)
            size = width // 2
            if size % 128:
                lane = lax.broadcasted_iota(jnp.int32, wide.shape, 1)
                nothing = jnp.zeros_like(wide)
                first = dot_nt(jnp.where(lane < size, wide, nothing), block_keys)
                second = dot_nt(jnp.where(lane < size, nothing, wide), block_keys)
            else:
                first = dot_nt(wide[:, :size], block_keys[:, :size])
                second = dot_nt(wide[:, size:], block_keys[:, size:])
            maps += [first * factors[group], second * factors[group]]
        return maps

    def visible(count):
        query_seg = (slot * rows + lax.broadcasted_iota(jnp.int32, (rows, 1), 0)) // SEG
        key_seg = lax.broadcasted_iota(jnp.int32, (1, count * rows), 1) // SEG
        return query_seg >= key_seg

    def combine(first, second, head, count, group):
        weights = (first - second).astype(BF16)
        begin, size = value_spans[group]
        block_values = kv[:count, head, :, begin : begin + size].reshape(count * rows, size)
        return jnp.dot(weights, block_values, preferred_element_type=F32)

    def finish(mixed, gain, out, head, size):
        mean_sq = jnp.mean(mixed * mixed, axis=1, keepdims=True)
        value = (mixed * lax.rsqrt(mean_sq + EPS) * gain[...]).astype(BF16)
        out[:, pl.ds(pl.multiple_of(head * size, size), size)] = value

    def finish_both(mixed, head):
        finish(mixed[0], r.gain_a, r.heads_a, head, value_a)
        finish(mixed[1], r.gain_b, r.heads_b, head, value_b)

    def own_lower(head, count):
        seen = visible(count)
        maps = [jnp.where(seen, one, -jnp.inf) for one in score_maps(query.at[head], head, count)]
        mixed = []
        for group in range(2):
            parts = []
            for at in range(2):
                scores = maps[2 * group + at]
                expo = jnp.exp2(scores - jnp.max(scores, axis=1, keepdims=True))
                scale = 1.0 / jnp.sum(expo, axis=1, keepdims=True)
                if at:
                    scale = scale * lams[group][head]
                parts.append(expo * scale)
            mixed.append(combine(parts[0], parts[1], head, count, group))
        finish_both(mixed, head)

    def wait_far(i, head):
        for at in range(pair):
            ask(i + at, head).wait_recv()
        for at in range(pair):
            tell(i + at, head).wait_recv()

    def for_upper(i, head, values_here):
        queries = r.far_query[pl.ds(i, pair), head].reshape(pair * rows, wide_q)
        maps = score_maps(queries, head, blocks)
        far = jnp.concatenate(
            [columns_of(r.far_stats[i + at, head]) for at in range(pair)], axis=0
        )
        stats, expos, scales = [], [], []
        for k in range(4):
            far_max, far_sum = far[:, k : k + 1], far[:, 4 + k : 5 + k]
            own_max = jnp.max(maps[k], axis=1, keepdims=True)
            expo = jnp.exp2(maps[k] - own_max)
            top = jnp.maximum(own_max, far_max)
            down = jnp.exp2(own_max - top)
            summed = jnp.sum(expo, axis=1, keepdims=True) * down + far_sum * jnp.exp2(far_max - top)
            stats.append((top, summed))
            expos.append(expo)
            scales.append(down / summed)
        values_here()
        for group in range(2):
            first = expos[2 * group] * scales[2 * group]
            second = expos[2 * group + 1] * (lams[group][head] * scales[2 * group + 1])
            mixed = combine(first, second, head, blocks, group)
            begin, size = (0, value_a) if group == 0 else (value_a, value_b)
            r.part[pl.ds(i, pair), head, :, begin : begin + size] = mixed.astype(BF16).reshape(
                pair, rows, size
            )
        for at in range(pair):
            part = slice(at * rows, (at + 1) * rows)
            r.total[i + at, head] = rows_of(
                [one[0][part] for one in stats] + [one[1][part] for one in stats]
            )
        for at in reversed(range(pair)):
            answer_total(i + at, head).start()
            answer(i + at, head).start()

    def upper_first(head, count):
        seen = visible(count)
        maps = [jnp.where(seen, one, -jnp.inf) for one in score_maps(query.at[head], head, count)]
        tops, sums = [], []
        for k in range(4):
            top = jnp.max(maps[k], axis=1, keepdims=True)
            expo = jnp.exp2(maps[k] - top)
            r.keep[head, k, :, : count * rows] = expo
            tops.append(top)
            sums.append(jnp.sum(expo, axis=1, keepdims=True))
        r.own_stats[head] = rows_of(tops + sums)
        tell(place, head).start()

    def upper_second(head, count):
        answer_total(0, head).wait_recv()
        own = columns_of(r.own_stats[head])
        whole = columns_of(r.far_total[head])
        scales = []
        for k in range(4):
            scale = jnp.exp2(own[:, k : k + 1] - whole[:, k : k + 1]) / whole[:, 4 + k : 5 + k]
            if k % 2:
                scale = scale * lams[k // 2][head]
            scales.append(scale)
        mixed = []
        for group in range(2):
            first = r.keep[head, 2 * group, :, : count * rows] * scales[2 * group]
            second = r.keep[head, 2 * group + 1, :, : count * rows] * scales[2 * group + 1]
            mixed.append(combine(first, second, head, count, group))
        answer(0, head).wait_recv()
        far = r.far_part[head].astype(F32)
        finish_both([mixed[0] + far[:, :value_a], mixed[1] + far[:, value_a:]], head)

    for here in range(half):

        @pl.when((place == here) & lower)
        def _():
            meanwhile()

            pass_on(here, 0, 0)

            def values_here(head):
                landed(here, head, 1)

            def step(head, carry):
                landed(here, head, 0)
                pl.when(head == 0)(lambda: pass_on(here, 0, 1))
                if here < half - 1:
                    values_here(head)
                if here == half - 1:

                    def each(i, inner):
                        wait_far(i * pair, head)
                        for_upper(i * pair, head, lambda: None)
                        return inner

                    wait_far(0, head)
                    for_upper(0, head, lambda: values_here(head))
                    lax.fori_loop(1, half // pair, each, 0)
                own_lower(head, 2 * here + 2)
                if here:

                    @pl.when((head == 0) & (heads > 1))
                    def _():
                        pass_on(here, min(1, heads - 1), 0)
                        pass_on(here, min(1, heads - 1), 1)

                    @pl.when(head + 2 < heads)
                    def _():
                        pass_on(here, head + 2, 0)
                        pass_on(here, head + 2, 1)

                return carry

            lax.fori_loop(0, heads, step, 0)

        @pl.when((place == here) & upper)
        def _():
            def step(head, carry):
                gather(here, head, 0)
                upper_first(head, 2 * here + 2)
                if here < half - 1:
                    chain(here, head, 0).wait_send()

                @pl.when(head + 1 < heads)
                def _():
                    ask(place, head + 1).start()

                return carry

            lax.fori_loop(0, heads, step, 0)
            meanwhile()

            def rest(head, carry):
                gather(here, head, 1)
                return carry

            lax.fori_loop(0, heads, rest, 0)

            def second(head, carry):
                upper_second(head, 2 * here + 2)
                return carry

            lax.fori_loop(0, heads, second, 0)

    def drain():
        for here in range(half):

            @pl.when(place == here)
            def _():
                wait_bytes(kv.at[: here + 1], r.part_s.at[0])
                if here < half - 1:

                    def each(head, carry):
                        for y in range(here + 1):
                            if y < here:
                                chain(y, head, 0).wait_send()
                            else:
                                pl.when(lower)(chain(y, head, 0).wait_send)
                            chain(y, head, 1).wait_send()
                        return carry

                    lax.fori_loop(0, heads, each, 0)

        @pl.when(upper)
        def _():
            wait_bytes(query, r.query_s.at[0])
            wait_bytes(r.own_stats, r.stats_s.at[0])

    def answered():
        wait_bytes(r.part, r.back_s.at[0])
        wait_bytes(r.total, r.total_s.at[0])

    return drain, answered


def grid_of(count):
    side = math.isqrt(count)
    return (side, side) if side * side == count else (1, count)


def peer_at(dy, dx):
    ny, nx = grid_of(lax.axis_size("tp"))
    me = lax.axis_index("tp")
    return lax.rem(me // nx + dy, ny) * nx + lax.rem(lax.rem(me, nx) + dx, nx)


def peer_offsets():
    ny, nx = grid_of(lax.axis_size("tp"))
    offsets = [(dy, dx) for dy in range(ny) for dx in range(nx) if dy or dx]
    far = lambda one: min(one[0], ny - one[0]) + min(one[1], nx - one[1])
    return sorted(offsets, key=far, reverse=True), ny, nx


def block_of(index, width):
    return pl.ds(pl.multiple_of(index * width, width), width)


def route(r):
    experts, slots, rows = r.select.shape
    square = (rows, rows)
    lane = lax.broadcasted_iota(jnp.int32, square, 1)
    line = lax.broadcasted_iota(jnp.int32, square, 0)
    named = r.routes[...]
    weight = r.route_weight[...]
    share = weight / jnp.sum(weight, axis=0, keepdims=True)
    chosen = jnp.zeros(square, F32)
    gate = jnp.zeros(square, F32)
    for k in range(TOP):
        match = named[k : k + 1] == line
        chosen = chosen + jnp.where(match, 1.0, 0.0)
        gate = gate + jnp.where(match, share[k : k + 1], 0.0)
    earlier = jnp.dot(
        chosen.astype(BF16),
        jnp.where(line < lane, 1.0, 0.0).astype(BF16),
        preferred_element_type=F32,
    )
    slot = lax.broadcasted_iota(jnp.int32, (slots, rows), 0).astype(F32)
    for expert in range(experts):
        pick = (chosen[expert : expert + 1] > 0.5) & (earlier[expert : expert + 1] == slot)
        r.select[expert] = jnp.where(pick, 1.0, 0.0).astype(BF16)
        r.weigh[expert * slots : (expert + 1) * slots, :] = jnp.where(
            pick, gate[expert : expert + 1], 0.0
        )
    weigh = r.weigh[...].T
    high = weigh.astype(BF16)
    r.high[...] = high
    r.low[...] = (weigh - high.astype(F32)).astype(BF16)


def project(r, loaded):
    offsets, _, _ = peer_offsets()
    me = lax.axis_index("tp")
    width = r.stream.shape[1]

    def piece(owner):
        columns = block_of(owner, width)
        return jnp.dot(
            r.heads_a[...], r.proj_a[:, columns], preferred_element_type=F32
        ) + jnp.dot(r.heads_b[...], r.proj_b[:, columns], preferred_element_type=F32)

    loaded()
    copies = []
    for at, offset in enumerate(offsets):
        peer = peer_at(*offset)
        r.branch_out[at] = piece(peer).astype(BF16)
        copy = remote(
            r.branch_out.at[at], r.branch_in.at[at], r.branch_s.at[0], r.branch_r.at[at], "tp", peer
        )
        copy.start()
        copies.append(copy)
    r.branch_own[...] = r.residual[...].astype(F32) + piece(me)

    def settle():
        summed = r.branch_own[...]
        for at, copy in reversed(list(enumerate(copies))):
            copy.wait_recv()
            summed = summed + r.branch_in[at].astype(F32)
        r.stream[...] = summed.astype(BF16)

    def drain():
        wait_bytes(r.branch_out, r.branch_s.at[0])

    return settle, drain


def experts_part(r):
    offsets, ny, nx = peer_offsets()
    seq, heads = lax.axis_size("sp"), lax.axis_size("tp")
    me, mine = lax.axis_index("sp"), lax.axis_index("tp")
    chips = seq // 2
    chip, core = me // 2, lax.rem(me, 2)
    experts, slots, rows = r.select.shape
    width = r.stream.shape[1]
    square = ny == 2 and nx == 2
    across_x, across_y, across_both = peer_at(0, 1), peer_at(1, 0), peer_at(1, 1)
    top, bottom = pl.ds(0, slots), pl.ds(slots, slots)

    half = chips // 2

    def source(k):
        late = half + lax.rem(lax.rem(chip, half) + 1 + k, half)
        return jnp.where(k < half, k, late)

    def distance(k):
        return lax.rem(chip + chips - source(k), chips)

    def outgoing(step, side):
        target_core = core if side == 0 else 1 - core
        expert = 2 * lax.rem(chip + step, chips) + target_core
        return expert, remote(
            r.send.at[expert],
            r.rows.at[chip, block_of(core, slots), block_of(mine, width)],
            r.out_s.at[0],
            r.out_r.at[step],
            "sp",
            expert,
        )

    def send_out(steps, upward=False):
        for step in sorted(
            steps, key=lambda step: (step == 0, step if upward else 0, step % 2 == 0, -step)
        ):
            for side in range(2):
                expert, copy = outgoing(step, side)
                picked = jnp.dot(r.select[expert], r.stream[...], preferred_element_type=F32)
                if step == 0 and side == 0:
                    place = (chip, block_of(core, slots), block_of(mine, width))
                    r.rows[place] = picked.astype(BF16)
                else:
                    r.send[expert] = picked.astype(BF16)
                    copy.start()

    def land(k):
        @pl.when(distance(k) > 0)
        def _():
            wait_bytes(r.rows.at[source(k), :, block_of(mine, width)], r.out_r.at[distance(k)])

        @pl.when(distance(k) == 0)
        def _():
            wait_bytes(r.rows.at[source(k), bottom, block_of(mine, width)], r.out_r.at[0])

    def spread(step, at, peer, owner):
        ref = r.rows.at[source(step), :, block_of(owner, width)]
        return remote(ref, ref, r.spread_s.at[0], r.spread_r.at[step], "tp", peer)

    def relay(step, at, peer, owner):
        ref = r.rows.at[source(step), top if at == 0 else bottom, block_of(owner, width)]
        return remote(ref, ref, r.relay_s.at[0], r.relay_r.at[step], "tp", peer)

    near = ((0, 1), (1, 0)) if square else offsets

    def start_spread(step):
        land(step)
        for at, offset in enumerate(near):
            spread(step, at, peer_at(*offset), mine).start()

    def start_relay(step):
        wait_bytes(r.rows.at[source(step), :, : len(near) * width], r.spread_r.at[step])
        if square:
            relay(step, 0, across_y, across_x).start()
            relay(step, 1, across_x, across_y).start()

    def ready(step):
        if square:
            wait_bytes(r.rows.at[source(step), :, :width], r.relay_r.at[step])

    def compute(step):
        origin = source(step)
        wide = r.rows[origin].astype(F32)
        mean_sq = jnp.mean(wide * wide, axis=1, keepdims=True)
        normed = (wide * lax.rsqrt(mean_sq + EPS) * r.norm_gain[...]).astype(BF16)
        gate = jnp.dot(normed, r.gate[...], preferred_element_type=F32)
        up = jnp.dot(normed, r.up[...], preferred_element_type=F32)
        hidden = (gate / (1.0 + jnp.exp(-gate)) * up).astype(BF16)
        r.down_out[step] = jnp.dot(hidden, r.down[...], preferred_element_type=F32).astype(BF16)

    def first_copies(step):
        if not square:
            return [
                remote(
                    r.down_out.at[step, :, block_of(peer_at(*offset), width)],
                    r.first.at[step, at],
                    r.first_s.at[0],
                    r.first_r.at[step, 0],
                    "tp",
                    peer_at(*offset),
                )
                for at, offset in enumerate(offsets)
            ]
        plan = (
            (top, across_x, across_both, 1),
            (bottom, across_y, across_both, 3),
            (top, across_x, across_x, 0),
            (bottom, across_y, across_y, 2),
        )
        return [
            remote(
                r.down_out.at[step, part, block_of(owner, width)],
                r.first.at[step, slot],
                r.first_s.at[0],
                r.first_r.at[step, slot % 2],
                "tp",
                peer,
            )
            for part, peer, owner, slot in plan
        ]

    def second_copies(step):
        return [
            remote(
                r.second_out.at[step, at],
                r.second.at[step, at],
                r.second_s.at[0],
                r.second_r.at[step],
                "tp",
                peer,
            )
            for at, peer in enumerate((across_y, across_x))
        ]

    def start_first(step):
        for copy in first_copies(step):
            copy.start()

    def start_second(step):
        if not square:
            return
        seconds = second_copies(step)
        wait_bytes(r.first.at[step, :2], r.first_r.at[step, 1])
        for at, part, owner, slot in ((0, top, across_y, 1), (1, bottom, across_x, 3)):
            summed = r.down_out[step, part, block_of(owner, width)].astype(F32)
            summed = summed + r.first[step, slot].astype(F32)
            r.second_out[step, at] = summed.astype(BF16)
            seconds[at].start()

    def home(step, side):
        origin_core = core if side == 0 else 1 - core
        return remote(
            r.summed.at[step, side],
            r.back.at[me],
            r.home_s.at[0],
            r.home_r.at[0],
            "sp",
            2 * source(step) + origin_core,
        )

    def start_home(step):
        own = block_of(mine, width)
        if square:
            wait_bytes(r.first.at[step, :2], r.first_r.at[step, 0])
            wait_bytes(r.second.at[step], r.second_r.at[step])
            halves = []
            for at, part, slot in ((0, top, 0), (1, bottom, 2)):
                halves.append(
                    r.down_out[step, part, own].astype(F32)
                    + r.first[step, slot].astype(F32)
                    + r.second[step, at].astype(F32)
                )
            r.sums[0] = halves[0].astype(BF16)
            r.sums[1] = halves[1].astype(BF16)
        else:
            wait_bytes(r.first.at[step], r.first_r.at[step, 0])
            summed = r.down_out[step, :, own].astype(F32)
            for at in range(len(offsets)):
                summed = summed + r.first[step, at].astype(F32)
            r.sums[0] = summed[:slots].astype(BF16)
            r.sums[1] = summed[slots:].astype(BF16)
        r.summed[step, 0] = r.sums[core]
        r.summed[step, 1] = r.sums[1 - core]

        @pl.when(distance(step) == 0)
        def _():
            r.back[me] = r.summed[step, 0]

        @pl.when(distance(step) > 0)
        def _():
            home(step, 0).start()

        home(step, 1).start()

    def start():
        start_spread(0)

    def first_relay():
        start_relay(0)

    def others():
        def body(k, carry):
            start_relay(k)

            @pl.when(k + 1 < chips)
            def _():
                start_spread(k + 1)

            ready(k)
            start_second(k - 1)

            @pl.when(k >= 2)
            def _():
                start_home(k - 2)

            compute(k)
            start_first(k)
            return carry

        lax.fori_loop(1, chips, body, 0)
        start_home(chips - 2)
        start_second(chips - 1)
        start_home(chips - 1)
        finish()

    def finish():
        wait_bytes(r.back.at[: experts - 1], r.home_r.at[0])
        back = r.back[...].reshape(experts * slots, width)
        mixed = jnp.dot(r.high[...], back, preferred_element_type=F32)
        mixed = mixed + jnp.dot(r.low[...], back, preferred_element_type=F32)
        r.out[...] = (r.stream[...].astype(F32) + mixed).astype(BF16)

    def drain():
        wait_bytes(r.send.at[: experts - 1], r.out_s.at[0])
        wait_bytes(r.back.at[: experts - 1], r.home_s.at[0])
        wait_bytes(r.rows.at[:, :, : len(near) * width], r.spread_s.at[0])
        wait_bytes(r.first, r.first_s.at[0])
        if square:
            wait_bytes(r.rows.at[:, :, :width], r.relay_s.at[0])
            wait_bytes(r.second, r.second_s.at[0])

    return send_out, start, first_relay, ready, compute, start_first, start_spread, others, drain


def layer(args):
    seq, heads_dev = lax.axis_size("sp"), lax.axis_size("tp")
    rows, heads, width_a = args["qa"].shape
    width_b = args["qb"].shape[2]
    value_a, value_b = args["va"].shape[2], args["vb"].shape[2]
    model = args["residual"].shape[1]
    width = model // heads_dev
    chips = seq // 2
    half = chips // 2
    blocks = 2 * half
    slots = 2 * rows * TOP // seq
    _, ny, nx = peer_offsets()
    square = ny == 2 and nx == 2
    first_shape = (4, slots, width) if square else (heads_dev - 1, 2 * slots, width)
    dma = pltpu.SemaphoreType.DMA
    big = ("qa", "ka", "va", "qb", "kb", "vb", "residual", "proj_a", "proj_b", "gate", "up", "down")
    small = ("lam_a", "lam_b", "gain_a", "gain_b", "norm_gain", "routes", "route_weight")

    def landing(name):
        shape = args[name].shape
        if name == "residual":
            shape = (rows, width)
        if len(shape) == 3 and name in ("gate", "up", "down"):
            shape = shape[1:]
        return pltpu.VMEM(shape, args[name].dtype)

    scratch = {name: landing(name) for name in big}
    scratch.update(
        load_s=dma((len(big),)),
        go=pltpu.SemaphoreType.REGULAR,
        heads_a=pltpu.VMEM((rows, heads * value_a), BF16),
        heads_b=pltpu.VMEM((rows, heads * value_b), BF16),
        kv=pltpu.VMEM((blocks, heads, rows, width_a + value_a + width_b + value_b), BF16),
        query=pltpu.VMEM((heads, rows, width_a + width_b), BF16),
        far_query=pltpu.VMEM((half, heads, rows, width_a + width_b), BF16),
        far_stats=pltpu.VMEM((half, heads, 8, rows), F32),
        own_stats=pltpu.VMEM((heads, 8, rows), F32),
        keep=pltpu.VMEM((heads, 4, rows, blocks * rows), F32),
        part=pltpu.VMEM((half, heads, rows, value_a + value_b), BF16),
        far_part=pltpu.VMEM((heads, rows, value_a + value_b), BF16),
        total=pltpu.VMEM((half, heads, 8, rows), F32),
        far_total=pltpu.VMEM((heads, 8, rows), F32),
        chain_s=dma((max(half - 1, 1), heads, 2)), chain_r=dma((max(half - 1, 1), heads, 2)),
        part_s=dma((1,)), part_r=dma((heads, 2)),
        query_s=dma((1,)), query_r=dma((half, heads)),
        stats_s=dma((1,)), stats_r=dma((half, heads)),
        back_s=dma((1,)), back_r=dma((heads,)),
        total_s=dma((1,)), total_r=dma((heads,)),
        branch_out=pltpu.VMEM((heads_dev - 1, rows, width), BF16),
        branch_own=pltpu.VMEM((rows, width), F32),
        branch_in=pltpu.VMEM((heads_dev - 1, rows, width), BF16),
        branch_s=dma((1,)), branch_r=dma((heads_dev - 1,)),
        stream=pltpu.VMEM((rows, width), BF16),
        select=pltpu.VMEM((seq, slots, rows), BF16),
        weigh=pltpu.VMEM((seq * slots, rows), F32),
        high=pltpu.VMEM((rows, seq * slots), BF16),
        low=pltpu.VMEM((rows, seq * slots), BF16),
        send=pltpu.VMEM((seq, slots, width), BF16),
        rows=pltpu.VMEM((chips, 2 * slots, model), BF16),
        out_s=dma((1,)), out_r=dma((chips,)),
        spread_s=dma((1,)), spread_r=dma((chips,)),
        relay_s=dma((1,)), relay_r=dma((chips,)),
        down_out=pltpu.VMEM((chips, 2 * slots, model), BF16),
        first=pltpu.VMEM((chips,) + first_shape, BF16),
        first_s=dma((1,)), first_r=dma((chips, 2)),
        second_out=pltpu.VMEM((chips, 2, slots, width), BF16),
        second=pltpu.VMEM((chips, 2, slots, width), BF16),
        second_s=dma((1,)), second_r=dma((chips,)),
        sums=pltpu.VMEM((2, slots, width), BF16),
        summed=pltpu.VMEM((chips, 2, slots, width), BF16),
        back=pltpu.VMEM((seq, slots, width), BF16),
        home_s=dma((1,)), home_r=dma((1,)),
    )

    def kernel(*refs):
        small_refs = refs[: len(small)]
        hbm = Refs(big, refs[len(small) : len(small) + len(big)])
        at = len(small) + len(big)
        r = Refs(
            small + ("out",) + tuple(scratch), tuple(small_refs) + (refs[at],) + tuple(refs[at + 1 :])
        )

        def load(name):
            source = getattr(hbm, name)
            if name == "residual":
                source = source.at[:, block_of(lax.axis_index("tp"), width)]
            if name in ("gate", "up", "down"):
                source = source.at[0]
            return pltpu.make_async_copy(source, getattr(r, name), r.load_s.at[big.index(name)])

        def wait(*names):
            for name in names:
                load(name).wait()

        for name in big:
            load(name).start()
        greeted = greet(("sp", "tp"))
        (
            send_out, start, first_relay, ready, compute, start_first, start_spread, others,
            drain_experts,
        ) = experts_part(r)
        chip = lax.axis_index("sp") // 2
        drain_heads, answered = attend(
            r, lambda: wait("qa", "ka", "va", "qb", "kb", "vb"), greeted, lambda: route(r)
        )

        settle, drain_branch = project(r, lambda: wait("residual", "proj_a", "proj_b"))
        wait("gate", "up", "down")

        @pl.when(chip == half - 1)
        def _():
            answered()
            if half > 1:
                pl.semaphore_signal(
                    r.go, inc=1, device_id={"sp": lax.rem(lax.axis_index("sp"), 2)}, device_id_type=MESH
                )

        @pl.when(chip == 0)
        def _():
            settle()
            send_out(range(half))
            start()
            first_relay()
            ready(0)
            compute(0)
            start_first(0)
            if half > 1:
                pl.semaphore_wait(r.go, 1)
            send_out(range(half, chips))
            start_spread(1)

        @pl.when(chip > 0)
        def _():
            start()
            settle()
            pl.when(chip >= half)(lambda: send_out(range(chips)))
            pl.when(chip < half)(lambda: send_out(range(chips), True))
            first_relay()
            start_spread(1)
            ready(0)
            compute(0)
            start_first(0)

        others()
        drain_heads()
        drain_branch()
        drain_experts()

    vmem = pl.BlockSpec(memory_space=pltpu.VMEM)
    specs = [pl.BlockSpec(memory_space=pltpu.SMEM)] * 2 + [vmem] * (len(small) - 2)
    specs += [pl.BlockSpec(memory_space=pl.ANY)] * len(big)
    return pl.pallas_call(
        kernel,
        out_shape=jax.ShapeDtypeStruct((rows, width), BF16),
        in_specs=specs,
        out_specs=vmem,
        scratch_shapes=list(scratch.values()),
        compiler_params=pltpu.CompilerParams(
            collective_id=0, has_side_effects=True, vmem_limit_bytes=56 * 2**20
        ),
        name="layer",
    )(*[args[name] for name in small + big])


def local(
    residual,
    query_a,
    keys_a,
    values_a,
    query_b,
    keys_b,
    values_b,
    lambda_a,
    lambda_b,
    gain_a,
    gain_b,
    proj_a,
    proj_b,
    norm_gain,
    routes,
    route_weight,
    expert_gate,
    expert_up,
    expert_down,
):
    args = dict(
        residual=residual,
        qa=query_a,
        ka=keys_a,
        va=values_a,
        qb=query_b,
        kb=keys_b,
        vb=values_b,
        lam_a=lambda_a,
        lam_b=lambda_b,
        gain_a=gain_a.reshape(1, -1),
        gain_b=gain_b.reshape(1, -1),
        proj_a=proj_a,
        proj_b=proj_b,
        norm_gain=norm_gain.reshape(1, -1),
        routes=routes.T,
        route_weight=route_weight.T,
        gate=expert_gate,
        up=expert_up,
        down=expert_down,
    )
    return layer(args)


def solution(mesh):
    placed = (
        P("sp", None),
        P("sp", "tp", None),
        P("sp", "tp", None),
        P("sp", "tp", None),
        P("sp", "tp", None),
        P("sp", "tp", None),
        P("sp", "tp", None),
        P("tp"),
        P("tp"),
        P(),
        P(),
        P("tp", None),
        P("tp", None),
        P(),
        P("sp", None),
        P("sp", None),
        P("sp", None, "tp"),
        P("sp", None, "tp"),
        P("sp", "tp", None),
    )
    return jax.shard_map(
        local, mesh=mesh, in_specs=placed, out_specs=P("sp", "tp"), check_vma=False
    )
```
